256 devices in a mesh: ep: 32 (over z, x), tp: 8 (over y, core).
Axes of the slice: x: 4, y: 4, z: 8, core: 2. Of those that a mesh axis runs over, the one named last changes fastest.
Arguments:
- tokens: bfloat16 [1536, 2048], P('ep'), may hold values from -6 to 6
- state: float32 [1536, 8, 128, 128], P('ep', 'tp'), may hold values from -4 to 4
- norm_gain: float32 [2048], replicated, may hold values from 0.1 to 1.9
- w_query: bfloat16 [2048, 1024], P('ep', 'tp'), may hold values from -0.125 to 0.125
- w_forget: bfloat16 [2048, 1024], P('ep', 'tp'), may hold values from -0.125 to 0.125
- w_input: bfloat16 [2048, 1024], P('ep', 'tp'), may hold values from -0.125 to 0.125
- w_outgate: bfloat16 [2048, 1024], P('ep', 'tp'), may hold values from -0.125 to 0.125
- lower_bound: float32 [1024], P('tp'), may hold values from 0 to 0.9
- head_gain: float32 [1024], P('tp'), may hold values from 0.1 to 1.9
- w_output: bfloat16 [1024, 2048], P('tp'), may hold values from -0.1875 to 0.1875
- ffn_gain: float32 [2048], replicated, may hold values from 0.1 to 1.9
- route_ids: int32 [1536, 4], P('ep'), may hold values from 0 to 63, all different within a row; in each aligned block of 48 rows (0 to 47, 48 to 95, ...) at most 6 rows name the same one
- route_weight: float32 [1536, 4], P('ep'), may hold values from 0.2 to 1
- expert_gate: bfloat16 [64, 2048, 1024], P('ep', None, 'tp'), may hold values from -0.125 to 0.125
- expert_up: bfloat16 [64, 2048, 1024], P('ep', None, 'tp'), may hold values from -0.125 to 0.125
- expert_down: bfloat16 [64, 1024, 2048], P('ep', 'tp'), may hold values from -0.1875 to 0.1875
- shared_gate: bfloat16 [2048, 1024], P(None, 'tp'), may hold values from -0.125 to 0.125
- shared_up: bfloat16 [2048, 1024], P(None, 'tp'), may hold values from -0.125 to 0.125
- shared_down: bfloat16 [1024, 2048], P('tp'), may hold values from -0.1875 to 0.1875
- dense_gate: bfloat16 [2048, 8192], P('tp', 'ep'), may hold values from -0.125 to 0.125
- dense_up: bfloat16 [2048, 8192], P('tp', 'ep'), may hold values from -0.125 to 0.125
- dense_down: bfloat16 [8192, 2048], P('ep', 'tp'), may hold values from -0.0625 to 0.0625
- dense_mix: float32 [2048], P('tp'), may hold values from -6 to 6
Outputs:
- mixed: bfloat16 [1536, 2048], P('ep', 'tp')
- new_state: float32 [1536, 8, 128, 128], P('ep', 'tp')
The draws below stay inside these ranges and needn't reach their ends.
Inputs may be any that keep to these rules, and one draw needn't show every extreme that they name: `route_ids`: each row names 4 different experts. Among the rows of one device no expert is named more than 6 times, and in every draw some expert is named exactly 6 times by some device's rows.
All inputs are finite; a program needn't handle non-finite values.
Results may differ from the reference program's by a relative error of at most 0.025.
Values may be sent and summed in bfloat16 or wider, within the bound.
No kernel may reach another device: no remote copies, remote signals or barrier semaphores. Data moves between devices by JAX's collectives and lax.ppermute only.
A program may use at most 64 MiB of HBM per device.

```python
import math
import jax
import jax.numpy as jnp
import numpy as np
from jax import lax

WIDTH = 2048
HEADS = 8
HEAD_DIM = 128
MIX_WIDTH = 1024
EXPERTS = 64
TOPK = 4
EXPERT_FF = 1024
SHARED_FF = 1024
DENSE_FF = 8192
SEQ_DEV = 48
BATCH = 1536
CAP = 6
N_EP = 32
N_TP = 8


def shard_levels(rng, extent, cuts, smallest, largest):
    level = 1.0
    for axis_at, blocks in cuts:
        steps = jax.random.uniform(jax.random.fold_in(jax.random.fold_in(rng, 6), axis_at), (blocks,), jnp.float32, smallest / len(cuts), largest / len(cuts))
        level = level * jnp.repeat(jnp.exp(steps), extent[axis_at] // blocks).reshape((-1,) + (1,) * (len(extent) - 1 - axis_at))
    return level


def assign_block(key, own, number, rows, amount, top, limit, skew):
    order = jax.random.permutation(key, amount)
    crowded, usual = portions_of(amount, rows * top, limit, skew, True), portions_of(amount, rows * top, limit, skew, False)
    places = jnp.arange(amount)

    def named(tallies, turn):
        used = int((tallies > 0).sum())
        fixed = max(1, used // 4)
        moved = fixed + (places - fixed + turn * (used - fixed)) % max(1, amount - fixed)
        return jnp.zeros((amount,), jnp.int32).at[order[jnp.where(places < fixed, places, moved)]].set(jnp.asarray(tallies, jnp.int32))

    tallies = jnp.where(number % 4 == 0, named(crowded, number // 4), named(usual, number - number // 4 - 1))
    mixed = jax.random.permutation(jax.random.fold_in(own, 3), amount)
    giver, taker = mixed[0:amount // 2 * 2:2], mixed[1:amount // 2 * 2:2]
    room = jnp.minimum(tallies[giver] - 1, limit - tallies[taker]) // 2
    room = jnp.where((giver == order[0]) | (taker == order[0]) | (tallies[taker] == 0), 0, jnp.maximum(room, 0))
    moved = jax.random.randint(jax.random.fold_in(own, 4), (amount // 2,), 0, 1 << 20) % (room + 1)
    tallies = tallies.at[giver].add(-moved).at[taker].add(moved)
    members = jnp.searchsorted(jnp.cumsum(tallies), jnp.arange(rows * top), side="right").astype(jnp.int32)
    listing = members.reshape(top, rows).T
    listing = listing[jax.random.permutation(jax.random.fold_in(own, 1), rows)]
    turn = jax.random.randint(jax.random.fold_in(own, 2), (rows, 1), 0, top)
    return jnp.take_along_axis(listing, (jnp.arange(top)[None, :] + turn) % top, axis=1)


def portions_of(count, total, reach, skew, full):
    loads = [(1 << 20) // math.isqrt(rank ** skew) + 1 for rank in range(1, count + 1)]
    largest = reach if full else min(reach, max(-(-total // count), total * loads[0] // sum(loads)))
    least = 1 if total - largest >= count - 1 else 0
    holding, rest = [largest] + [least] * (count - 1), total - largest - least * (count - 1)
    while rest > 0:
        movable = [i for i in range(1, count) if holding[i] < largest] or [i for i in range(1, count) if holding[i] < reach]
        whole, remaining = sum([loads[i] for i in movable]), rest
        for i in movable:
            more = min(reach - holding[i], max(1, remaining * loads[i] // whole), rest)
            holding[i] = holding[i] + more
            rest = rest - more
    return np.array(holding)


def bell_draw(stream_key, shape, deviation, bound, cuts=(), held_as=jnp.bfloat16):
    result = deviation * jax.random.normal(stream_key, shape, jnp.float32)
    if cuts:
        result = result * shard_levels(stream_key, shape, cuts, -0.22, 0.18)
    return jnp.clip(result, -bound, bound).astype(held_as)


def setup_inputs(seed: int = 0) -> dict:
    keys = jax.random.split(jax.random.key(seed), 24)
    tokens = bell_draw(keys[0], (BATCH, WIDTH), 1.0, 6.0, ((0, 32),))
    state = bell_draw(keys[1], (BATCH, HEADS, HEAD_DIM, HEAD_DIM), 0.5, 4.0, ((0, 32), (1, 8)), jnp.float32)
    norm_gain = jnp.clip(1.0 + 0.18 * jax.random.normal(keys[2], (WIDTH,), jnp.float32), 0.1, 1.9)
    w_query = bell_draw(keys[3], (WIDTH, MIX_WIDTH), WIDTH ** -0.5, 0.125, ((0, 32), (1, 8)))
    w_forget = bell_draw(keys[4], (WIDTH, MIX_WIDTH), WIDTH ** -0.5, 0.125, ((0, 32), (1, 8)))
    w_input = bell_draw(keys[5], (WIDTH, MIX_WIDTH), WIDTH ** -0.5, 0.125, ((0, 32), (1, 8)))
    w_outgate = bell_draw(keys[6], (WIDTH, MIX_WIDTH), WIDTH ** -0.5, 0.125, ((0, 32), (1, 8)))
    lower_bound = jnp.clip(0.9 * jax.random.uniform(keys[7], (MIX_WIDTH,), jnp.float32) ** shard_levels(keys[7], (MIX_WIDTH,), ((0, 8),), -0.2, 0.2), 0.0, 0.9)
    head_gain = jnp.clip(1.0 + 0.18 * jax.random.normal(keys[8], (MIX_WIDTH,), jnp.float32), 0.1, 1.9)
    w_output = bell_draw(keys[9], (MIX_WIDTH, WIDTH), MIX_WIDTH ** -0.5, 0.1875, ((0, 8),))
    ffn_gain = jnp.clip(1.0 + 0.18 * jax.random.normal(keys[10], (WIDTH,), jnp.float32), 0.1, 1.9)
    route_ids_keys = jax.random.split(jax.random.fold_in(keys[11], 1), BATCH // SEQ_DEV)
    route_ids_turns = jax.random.permutation(jax.random.fold_in(keys[11], 3), BATCH // SEQ_DEV)
    route_ids = jax.vmap(lambda own, number: assign_block(jax.random.fold_in(keys[11], 2), own, number, SEQ_DEV, EXPERTS, TOPK, CAP, 2))(route_ids_keys, route_ids_turns).reshape((BATCH, TOPK))
    route_weight = jnp.clip(0.2 + 0.8 * jax.random.uniform(keys[12], (BATCH, TOPK), jnp.float32) ** shard_levels(keys[12], (BATCH, TOPK), ((0, 32),), -0.2, 0.2), 0.2, 1.0)
    expert_gate = bell_draw(keys[13], (EXPERTS, WIDTH, EXPERT_FF), WIDTH ** -0.5, 0.125, ((0, 32), (2, 8)))
    expert_up = bell_draw(keys[14], (EXPERTS, WIDTH, EXPERT_FF), WIDTH ** -0.5, 0.125, ((0, 32), (2, 8)))
    expert_down = bell_draw(keys[15], (EXPERTS, EXPERT_FF, WIDTH), EXPERT_FF ** -0.5, 0.1875, ((0, 32), (1, 8)))
    shared_gate = bell_draw(keys[16], (WIDTH, SHARED_FF), WIDTH ** -0.5, 0.125, ((1, 8),))
    shared_up = bell_draw(keys[17], (WIDTH, SHARED_FF), WIDTH ** -0.5, 0.125, ((1, 8),))
    shared_down = bell_draw(keys[18], (SHARED_FF, WIDTH), SHARED_FF ** -0.5, 0.1875, ((0, 8),))
    dense_gate = bell_draw(keys[19], (WIDTH, DENSE_FF), WIDTH ** -0.5, 0.125, ((0, 8), (1, 32)))
    dense_up = bell_draw(keys[20], (WIDTH, DENSE_FF), WIDTH ** -0.5, 0.125, ((0, 8), (1, 32)))
    dense_down = bell_draw(keys[21], (DENSE_FF, WIDTH), DENSE_FF ** -0.5, 0.0625, ((0, 32), (1, 8)))
    dense_mix = bell_draw(keys[22], (WIDTH,), 1.5, 6.0, ((0, 8),), jnp.float32)
    return dict(tokens=tokens, state=state, norm_gain=norm_gain, w_query=w_query, w_forget=w_forget, w_input=w_input, w_outgate=w_outgate, lower_bound=lower_bound, head_gain=head_gain, w_output=w_output, ffn_gain=ffn_gain, route_ids=route_ids, route_weight=route_weight, expert_gate=expert_gate, expert_up=expert_up, expert_down=expert_down, shared_gate=shared_gate, shared_up=shared_up, shared_down=shared_down, dense_gate=dense_gate, dense_up=dense_up, dense_down=dense_down, dense_mix=dense_mix)


EPS = 1e-06

def rms_scale(values, gain):
    values = values.astype(jnp.float32)
    return values * lax.rsqrt(lax.optimization_barrier(jnp.mean(values * values, axis=-1, keepdims=True)) + EPS) * gain

def rounded(values):
    return lax.optimization_barrier(values.astype(jnp.bfloat16)).astype(jnp.float32)

def blocked_sum(left, right, pieces):
    inner = left.shape[1] // pieces
    total = jnp.zeros((left.shape[0], right.shape[1]), jnp.float32)
    for index in range(pieces):
        part = jnp.dot(left[:, index * inner:(index + 1) * inner], right[index * inner:(index + 1) * inner], preferred_element_type=jnp.float32)
        total = total + rounded(part)
    return total

def reference(tokens, state, norm_gain, w_query, w_forget, w_input, w_outgate, lower_bound, head_gain, w_output, ffn_gain, route_ids, route_weight, expert_gate, expert_up, expert_down, shared_gate, shared_up, shared_down, dense_gate, dense_up, dense_down, dense_mix):
    batch = tokens.shape[0]
    normed = rms_scale(tokens, norm_gain).astype(jnp.bfloat16)

    def project(weight):
        return rounded(jnp.dot(normed, weight, preferred_element_type=jnp.float32))
    query, forget_pre, values, out_gate = [project(w) for w in (w_query, w_forget, w_input, w_outgate)]
    forget_sig = jax.nn.sigmoid(forget_pre)
    shape = (batch, HEADS, HEAD_DIM)
    decay = (lower_bound + (1.0 - lower_bound) * forget_sig).reshape(shape)
    keygate = ((1.0 - lower_bound) * (1.0 - forget_sig)).reshape(shape)
    new_state = decay[..., None] * state + keygate[..., None] * values.reshape(shape)[:, :, None, :]
    readout = jnp.einsum('bhk,bhkv->bhv', query.reshape(shape), new_state, precision=lax.Precision.HIGHEST)
    readout = readout * lax.rsqrt(lax.optimization_barrier(jnp.mean(readout * readout, axis=-1, keepdims=True)) + EPS)
    head_out = (readout.reshape(batch, MIX_WIDTH) * head_gain * jax.nn.silu(out_gate)).astype(jnp.bfloat16)
    resid = tokens.astype(jnp.float32) + blocked_sum(head_out, w_output, N_TP)
    moe_in = rms_scale(resid, ffn_gain).astype(jnp.bfloat16)
    flat_ids = route_ids.reshape(N_EP, SEQ_DEV * TOPK)
    onehot = (flat_ids[..., None] == jnp.arange(EXPERTS, dtype=jnp.int32)).astype(jnp.int32)
    slot_rank = lax.optimization_barrier(jnp.sum((jnp.cumsum(onehot, axis=1) - onehot) * onehot, axis=-1))
    device = jnp.arange(N_EP, dtype=jnp.int32)[:, None]
    slot_index = ((flat_ids * N_EP + device) * CAP + slot_rank).reshape(-1).astype(jnp.int32)
    token_index = jnp.repeat(jnp.arange(batch, dtype=jnp.int32), TOPK)
    table = jnp.full((EXPERTS * N_EP * CAP,), batch, jnp.int32).at[slot_index].set(token_index)
    padded = jnp.concatenate([moe_in, jnp.zeros((1, WIDTH), jnp.bfloat16)], axis=0)
    gathered = padded[table].reshape(EXPERTS, N_EP * CAP, WIDTH)

    def one_expert(args):
        rows_in, gate_weight, up_weight, down_weight = args
        gate_pre = jnp.dot(rows_in, gate_weight, preferred_element_type=jnp.float32)
        up_pre = jnp.dot(rows_in, up_weight, preferred_element_type=jnp.float32)
        hidden = (jax.nn.silu(gate_pre) * up_pre).astype(jnp.bfloat16)
        return blocked_sum(hidden, down_weight, N_TP).astype(jnp.bfloat16)
    outputs = lax.map(one_expert, (gathered, expert_gate, expert_up, expert_down)).reshape(-1, WIDTH)
    picked = outputs[slot_index].reshape(batch, TOPK, WIDTH).astype(jnp.float32)
    routed = lax.optimization_barrier(jnp.sum(route_weight[..., None] * picked, axis=1))
    shared_hidden = (jax.nn.silu(jnp.dot(moe_in, shared_gate, preferred_element_type=jnp.float32)) * jnp.dot(moe_in, shared_up, preferred_element_type=jnp.float32)).astype(jnp.bfloat16)
    shared_out = blocked_sum(shared_hidden, shared_down, N_TP)
    dense_pre_gate = blocked_sum(moe_in, dense_gate, N_TP)
    dense_pre_up = blocked_sum(moe_in, dense_up, N_TP)
    dense_hidden = (jax.nn.silu(dense_pre_gate) * dense_pre_up).astype(jnp.bfloat16)
    dense_out = jnp.dot(dense_hidden, dense_down, preferred_element_type=jnp.float32)
    mixed = (resid + routed + shared_out + jax.nn.sigmoid(dense_mix) * dense_out).astype(jnp.bfloat16)
    return (mixed, new_state)
```

```python
import jax
import jax.numpy as jnp
from jax import lax
from jax.sharding import Mesh
from jax.sharding import PartitionSpec as P

EP = ("z", "x")
TP = ("y", "c")
HUB = ("z", "x", "c")

EPS = 1e-06
BF = jnp.bfloat16
F32 = jnp.float32


def swap(x, axis):
    return lax.all_to_all(x, axis, split_axis=0, concat_axis=0, tiled=True)


def spread(x, axis):
    return swap(jnp.broadcast_to(x, (lax.axis_size(axis), *x.shape)), axis)


def partner(x):
    return lax.ppermute(x, "c", [(0, 1), (1, 0)])


def dot(a, b):
    return jnp.dot(a, b, preferred_element_type=F32)


def local(
    tokens,
    state,
    norm_gain,
    w_query,
    w_forget,
    w_input,
    w_outgate,
    lower_bound,
    head_gain,
    w_output,
    ffn_gain,
    route_ids,
    route_weight,
    expert_gate,
    expert_up,
    expert_down,
    shared_gate,
    shared_up,
    shared_down,
    dense_gate,
    dense_up,
    dense_down,
    dense_mix,
):
    nz, nx, ny, nc = (lax.axis_size(a) for a in ("z", "x", "y", "c"))
    y, c = lax.axis_index("y"), lax.axis_index("c")
    seq, width = tokens.shape
    rows_w, chan = w_query.shape
    head_dim = state.shape[2]
    cols = width // (ny * nc)
    own_at = (y * nc + c) * cols

    joined = jnp.concatenate([w_query, w_forget, w_input, w_outgate], axis=1)
    weights = spread(joined, "z").reshape(nz * rows_w, 4 * chan)
    wide = tokens.astype(F32)
    normed = wide * lax.rsqrt(jnp.mean(wide * wide, axis=-1, keepdims=True) + EPS) * norm_gain
    normed = normed.astype(BF).reshape(seq, nz, nx, rows_w)
    normed = jnp.transpose(normed, (2, 0, 1, 3)).reshape(nx, seq, nz * rows_w)
    mine = swap(normed, "x").reshape(nx * seq, nz * rows_w)
    part = dot(mine, weights).astype(BF).reshape(nx, seq, 4 * chan)
    projected = swap(part, "x").astype(F32).sum(axis=0)
    projected = lax.optimization_barrier(projected.astype(BF)).astype(F32)
    query, forget_pre, values, out_gate = jnp.split(projected, 4, axis=1)

    dense_own = spread(jnp.stack([dense_gate, dense_up, dense_down]), "x")
    dense_other = partner(dense_own)

    def paired(stack, axis):
        keep = lax.dynamic_index_in_dim(stack, c, 0, keepdims=False)
        other = partner(lax.dynamic_index_in_dim(stack, 1 - c, 0, keepdims=False))
        return jnp.concatenate([keep, other], axis=axis)

    gate_w, up_w, down_w = (
        paired(expert_gate, 1),
        paired(expert_up, 1),
        paired(expert_down, 0),
    )

    def side(stack, index):
        picked = stack[:, index]
        return jnp.moveaxis(picked, 0, 1).reshape(picked.shape[1], -1)

    dense_in_w = jnp.concatenate(
        [
            jnp.concatenate([side(s, 0), side(s, 1)], axis=1)
            for s in (dense_own, dense_other)
        ],
        axis=0,
    )
    dense_out_w = jnp.concatenate(
        [s[:, 2].reshape(-1, cols) for s in (dense_own, dense_other)], axis=1
    )

    forget_sig = jax.nn.sigmoid(forget_pre)
    shape = (seq, 1, head_dim)
    decay = (lower_bound + (1.0 - lower_bound) * forget_sig).reshape(shape)
    keygate = ((1.0 - lower_bound) * (1.0 - forget_sig)).reshape(shape)
    new_state = decay[..., None] * state + keygate[..., None] * values.reshape(shape)[:, :, None, :]
    readout = jnp.einsum("bhk,bhkv->bhv", query.reshape(shape), new_state)
    readout = readout * lax.rsqrt(jnp.mean(readout * readout, axis=-1, keepdims=True) + EPS)
    head_out = (readout.reshape(seq, chan) * head_gain * jax.nn.silu(out_gate)).astype(BF)

    head_part = dot(head_out, w_output).astype(BF)
    head_part = jnp.moveaxis(head_part.reshape(seq, ny * nc, cols), 1, 0)
    resid = swap(head_part, TP).astype(F32).sum(axis=0)
    resid = resid + lax.dynamic_slice_in_dim(tokens, own_at, cols, 1).astype(F32)
    own = resid.astype(BF)

    topk = route_ids.shape[1]
    experts = nz * nx * nc
    cap = max(2, 2 * seq * topk // experts)
    flat_ids = route_ids.reshape(-1)
    onehot = (flat_ids[:, None] == jnp.arange(experts, dtype=jnp.int32)[None, :]).astype(jnp.int32)
    rank = jnp.sum((jnp.cumsum(onehot, axis=0) - onehot) * onehot, axis=1)
    slots = 2 * cap
    slot_index = (flat_ids * slots + rank).reshape(seq, topk)
    slot_ids = jnp.arange(experts * slots, dtype=jnp.int32)
    place = slot_ids % slots
    line = (slot_ids // slots) % (nx * nc) * cap + place - cap
    is_dense = place >= cap
    token_ids = jnp.arange(seq, dtype=jnp.int32)
    dense_hits = is_dense[None, :] & (line[None, :] == token_ids[:, None])
    hits = slot_index[:, :, None] == slot_ids[None, None, :]
    routed_hits = jnp.any(hits, axis=1)
    select = (routed_hits | dense_hits).astype(BF)
    half = cols // 2

    def to_lines(rows):
        rows = rows.reshape(experts, slots, 2, half)
        return jnp.transpose(rows, (0, 2, 1, 3)).reshape(experts, 2 * slots, half)

    def from_lines(lines):
        return jnp.transpose(lines.reshape(experts, 2, slots, half), (0, 2, 1, 3)).reshape(
            experts, slots, cols
        )

    outgoing = jnp.einsum("bs,bw->sw", select, own, preferred_element_type=F32).astype(BF)
    arrived = from_lines(swap(to_lines(outgoing), HUB)).reshape(nz * nx, nc, slots, cols)
    arrived_first, arrived_second = arrived[:, 0], arrived[:, 1]
    count = nz * nx * cap

    routed_rows = jnp.concatenate([arrived_first[:, :cap], arrived_second[:, :cap]], axis=2)
    routed_rows = routed_rows.reshape(count, nc * cols)
    other = partner(own)
    shared_rows = jnp.concatenate(
        [jnp.where(c == 0, own, other), jnp.where(c == 0, other, own)], axis=1
    )
    both = jnp.concatenate([routed_rows, shared_rows], axis=0)
    whole = spread(both, "y")
    whole = jnp.moveaxis(whole, 0, 1).reshape(count + seq, width).astype(F32)
    scale = lax.rsqrt(jnp.mean(whole * whole, axis=-1, keepdims=True) + EPS)
    moe_in = (whole * scale * ffn_gain).astype(BF)

    dense_own_rows = jnp.where(c == 0, arrived_first[:, cap:], arrived_second[:, cap:])
    dense_other_rows = jnp.where(c == 0, arrived_second[:, cap:], arrived_first[:, cap:])
    gain_own = lax.dynamic_slice_in_dim(ffn_gain, own_at, cols, 0)
    gain_other = lax.dynamic_slice_in_dim(ffn_gain, (y * nc + 1 - c) * cols, cols, 0)
    dense_rows = jnp.concatenate([dense_own_rows, dense_other_rows], axis=2)
    dense_rows = dense_rows.reshape(count, nc * cols).astype(F32)
    square = jnp.sum(dense_rows * dense_rows, axis=-1, keepdims=True)
    square_high = square.astype(BF)
    square_low = (square - square_high.astype(F32)).astype(BF)
    dense_scaled = (dense_rows * jnp.concatenate([gain_own, gain_other])).astype(BF)
    dense_pre = dot(dense_scaled, dense_in_w).astype(BF)
    lanes = 128
    dense_pre = jnp.concatenate(
        [
            dense_pre,
            jnp.broadcast_to(square_high, (count, lanes // 2)),
            jnp.broadcast_to(square_low, (count, lanes // 2)),
        ],
        axis=1,
    )
    dense_pre = swap(dense_pre.reshape(ny, count // ny, -1), "y").astype(F32).sum(axis=0)
    hidden_width = dense_in_w.shape[1] // 2
    total = dense_pre[:, 2 * hidden_width] + dense_pre[:, 2 * hidden_width + lanes // 2]
    dense_scale = lax.rsqrt(total / width + EPS)[:, None]
    dense_gate_pre = dense_pre[:, :hidden_width] * dense_scale
    dense_up_pre = dense_pre[:, hidden_width : 2 * hidden_width] * dense_scale
    dense_hidden = (jax.nn.silu(dense_gate_pre) * dense_up_pre).astype(BF)
    dense_hidden = spread(dense_hidden, "y").reshape(count, hidden_width)
    dense_part = dot(dense_hidden, dense_out_w).astype(BF).reshape(nz * nx, cap, nc, cols)
    dense_first = jnp.where(c == 0, dense_part[:, :, 0], dense_part[:, :, 1])
    dense_second = jnp.where(c == 0, dense_part[:, :, 1], dense_part[:, :, 0])

    routed_in, shared_in = moe_in[:count], moe_in[count:]
    hidden = (jax.nn.silu(dot(routed_in, gate_w)) * dot(routed_in, up_w)).astype(BF)
    expert_part = dot(hidden, down_w).astype(BF)
    shared_hidden = (
        jax.nn.silu(dot(shared_in, shared_gate)) * dot(shared_in, shared_up)
    ).astype(BF)
    shared_part = dot(shared_hidden, shared_down).astype(BF)
    parts = jnp.concatenate([expert_part, shared_part], axis=0)
    parts = jnp.moveaxis(parts.reshape(count + seq, ny, nc * cols), 1, 0)
    summed = swap(parts, "y").astype(F32).sum(axis=0)
    expert_out = summed[:count].astype(BF).reshape(nz * nx, cap, nc, cols)
    shared_sum = summed[count:]
    shared_own = jnp.where(c == 0, shared_sum[:, :cols], shared_sum[:, cols:])
    shared_send = jnp.where(c == 0, shared_sum[:, cols:], shared_sum[:, :cols])
    shared_out = shared_own + partner(shared_send.astype(BF)).astype(F32)

    first = jnp.concatenate([expert_out[:, :, 0], dense_first], axis=1)
    second = jnp.concatenate([expert_out[:, :, 1], dense_second], axis=1)
    back = jnp.stack([first, second], axis=1).reshape(experts * slots, cols)
    results = from_lines(swap(to_lines(back), HUB)).reshape(experts * slots, cols)
    combine = jnp.sum(jnp.where(hits, route_weight[:, :, None], F32(0.0)), axis=1)
    routed = dot(combine.astype(BF), results)
    dense_out = dot(dense_hits.astype(BF), results)
    mixed = (resid + routed + shared_out + jax.nn.sigmoid(dense_mix) * dense_out).astype(BF)
    return (mixed, new_state)


def solution(mesh):
    torus = Mesh(mesh.devices.reshape(8, 4, 4, 2), ("z", "x", "y", "c"))
    return jax.shard_map(
        local,
        mesh=torus,
        in_specs=(
            P(EP, None),
            P(EP, TP, None, None),
            P(),
            P(EP, TP),
            P(EP, TP),
            P(EP, TP),
            P(EP, TP),
            P(TP),
            P(TP),
            P(TP, None),
            P(),
            P(EP, None),
            P(EP, None),
            P(EP, None, TP),
            P(EP, None, TP),
            P(EP, TP, None),
            P(None, TP),
            P(None, TP),
            P(TP, None),
            P(TP, EP),
            P(TP, EP),
            P(EP, TP),
            P(TP),
        ),
        out_specs=(P(EP, TP), P(EP, TP, None, None)),
        check_vma=False,
    )
```

```python
import jax
import jax.numpy as jnp
from jax import lax
from jax.sharding import Mesh
from jax.sharding import PartitionSpec as P

EP = ("z", "x")
TP = ("y", "c")
HUB = ("z", "x", "c")


EPS = 1e-06
BF = jnp.bfloat16
F32 = jnp.float32


def swap(x, axis):
    return lax.all_to_all(x, axis, split_axis=0, concat_axis=0, tiled=True)


def spread(x, axis):
    return swap(jnp.broadcast_to(x, (lax.axis_size(axis), *x.shape)), axis)


def partner(x):
    return lax.ppermute(x, "c", [(0, 1), (1, 0)])


def shift(x, axis, by):
    size = lax.axis_size(axis)
    return lax.ppermute(x, axis, [(i, (i + by) % size) for i in range(size)])


def pick(x, index):
    return lax.dynamic_index_in_dim(x, index, 0, keepdims=False)


def dot(a, b):
    return jnp.dot(a, b, preferred_element_type=F32)


def step(
    tokens,
    state,
    norm_gain,
    w_query,
    w_forget,
    w_input,
    w_outgate,
    lower_bound,
    head_gain,
    w_output,
    ffn_gain,
    route_ids,
    route_weight,
    expert_gate,
    expert_up,
    expert_down,
    shared_gate,
    shared_up,
    shared_down,
    dense_gate,
    dense_up,
    dense_down,
    dense_mix,
):
    nz, nx, ny, nc = (lax.axis_size(a) for a in ("z", "x", "y", "c"))
    x, y, c = (lax.axis_index(a) for a in ("x", "y", "c"))
    seq, width = tokens.shape
    rows_w, chan = w_query.shape
    head_dim = state.shape[2]
    cols = width // (ny * nc)
    own_at = (y * nc + c) * cols

    joined = jnp.concatenate([w_query, w_forget, w_input, w_outgate], axis=1)
    weights = spread(joined, "z").reshape(nz * rows_w, 4 * chan)
    wide = tokens.astype(F32)
    normed = wide * lax.rsqrt(jnp.mean(wide * wide, axis=-1, keepdims=True) + EPS) * norm_gain
    normed = normed.astype(BF).reshape(seq, nz, nx, rows_w)
    normed = jnp.transpose(normed, (2, 0, 1, 3)).reshape(nx, seq, nz * rows_w)
    mine = [pick(normed, x)] + [shift(pick(normed, (x + d) % nx), "x", d) for d in range(1, nx)]
    part = dot(jnp.concatenate(mine, axis=0), weights).astype(BF)
    part = part.reshape(nx, seq, 4 * chan)
    projected = part[0].astype(F32)
    for d in range(1, nx):
        projected = projected + shift(part[d], "x", -d).astype(F32)
    projected = lax.optimization_barrier(projected.astype(BF)).astype(F32)
    query, forget_pre, values, out_gate = jnp.split(projected, 4, axis=1)

    dense_block = jnp.stack([dense_gate, dense_up, dense_down])
    dense_own = jnp.stack([dense_block] + [shift(dense_block, "x", d) for d in range(1, nx)])
    dense_other = partner(dense_own)

    def paired(stack, axis):
        keep = lax.dynamic_index_in_dim(stack, c, 0, keepdims=False)
        other = partner(lax.dynamic_index_in_dim(stack, 1 - c, 0, keepdims=False))
        return jnp.concatenate([keep, other], axis=axis)

    gate_w, up_w, down_w = (
        paired(expert_gate, 1),
        paired(expert_up, 1),
        paired(expert_down, 0),
    )

    def side(stack, index):
        picked = stack[:, index]
        return jnp.moveaxis(picked, 0, 1).reshape(picked.shape[1], -1)

    dense_in_w = jnp.concatenate(
        [
            jnp.concatenate([side(s, 0), side(s, 1)], axis=1)
            for s in (dense_own, dense_other)
        ],
        axis=0,
    )
    dense_out_w = jnp.concatenate(
        [s[:, 2].reshape(-1, cols) for s in (dense_own, dense_other)], axis=1
    )

    forget_sig = jax.nn.sigmoid(forget_pre)
    shape = (seq, 1, head_dim)
    decay = (lower_bound + (1.0 - lower_bound) * forget_sig).reshape(shape)
    keygate = ((1.0 - lower_bound) * (1.0 - forget_sig)).reshape(shape)
    new_state = decay[..., None] * state + keygate[..., None] * values.reshape(shape)[:, :, None, :]
    readout = jnp.einsum("bhk,bhkv->bhv", query.reshape(shape), new_state)
    readout = readout * lax.rsqrt(jnp.mean(readout * readout, axis=-1, keepdims=True) + EPS)
    head_out = (readout.reshape(seq, chan) * head_gain * jax.nn.silu(out_gate)).astype(BF)

    head_part = dot(head_out, w_output).astype(BF)
    head_part = jnp.moveaxis(head_part.reshape(seq, ny, nc, cols), 2, 0)
    head_first, head_second = (jnp.moveaxis(h, 1, 0) for h in (head_part[0], head_part[1]))
    keep = jnp.where(c == 0, head_first, head_second)
    give = jnp.where(c == 0, head_second, head_first)
    pair = (keep.astype(F32) + partner(give).astype(F32)).astype(BF)
    resid = swap(pair, "y").astype(F32).sum(axis=0)
    resid = resid + lax.dynamic_slice_in_dim(tokens, own_at, cols, 1).astype(F32)
    own = resid.astype(BF)

    topk = route_ids.shape[1]
    experts = nz * nx * nc
    cap = max(2, 2 * seq * topk // experts)
    flat_ids = route_ids.reshape(-1)
    onehot = (flat_ids[:, None] == jnp.arange(experts, dtype=jnp.int32)[None, :]).astype(jnp.int32)
    rank = jnp.sum((jnp.cumsum(onehot, axis=0) - onehot) * onehot, axis=1)
    slots = 2 * cap
    slot_index = (flat_ids * slots + rank).reshape(seq, topk)
    slot_ids = jnp.arange(experts * slots, dtype=jnp.int32)
    place = slot_ids % slots
    line = (slot_ids // slots) % (nx * nc) * cap + place - cap
    is_dense = place >= cap
    token_ids = jnp.arange(seq, dtype=jnp.int32)
    dense_hits = is_dense[None, :] & (line[None, :] == token_ids[:, None])
    hits = slot_index[:, :, None] == slot_ids[None, None, :]
    routed_hits = jnp.any(hits, axis=1)
    select = (routed_hits | dense_hits).astype(BF)
    half = cols // 2

    def to_lines(rows):
        rows = rows.reshape(experts, slots, 2, half)
        return jnp.transpose(rows, (0, 2, 1, 3)).reshape(experts, 2 * slots, half)

    def from_lines(lines):
        return jnp.transpose(lines.reshape(experts, 2, slots, half), (0, 2, 1, 3)).reshape(
            experts, slots, cols
        )

    outgoing = jnp.einsum("bs,bw->sw", select, own, preferred_element_type=F32).astype(BF)
    arrived = from_lines(swap(to_lines(outgoing), HUB)).reshape(nz * nx, nc, slots, cols)
    arrived, gate_w, up_w, down_w, dense_in_w, dense_out_w = lax.optimization_barrier(
        (arrived, gate_w, up_w, down_w, dense_in_w, dense_out_w)
    )
    arrived_first, arrived_second = arrived[:, 0], arrived[:, 1]
    count = nz * nx * cap

    routed_rows = jnp.concatenate([arrived_first[:, :cap], arrived_second[:, :cap]], axis=2)
    routed_rows = routed_rows.reshape(count, nc * cols)
    other = partner(own)
    shared_rows = jnp.concatenate(
        [jnp.where(c == 0, own, other), jnp.where(c == 0, other, own)], axis=1
    )
    both = jnp.concatenate([routed_rows, shared_rows], axis=0)
    whole = spread(both, "y")
    whole = jnp.moveaxis(whole, 0, 1).reshape(count + seq, width).astype(F32)
    scale = lax.rsqrt(jnp.mean(whole * whole, axis=-1, keepdims=True) + EPS)
    moe_in = (whole * scale * ffn_gain).astype(BF)

    dense_own_rows = jnp.where(c == 0, arrived_first[:, cap:], arrived_second[:, cap:])
    dense_other_rows = jnp.where(c == 0, arrived_second[:, cap:], arrived_first[:, cap:])
    gain_own = lax.dynamic_slice_in_dim(ffn_gain, own_at, cols, 0)
    gain_other = lax.dynamic_slice_in_dim(ffn_gain, (y * nc + 1 - c) * cols, cols, 0)
    dense_rows = jnp.concatenate([dense_own_rows, dense_other_rows], axis=2)
    dense_rows = dense_rows.reshape(count, nc * cols).astype(F32)
    square = jnp.sum(dense_rows * dense_rows, axis=-1, keepdims=True)
    square_high = square.astype(BF)
    square_low = (square - square_high.astype(F32)).astype(BF)
    dense_scaled = (dense_rows * jnp.concatenate([gain_own, gain_other])).astype(BF)
    dense_pre = dot(dense_scaled, dense_in_w).astype(BF)
    lanes = 128
    dense_pre = jnp.concatenate(
        [
            dense_pre,
            jnp.broadcast_to(square_high, (count, lanes // 2)),
            jnp.broadcast_to(square_low, (count, lanes // 2)),
        ],
        axis=1,
    )
    quarters = dense_pre.reshape(ny, count // ny, -1)
    dense_pre = pick(quarters, y).astype(F32)
    for d in range(1, ny):
        dense_pre = dense_pre + shift(pick(quarters, (y + d) % ny), "y", d).astype(F32)
    hidden_width = dense_in_w.shape[1] // 2
    total = dense_pre[:, 2 * hidden_width] + dense_pre[:, 2 * hidden_width + lanes // 2]
    dense_scale = lax.rsqrt(total / width + EPS)[:, None]
    dense_gate_pre = dense_pre[:, :hidden_width] * dense_scale
    dense_up_pre = dense_pre[:, hidden_width : 2 * hidden_width] * dense_scale
    dense_hidden = (jax.nn.silu(dense_gate_pre) * dense_up_pre).astype(BF)
    dense_hidden = jnp.concatenate(
        [dense_hidden] + [shift(dense_hidden, "y", d) for d in range(1, ny)], axis=0
    )
    dense_part = dot(dense_hidden, dense_out_w).astype(BF).reshape(ny, count // ny, nc * cols)
    dense_part = jnp.stack([pick(dense_part, (y - q) % ny) for q in range(ny)])
    dense_part = dense_part.reshape(nz * nx, cap, nc, cols)
    dense_first = jnp.where(c == 0, dense_part[:, :, 0], dense_part[:, :, 1])
    dense_second = jnp.where(c == 0, dense_part[:, :, 1], dense_part[:, :, 0])

    routed_in, shared_in = moe_in[:count], moe_in[count:]
    hidden = (jax.nn.silu(dot(routed_in, gate_w)) * dot(routed_in, up_w)).astype(BF)
    expert_part = dot(hidden, down_w).astype(BF)
    shared_hidden = (
        jax.nn.silu(dot(shared_in, shared_gate)) * dot(shared_in, shared_up)
    ).astype(BF)
    shared_part = dot(shared_hidden, shared_down).astype(BF)
    parts = jnp.concatenate([expert_part, shared_part], axis=0)
    parts = jnp.moveaxis(parts.reshape(count + seq, ny, nc * cols), 1, 0)
    summed = swap(parts, "y").astype(F32).sum(axis=0)
    expert_out = summed[:count].astype(BF).reshape(nz * nx, cap, nc, cols)
    shared_sum = summed[count:]
    shared_own = jnp.where(c == 0, shared_sum[:, :cols], shared_sum[:, cols:])
    shared_send = jnp.where(c == 0, shared_sum[:, cols:], shared_sum[:, :cols])
    shared_out = shared_own + partner(shared_send.astype(BF)).astype(F32)

    first = jnp.concatenate([expert_out[:, :, 0], dense_first], axis=1)
    second = jnp.concatenate([expert_out[:, :, 1], dense_second], axis=1)
    back = jnp.stack([first, second], axis=1).reshape(experts * slots, cols)
    results = from_lines(swap(to_lines(back), HUB)).reshape(experts * slots, cols)
    combine = jnp.sum(jnp.where(hits, route_weight[:, :, None], F32(0.0)), axis=1)
    routed = dot(combine.astype(BF), results)
    dense_out = dot(dense_hits.astype(BF), results)
    mixed = (resid + routed + shared_out + jax.nn.sigmoid(dense_mix) * dense_out).astype(BF)
    return (mixed, new_state)


def solution(mesh):
    torus = Mesh(mesh.devices.reshape(8, 4, 4, 2), ("z", "x", "y", "c"))
    return jax.shard_map(
        step,
        mesh=torus,
        in_specs=(
            P(EP, None),
            P(EP, TP, None, None),
            P(),
            P(EP, TP),
            P(EP, TP),
            P(EP, TP),
            P(EP, TP),
            P(TP),
            P(TP),
            P(TP, None),
            P(),
            P(EP, None),
            P(EP, None),
            P(EP, None, TP),
            P(EP, None, TP),
            P(EP, TP, None),
            P(None, TP),
            P(None, TP),
            P(TP, None),
            P(TP, EP),
            P(TP, EP),
            P(EP, TP),
            P(TP),
        ),
        out_specs=(P(EP, TP), P(EP, TP, None, None)),
        check_vma=False,
    )
```

```python
import jax
import jax.numpy as jnp
from jax import lax
from jax.experimental import pallas as pl
from jax.experimental.pallas import tpu as pltpu
from jax.sharding import Mesh
from jax.sharding import PartitionSpec as P

EP = ("z", "x")
TP = ("y", "c")
HUB = ("z", "x", "c")


EPS = 1e-06
BF = jnp.bfloat16
F32 = jnp.float32


def swap(x, axis):
    return lax.all_to_all(x, axis, split_axis=0, concat_axis=0, tiled=True)


def spread(x, axis):
    return swap(jnp.broadcast_to(x, (lax.axis_size(axis), *x.shape)), axis)


def partner(x):
    return lax.ppermute(x, "c", [(0, 1), (1, 0)])


def shift(x, axis, by):
    size = lax.axis_size(axis)
    return lax.ppermute(x, axis, [(i, (i + by) % size) for i in range(size)])


def pick(x, index):
    return lax.dynamic_index_in_dim(x, index, 0, keepdims=False)


def dot(a, b):
    return jnp.dot(a, b, preferred_element_type=F32)


def silu(x):
    return x * jax.nn.sigmoid(x)


def call(body, outs, flops, *args):
    moved = sum(a.size * a.dtype.itemsize for a in args) + sum(
        o.size * o.dtype.itemsize for o in outs
    )
    specs = [
        pl.BlockSpec(memory_space=pltpu.SMEM if a.dtype == jnp.int32 and a.ndim == 1 else pltpu.VMEM)
        for a in args
    ]
    return pl.pallas_call(
        body,
        out_shape=outs,
        in_specs=specs,
        out_specs=[pl.BlockSpec(memory_space=pltpu.VMEM) for _ in outs],
        cost_estimate=pl.CostEstimate(flops=flops, bytes_accessed=moved, transcendentals=0),
    )(*args)


def shaped(*dims, dtype=BF):
    return jax.ShapeDtypeStruct(dims, dtype)


def unpack_rows(at, line_of, lines, own, other, both, dense):
    first = at[1] == 0
    group = line_of.shape[1]
    count = dense.shape[1]
    cols = dense.shape[2]
    half = cols // 2
    part = group // 8
    groups = lines.shape[0] // group
    move = jnp.where(
        lax.broadcasted_iota(jnp.int32, (group, group), 0) == line_of[...], 1.0, 0.0
    ).astype(BF)
    mine, others = own[...], other[...]
    both_rows = [
        jnp.where(first, mine, others),
        jnp.where(first, others, mine),
    ]
    for g in range(groups):
        rows = dot(move, lines[g * group : (g + 1) * group, :]).astype(BF)
        here = slice(g * part, (g + 1) * part)
        for side in range(2):
            for h in range(2):
                base = (side * 2 + h) * 2 * part
                at_col = side * cols + h * half
                for copy in range(both.shape[0]):
                    both[copy, here, at_col : at_col + half] = rows[base : base + part]
                dense[side, here, h * half : (h + 1) * half] = rows[base + part : base + 2 * part]
    for side in range(2):
        for copy in range(both.shape[0]):
            both[copy, count:, side * cols : (side + 1) * cols] = both_rows[side]


def dense_first_half(at, rows, gain, *refs):
    y, c = at[0], at[1]
    own_w, other_w, outs = refs[:4], refs[4:8], refs[8:]
    ny = len(outs)
    size = rows.shape[1] // ny
    cols = rows.shape[2]

    def turned(side):
        return jnp.concatenate(
            [
                rows[side, pl.ds(pl.multiple_of(lax.rem(y + d, ny) * size, size), size), :]
                for d in range(ny)
            ],
            axis=0,
        ).astype(F32)

    own, other = turned(c), turned(1 - c)
    square = jnp.sum(own * own + other * other, axis=1, keepdims=True)
    high = square.astype(BF).astype(F32)
    low = square - high
    own = (own * gain[pl.ds(2 * y + c, 1), :]).astype(BF)
    other = (other * gain[pl.ds(2 * y + 1 - c, 1), :]).astype(BF)
    for kind in range(2):
        for i in range(4):
            value = (dot(own, own_w[i][kind]) + dot(other, other_w[i][kind])).astype(BF)
            at_col = (kind * 4 + i) * cols
            for d in range(ny):
                outs[d][:, at_col : at_col + cols] = value[d * size : (d + 1) * size]
    lane = lax.broadcasted_iota(jnp.int32, (square.shape[0], 128), 1)
    both = jnp.where(lane < 64, high, low).astype(BF)
    for d in range(ny):
        outs[d][:, 8 * cols : 8 * cols + 128] = both[d * size : (d + 1) * size]


def dense_activation(a, b, c, d, out):
    width = out.shape[1]
    features = 2048

    def summed(cut):
        return (
            a[:, cut].astype(F32) + b[:, cut].astype(F32) + c[:, cut].astype(F32) + d[:, cut].astype(F32)
        )

    square = summed(slice(2 * width, 2 * width + 128))
    total = square[:, 0:1] + square[:, 64:65]
    scale = lax.rsqrt(total / features + EPS)
    gate = summed(slice(0, width)) * scale
    up = summed(slice(width, 2 * width)) * scale
    out[...] = (silu(gate) * up).astype(BF)


def dense_second_half(at, *refs):
    y = at[0]
    hidden, own_w, other_w, out = refs[:4], refs[4:8], refs[8:12], refs[12]
    ny = len(hidden)
    size, cols = hidden[0].shape[0], out.shape[2]
    rows = jnp.concatenate([h[...] for h in hidden], axis=0)
    for side, weights in enumerate((own_w, other_w)):
        total = None
        for i in range(4):
            term = dot(rows[:, i * cols : (i + 1) * cols], weights[i][2])
            total = term if total is None else total + term
        total = total.astype(BF)
        for d in range(ny):
            start = pl.multiple_of(lax.rem(y + ny - d, ny) * size, size)
            out[side, pl.ds(start, size), :] = total[d * size : (d + 1) * size]


def experts_and_shared(
    at, whole, gain, gate, gate_other, up, up_other, down, down_other,
    shared_gate, shared_up, shared_down, parts,
):
    c = at[1]
    ny, lines, block = whole.shape
    count = lines - 48
    square = jnp.zeros((lines, 1), F32)
    rows = []
    for i in range(ny):
        value = whole[i].astype(F32)
        square = square + jnp.sum(value * value, axis=1, keepdims=True)
        rows.append(value)
    scale = lax.rsqrt(square / (ny * block) + EPS)
    rows = [
        (value * scale * gain[:, i * block : (i + 1) * block]).astype(BF)
        for i, value in enumerate(rows)
    ]
    gate_pre = up_pre = gate_shared = up_shared = None

    def more(total, term):
        return term if total is None else total + term

    for i in range(ny):
        cut = slice(i * block, (i + 1) * block)
        gates = jnp.concatenate([gate[c, cut, :], gate_other[cut, :]], axis=1)
        ups = jnp.concatenate([up[c, cut, :], up_other[cut, :]], axis=1)
        shared = jnp.concatenate([shared_gate[cut, :], shared_up[cut, :]], axis=1)
        gate_pre = more(gate_pre, dot(rows[i][:count], gates))
        up_pre = more(up_pre, dot(rows[i][:count], ups))
        gate_shared = more(gate_shared, dot(rows[i][count:], shared))
    half = gate.shape[2]
    hidden = (silu(gate_pre) * up_pre).astype(BF)
    shared_hidden = (silu(gate_shared[:, :half]) * gate_shared[:, half:]).astype(BF)
    for i in range(ny):
        cut = slice(i * block, (i + 1) * block)
        downs = jnp.concatenate([down[c, :, cut], down_other[:, cut]], axis=0)
        parts[i, :count, :] = dot(hidden, downs).astype(BF)
        parts[i, count:, :] = dot(shared_hidden, shared_down[:, cut]).astype(BF)


def pack_lines(at, line_of, parts, dense, lines, shared_own, shared_send):
    first = at[1] == 0
    group = line_of.shape[0]
    part = group // 8
    cols = dense.shape[2]
    half = cols // 2
    count = dense.shape[1]
    groups = lines.shape[0] // group
    move = jnp.where(
        lax.broadcasted_iota(jnp.int32, (group, group), 1) == line_of[...], 1.0, 0.0
    ).astype(BF)
    total = parts[0].astype(F32)
    for i in range(1, parts.shape[0]):
        total = total + parts[i].astype(F32)
    routed = total[:count].astype(BF)
    shared = total[count:]
    shared_own[...] = jnp.where(first, shared[:, :cols], shared[:, cols:])
    shared_send[...] = jnp.where(first, shared[:, cols:], shared[:, :cols]).astype(BF)
    for g in range(groups):
        here = slice(g * part, (g + 1) * part)
        own, other = dense[0, here, :], dense[1, here, :]
        sides = [jnp.where(first, own, other), jnp.where(first, other, own)]
        stack = []
        for side in range(2):
            for h in range(2):
                at_col = side * cols + h * half
                stack.append(routed[here, at_col : at_col + half])
                stack.append(sides[side][:, h * half : (h + 1) * half])
        rows = jnp.concatenate(stack, axis=0)
        lines[g * group : (g + 1) * group, :] = dot(move, rows).astype(BF)


def step(
    tokens,
    state,
    norm_gain,
    w_query,
    w_forget,
    w_input,
    w_outgate,
    lower_bound,
    head_gain,
    w_output,
    ffn_gain,
    route_ids,
    route_weight,
    expert_gate,
    expert_up,
    expert_down,
    shared_gate,
    shared_up,
    shared_down,
    dense_gate,
    dense_up,
    dense_down,
    dense_mix,
):
    nz, nx, ny, nc = (lax.axis_size(a) for a in ("z", "x", "y", "c"))
    x, y, c = (lax.axis_index(a) for a in ("x", "y", "c"))
    seq, width = tokens.shape
    rows_w, chan = w_query.shape
    head_dim = state.shape[2]
    cols = width // (ny * nc)
    own_at = (y * nc + c) * cols

    joined = jnp.concatenate([w_query, w_forget, w_input, w_outgate], axis=1)
    weights = spread(joined, "z").reshape(nz * rows_w, 4 * chan)
    wide = tokens.astype(F32)
    normed = wide * lax.rsqrt(jnp.mean(wide * wide, axis=-1, keepdims=True) + EPS) * norm_gain
    normed = normed.astype(BF).reshape(seq, nz, nx, rows_w)
    normed = jnp.transpose(normed, (2, 0, 1, 3)).reshape(nx, seq, nz * rows_w)
    mine = [pick(normed, x)] + [shift(pick(normed, (x + d) % nx), "x", d) for d in range(1, nx)]
    part = dot(jnp.concatenate(mine, axis=0), weights).astype(BF)
    part = part.reshape(nx, seq, 4 * chan)
    projected = part[0].astype(F32)
    for d in range(1, nx):
        projected = projected + shift(part[d], "x", -d).astype(F32)
    projected = lax.optimization_barrier(projected.astype(BF)).astype(F32)
    query, forget_pre, values, out_gate = jnp.split(projected, 4, axis=1)

    at = jnp.stack([y, c]).astype(jnp.int32)
    dense_block = jnp.stack([dense_gate, dense_up, dense_down])
    dense_own = [dense_block] + [shift(dense_block, "x", d) for d in range(1, nx)]
    dense_other = [partner(block) for block in dense_own]
    gate_other, up_other, down_other = (
        partner(pick(stack, 1 - c)) for stack in (expert_gate, expert_up, expert_down)
    )

    forget_sig = jax.nn.sigmoid(forget_pre)
    shape = (seq, 1, head_dim)
    decay = (lower_bound + (1.0 - lower_bound) * forget_sig).reshape(shape)
    keygate = ((1.0 - lower_bound) * (1.0 - forget_sig)).reshape(shape)
    new_state = decay[..., None] * state + keygate[..., None] * values.reshape(shape)[:, :, None, :]
    readout = jnp.einsum("bhk,bhkv->bhv", query.reshape(shape), new_state)
    readout = readout * lax.rsqrt(jnp.mean(readout * readout, axis=-1, keepdims=True) + EPS)
    head_out = (readout.reshape(seq, chan) * head_gain * jax.nn.silu(out_gate)).astype(BF)

    head_part = dot(head_out, w_output).astype(BF)
    head_part = jnp.moveaxis(head_part.reshape(seq, ny, nc, cols), 2, 0)
    head_first, head_second = (jnp.moveaxis(h, 1, 0) for h in (head_part[0], head_part[1]))
    keep = jnp.where(c == 0, head_first, head_second)
    give = jnp.where(c == 0, head_second, head_first)
    pair = (keep.astype(F32) + partner(give).astype(F32)).astype(BF)
    resid = swap(pair, "y").astype(F32).sum(axis=0)
    resid = resid + lax.dynamic_slice_in_dim(tokens, own_at, cols, 1).astype(F32)
    own = resid.astype(BF)

    topk = route_ids.shape[1]
    experts = nz * nx * nc
    cap = max(2, 2 * seq * topk // experts)
    flat_ids = route_ids.reshape(-1)
    onehot = (flat_ids[:, None] == jnp.arange(experts, dtype=jnp.int32)[None, :]).astype(jnp.int32)
    rank = jnp.sum((jnp.cumsum(onehot, axis=0) - onehot) * onehot, axis=1)
    slots = 2 * cap
    slot_index = (flat_ids * slots + rank).reshape(seq, topk)
    slot_ids = jnp.arange(experts * slots, dtype=jnp.int32)
    place = slot_ids % slots
    line = (slot_ids // slots) % (nx * nc) * cap + place - cap
    is_dense = place >= cap
    token_ids = jnp.arange(seq, dtype=jnp.int32)
    dense_hits = is_dense[None, :] & (line[None, :] == token_ids[:, None])
    hits = slot_index[:, :, None] == slot_ids[None, None, :]
    routed_hits = jnp.any(hits, axis=1)
    half = cols // 2

    def as_lines(table):
        blocks = table.reshape(seq, experts, slots)
        none = jnp.zeros_like(blocks)
        pair = [jnp.stack([blocks, none], axis=2), jnp.stack([none, blocks], axis=2)]
        return [p.reshape(seq, experts * 2 * slots) for p in pair]

    select = jnp.concatenate(as_lines((routed_hits | dense_hits).astype(BF)), axis=0)
    halves = jnp.concatenate([own[:, :half], own[:, half:]], axis=0)
    outgoing = jnp.einsum("bs,bw->sw", select, halves, preferred_element_type=F32).astype(BF)
    arrived = swap(outgoing.reshape(experts, 2 * slots, half), HUB)
    other = partner(own)
    count = nz * nx * cap

    group = 8 * nc * 2 * slots
    lines = jnp.arange(group, dtype=jnp.int32)
    source, rest = lines // (4 * slots), lines % (4 * slots)
    side, h, kind, r = (
        rest // (2 * slots),
        rest // slots % 2,
        rest // cap % 2,
        rest % cap,
    )
    line_of = ((side * 2 + h) * 2 + kind) * (8 * cap) + source * cap + r
    both, dense_rows = call(
        unpack_rows,
        [shaped(ny, count + seq, nc * cols), shaped(nc, count, cols)],
        4 * 2 * group * group * half,
        at,
        line_of.reshape(1, group),
        arrived.reshape(-1, half),
        own,
        other,
    )
    whole = swap(both, "y")

    hidden_width = nx * dense_gate.shape[1]
    quarter = count // ny
    pre = call(
        dense_first_half,
        [shaped(quarter, 2 * hidden_width + 128)] * ny,
        2 * count * nc * cols * 2 * hidden_width,
        at,
        dense_rows,
        ffn_gain.reshape(ny * nc, cols),
        *dense_own,
        *dense_other,
    )
    pre = [pre[0]] + [shift(pre[d], "y", d) for d in range(1, ny)]
    (hidden,) = call(dense_activation, [shaped(quarter, hidden_width)], 10**6, *pre)
    hidden = [hidden] + [shift(hidden, "y", d) for d in range(1, ny)]
    (dense_part,) = call(
        dense_second_half,
        [shaped(nc, count, cols)],
        2 * count * nc * cols * hidden_width,
        at,
        *hidden,
        *dense_own,
        *dense_other,
    )

    (parts,) = call(
        experts_and_shared,
        [shaped(ny, count + seq, nc * cols)],
        2 * 3 * (count * 2 + seq) * width * expert_gate.shape[2],
        at,
        whole,
        ffn_gain.reshape(1, width),
        expert_gate,
        gate_other,
        expert_up,
        up_other,
        expert_down,
        down_other,
        shared_gate,
        shared_up,
        shared_down,
    )
    parts = swap(parts, "y")
    back, shared_own, shared_send = call(
        pack_lines,
        [
            shaped(experts * 2 * slots, half),
            shaped(seq, cols, dtype=F32),
            shaped(seq, cols),
        ],
        4 * 2 * group * group * half,
        at,
        line_of.reshape(group, 1),
        parts,
        dense_part,
    )

    results = swap(back.reshape(experts, 2 * slots, half), HUB)
    results = results.reshape(experts * 2 * slots, half)
    shared_out = shared_own + partner(shared_send).astype(F32)
    combine = jnp.sum(jnp.where(hits, route_weight[:, :, None], F32(0.0)), axis=1)
    sums = jnp.concatenate(
        as_lines(combine.astype(BF)) + as_lines(dense_hits.astype(BF)), axis=0
    )
    sums = dot(sums, results).reshape(2, 2, seq, half)
    routed = jnp.concatenate([sums[0, 0], sums[0, 1]], axis=1)
    dense_out = jnp.concatenate([sums[1, 0], sums[1, 1]], axis=1)
    mixed = (resid + routed + shared_out + jax.nn.sigmoid(dense_mix) * dense_out).astype(BF)
    return (mixed, new_state)


def solution(mesh):
    torus = Mesh(mesh.devices.reshape(8, 4, 4, 2), ("z", "x", "y", "c"))
    return jax.shard_map(
        step,
        mesh=torus,
        in_specs=(
            P(EP, None),
            P(EP, TP, None, None),
            P(),
            P(EP, TP),
            P(EP, TP),
            P(EP, TP),
            P(EP, TP),
            P(TP),
            P(TP),
            P(TP, None),
            P(),
            P(EP, None),
            P(EP, None),
            P(EP, None, TP),
            P(EP, None, TP),
            P(EP, TP, None),
            P(None, TP),
            P(None, TP),
            P(TP, None),
            P(TP, EP),
            P(TP, EP),
            P(EP, TP),
            P(TP),
        ),
        out_specs=(P(EP, TP), P(EP, TP, None, None)),
        check_vma=False,
    )
```

```python
import jax
import jax.numpy as jnp
from jax import lax
from jax.experimental import pallas as pl
from jax.experimental.pallas import tpu as pltpu
from jax.sharding import Mesh
from jax.sharding import PartitionSpec as P

EP = ("z", "x")
TP = ("y", "c")
HUB = ("z", "x", "c")


EPS = 1e-06
BF = jnp.bfloat16
F32 = jnp.float32


def swap(x, axis):
    return lax.all_to_all(x, axis, split_axis=0, concat_axis=0, tiled=True)


def spread(x, axis):
    return swap(jnp.broadcast_to(x, (lax.axis_size(axis), *x.shape)), axis)


def partner(x):
    return lax.ppermute(x, "c", [(0, 1), (1, 0)])


def shift(x, axis, by):
    size = lax.axis_size(axis)
    return lax.ppermute(x, axis, [(i, (i + by) % size) for i in range(size)])


def pick(x, index):
    return lax.dynamic_index_in_dim(x, index, 0, keepdims=False)


def dot(a, b):
    return jnp.dot(a, b, preferred_element_type=F32)


def silu(x):
    return x * jax.nn.sigmoid(x)


def call(body, outs, flops, *args, mib=12):
    moved = sum(a.size * a.dtype.itemsize for a in args) + sum(
        o.size * o.dtype.itemsize for o in outs
    )
    specs = [
        pl.BlockSpec(memory_space=pltpu.SMEM if a.dtype == jnp.int32 and a.ndim == 1 else pltpu.VMEM)
        for a in args
    ]
    return pl.pallas_call(
        body,
        out_shape=outs,
        in_specs=specs,
        out_specs=[pl.BlockSpec(memory_space=pltpu.VMEM) for _ in outs],
        cost_estimate=pl.CostEstimate(flops=flops, bytes_accessed=moved, transcendentals=0),
        compiler_params=pltpu.CompilerParams(vmem_limit_bytes=mib * 2**20),
    )(*args)


def shaped(*dims, dtype=BF):
    return jax.ShapeDtypeStruct(dims, dtype)


def unpack_rows(at, line_of, lines, own, other, both, dense):
    first = at[1] == 0
    group = line_of.shape[1]
    count = dense.shape[1]
    cols = dense.shape[2]
    half = cols // 2
    part = group // 8
    groups = lines.shape[0] // group
    move = jnp.where(
        lax.broadcasted_iota(jnp.int32, (group, group), 0) == line_of[...], 1.0, 0.0
    ).astype(BF)
    mine, others = own[...], other[...]
    both_rows = [
        jnp.where(first, mine, others),
        jnp.where(first, others, mine),
    ]
    for g in range(groups):
        rows = dot(move, lines[g * group : (g + 1) * group, :]).astype(BF)
        here = slice(g * part, (g + 1) * part)
        for side in range(2):
            for h in range(2):
                base = (side * 2 + h) * 2 * part
                at_col = side * cols + h * half
                for copy in range(both.shape[0]):
                    both[copy, here, at_col : at_col + half] = rows[base : base + part]
                dense[side, here, h * half : (h + 1) * half] = rows[base + part : base + 2 * part]
    for side in range(2):
        for copy in range(both.shape[0]):
            both[copy, count:, side * cols : (side + 1) * cols] = both_rows[side]


def dense_first_half(at, rows, gain, *refs):
    y, c = at[0], at[1]
    own_w, other_w, outs = refs[:4], refs[4:8], refs[8:]
    ny = len(outs)
    size = rows.shape[1] // ny
    cols = rows.shape[2]

    def turned(side):
        return jnp.concatenate(
            [
                rows[side, pl.ds(pl.multiple_of(lax.rem(y + d, ny) * size, size), size), :]
                for d in range(ny)
            ],
            axis=0,
        ).astype(F32)

    own, other = turned(c), turned(1 - c)
    square = jnp.sum(own * own + other * other, axis=1, keepdims=True)
    high = square.astype(BF).astype(F32)
    low = square - high
    own = (own * gain[pl.ds(2 * y + c, 1), :]).astype(BF)
    other = (other * gain[pl.ds(2 * y + 1 - c, 1), :]).astype(BF)
    for kind in range(2):
        for i in range(4):
            value = (dot(own, own_w[i][kind]) + dot(other, other_w[i][kind])).astype(BF)
            at_col = (kind * 4 + i) * cols
            for d in range(ny):
                outs[d][:, at_col : at_col + cols] = value[d * size : (d + 1) * size]
    lane = lax.broadcasted_iota(jnp.int32, (square.shape[0], 128), 1)
    both = jnp.where(lane < 64, high, low).astype(BF)
    for d in range(ny):
        outs[d][:, 8 * cols : 8 * cols + 128] = both[d * size : (d + 1) * size]


def dense_activation(a, b, c, d, out):
    width = out.shape[1]
    features = 2048

    def summed(cut):
        return (
            a[:, cut].astype(F32) + b[:, cut].astype(F32) + c[:, cut].astype(F32) + d[:, cut].astype(F32)
        )

    square = summed(slice(2 * width, 2 * width + 128))
    total = square[:, 0:1] + square[:, 64:65]
    scale = lax.rsqrt(total / features + EPS)
    gate = summed(slice(0, width)) * scale
    up = summed(slice(width, 2 * width)) * scale
    out[...] = (silu(gate) * up).astype(BF)


def dense_second_half(at, *refs):
    y = at[0]
    hidden, own_w, other_w, out = refs[:4], refs[4:8], refs[8:12], refs[12]
    ny = len(hidden)
    size, cols = hidden[0].shape[0], out.shape[2]
    rows = jnp.concatenate([h[...] for h in hidden], axis=0)
    for side, weights in enumerate((own_w, other_w)):
        total = None
        for i in range(4):
            term = dot(rows[:, i * cols : (i + 1) * cols], weights[i][2])
            total = term if total is None else total + term
        total = total.astype(BF)
        for d in range(ny):
            start = pl.multiple_of(lax.rem(y + ny - d, ny) * size, size)
            out[side, pl.ds(start, size), :] = total[d * size : (d + 1) * size]


def experts_and_shared(
    at, whole, gain, gate, gate_other, up, up_other, down, down_other,
    shared_gate, shared_up, shared_down, parts,
):
    c = at[1]
    ny, lines, block = whole.shape
    count = lines - 48
    square = jnp.zeros((lines, 1), F32)
    rows = []
    for i in range(ny):
        value = whole[i].astype(F32)
        square = square + jnp.sum(value * value, axis=1, keepdims=True)
        rows.append(value)
    scale = lax.rsqrt(square / (ny * block) + EPS)
    rows = [
        (value * scale * gain[:, i * block : (i + 1) * block]).astype(BF)
        for i, value in enumerate(rows)
    ]
    gate_pre = up_pre = gate_shared = up_shared = None

    def more(total, term):
        return term if total is None else total + term

    for i in range(ny):
        cut = slice(i * block, (i + 1) * block)
        gates = jnp.concatenate([gate[c, cut, :], gate_other[cut, :]], axis=1)
        ups = jnp.concatenate([up[c, cut, :], up_other[cut, :]], axis=1)
        shared = jnp.concatenate([shared_gate[cut, :], shared_up[cut, :]], axis=1)
        gate_pre = more(gate_pre, dot(rows[i][:count], gates))
        up_pre = more(up_pre, dot(rows[i][:count], ups))
        gate_shared = more(gate_shared, dot(rows[i][count:], shared))
    half = gate.shape[2]
    hidden = (silu(gate_pre) * up_pre).astype(BF)
    shared_hidden = (silu(gate_shared[:, :half]) * gate_shared[:, half:]).astype(BF)
    for i in range(ny):
        cut = slice(i * block, (i + 1) * block)
        downs = jnp.concatenate([down[c, :, cut], down_other[:, cut]], axis=0)
        parts[i, :count, :] = dot(hidden, downs).astype(BF)
        parts[i, count:, :] = dot(shared_hidden, shared_down[:, cut]).astype(BF)


def pack_lines(at, line_of, parts, dense, lines, shared_own, shared_send):
    first = at[1] == 0
    group = line_of.shape[0]
    part = group // 8
    cols = dense.shape[2]
    half = cols // 2
    count = dense.shape[1]
    groups = lines.shape[0] // group
    move = jnp.where(
        lax.broadcasted_iota(jnp.int32, (group, group), 1) == line_of[...], 1.0, 0.0
    ).astype(BF)
    total = parts[0].astype(F32)
    for i in range(1, parts.shape[0]):
        total = total + parts[i].astype(F32)
    routed = total[:count].astype(BF)
    shared = total[count:]
    shared_own[...] = jnp.where(first, shared[:, :cols], shared[:, cols:])
    shared_send[...] = jnp.where(first, shared[:, cols:], shared[:, :cols]).astype(BF)
    for g in range(groups):
        here = slice(g * part, (g + 1) * part)
        own, other = dense[0, here, :], dense[1, here, :]
        sides = [jnp.where(first, own, other), jnp.where(first, other, own)]
        stack = []
        for side in range(2):
            for h in range(2):
                at_col = side * cols + h * half
                stack.append(routed[here, at_col : at_col + half])
                stack.append(sides[side][:, h * half : (h + 1) * half])
        rows = jnp.concatenate(stack, axis=0)
        lines[g * group : (g + 1) * group, :] = dot(move, rows).astype(BF)


def step(
    tokens,
    state,
    norm_gain,
    w_query,
    w_forget,
    w_input,
    w_outgate,
    lower_bound,
    head_gain,
    w_output,
    ffn_gain,
    route_ids,
    route_weight,
    expert_gate,
    expert_up,
    expert_down,
    shared_gate,
    shared_up,
    shared_down,
    dense_gate,
    dense_up,
    dense_down,
    dense_mix,
):
    nz, nx, ny, nc = (lax.axis_size(a) for a in ("z", "x", "y", "c"))
    x, y, c = (lax.axis_index(a) for a in ("x", "y", "c"))
    seq, width = tokens.shape
    rows_w, chan = w_query.shape
    head_dim = state.shape[2]
    cols = width // (ny * nc)
    own_at = (y * nc + c) * cols

    joined = jnp.concatenate([w_query, w_forget, w_input, w_outgate], axis=1)
    weights = spread(joined, "z").reshape(nz * rows_w, 4 * chan)
    wide = tokens.astype(F32)
    normed = wide * lax.rsqrt(jnp.mean(wide * wide, axis=-1, keepdims=True) + EPS) * norm_gain
    normed = normed.astype(BF).reshape(seq, nz, nx, rows_w)
    normed = jnp.transpose(normed, (2, 0, 1, 3)).reshape(nx, seq, nz * rows_w)
    mine = [pick(normed, x)] + [shift(pick(normed, (x + d) % nx), "x", d) for d in range(1, nx)]
    part = dot(jnp.concatenate(mine, axis=0), weights).astype(BF)
    part = part.reshape(nx, seq, 4 * chan)
    projected = part[0].astype(F32)
    for d in range(1, nx):
        projected = projected + shift(part[d], "x", -d).astype(F32)
    projected = projected.astype(BF).astype(F32)
    query, forget_pre, values, out_gate = jnp.split(projected, 4, axis=1)

    at = jnp.stack([y, c]).astype(jnp.int32)
    dense_block = jnp.stack([dense_gate, dense_up, dense_down])
    dense_own = [dense_block] + [shift(dense_block, "x", d) for d in range(1, nx)]
    dense_other = [partner(block) for block in dense_own]
    gate_other, up_other, down_other = (
        partner(pick(stack, 1 - c)) for stack in (expert_gate, expert_up, expert_down)
    )

    forget_sig = jax.nn.sigmoid(forget_pre)
    shape = (seq, 1, head_dim)
    decay = (lower_bound + (1.0 - lower_bound) * forget_sig).reshape(shape)
    keygate = ((1.0 - lower_bound) * (1.0 - forget_sig)).reshape(shape)
    new_state = decay[..., None] * state + keygate[..., None] * values.reshape(shape)[:, :, None, :]
    readout = jnp.einsum("bhk,bhkv->bhv", query.reshape(shape), new_state)
    readout = readout * lax.rsqrt(jnp.mean(readout * readout, axis=-1, keepdims=True) + EPS)
    head_out = (readout.reshape(seq, chan) * head_gain * jax.nn.silu(out_gate)).astype(BF)

    head_part = dot(head_out, w_output).astype(BF)
    head_part = jnp.moveaxis(head_part.reshape(seq, ny, nc, cols), 2, 0)
    head_first, head_second = (jnp.moveaxis(h, 1, 0) for h in (head_part[0], head_part[1]))
    keep = jnp.where(c == 0, head_first, head_second)
    give = jnp.where(c == 0, head_second, head_first)
    pair = (keep.astype(F32) + partner(give).astype(F32)).astype(BF)
    resid = swap(pair, "y").astype(F32).sum(axis=0)
    resid = resid + lax.dynamic_slice_in_dim(tokens, own_at, cols, 1).astype(F32)
    own = resid.astype(BF)

    topk = route_ids.shape[1]
    experts = nz * nx * nc
    cap = max(2, 2 * seq * topk // experts)
    flat_ids = route_ids.reshape(-1)
    onehot = (flat_ids[:, None] == jnp.arange(experts, dtype=jnp.int32)[None, :]).astype(jnp.int32)
    rank = jnp.sum((jnp.cumsum(onehot, axis=0) - onehot) * onehot, axis=1)
    slots = 2 * cap
    slot_index = (flat_ids * slots + rank).reshape(seq, topk)
    slot_ids = jnp.arange(experts * slots, dtype=jnp.int32)
    place = slot_ids % slots
    line = (slot_ids // slots) % (nx * nc) * cap + place - cap
    is_dense = place >= cap
    token_ids = jnp.arange(seq, dtype=jnp.int32)
    dense_hits = is_dense[None, :] & (line[None, :] == token_ids[:, None])
    hits = slot_index[:, :, None] == slot_ids[None, None, :]
    routed_hits = jnp.any(hits, axis=1)
    half = cols // 2

    def as_lines(table):
        blocks = table.reshape(seq, experts, slots)
        none = jnp.zeros_like(blocks)
        pair = [jnp.stack([blocks, none], axis=2), jnp.stack([none, blocks], axis=2)]
        return [p.reshape(seq, experts * 2 * slots) for p in pair]

    select = jnp.concatenate(as_lines((routed_hits | dense_hits).astype(BF)), axis=0)
    halves = jnp.concatenate([own[:, :half], own[:, half:]], axis=0)
    outgoing = jnp.einsum("bs,bw->sw", select, halves, preferred_element_type=F32).astype(BF)
    arrived = swap(outgoing.reshape(experts, 2 * slots, half), HUB)
    other = partner(own)
    count = nz * nx * cap

    group = 8 * nc * 2 * slots
    lines = jnp.arange(group, dtype=jnp.int32)
    source, rest = lines // (4 * slots), lines % (4 * slots)
    side, h, kind, r = (
        rest // (2 * slots),
        rest // slots % 2,
        rest // cap % 2,
        rest % cap,
    )
    line_of = ((side * 2 + h) * 2 + kind) * (8 * cap) + source * cap + r
    both, dense_rows = call(
        unpack_rows,
        [shaped(ny, count + seq, nc * cols), shaped(nc, count, cols)],
        4 * 2 * group * group * half,
        at,
        line_of.reshape(1, group),
        arrived.reshape(-1, half),
        own,
        other,
        mib=60,
    )
    whole = swap(both, "y")

    hidden_width = nx * dense_gate.shape[1]
    quarter = count // ny
    pre = call(
        dense_first_half,
        [shaped(quarter, 2 * hidden_width + 128)] * ny,
        2 * count * nc * cols * 2 * hidden_width,
        at,
        dense_rows,
        ffn_gain.reshape(ny * nc, cols),
        *dense_own,
        *dense_other,
    )
    pre = [pre[0]] + [shift(pre[d], "y", d) for d in range(1, ny)]
    (hidden,) = call(dense_activation, [shaped(quarter, hidden_width)], 10**6, *pre)
    hidden = [hidden] + [shift(hidden, "y", d) for d in range(1, ny)]
    (dense_part,) = call(
        dense_second_half,
        [shaped(nc, count, cols)],
        2 * count * nc * cols * hidden_width,
        at,
        *hidden,
        *dense_own,
        *dense_other,
    )

    (parts,) = call(
        experts_and_shared,
        [shaped(ny, count + seq, nc * cols)],
        2 * 3 * (count * 2 + seq) * width * expert_gate.shape[2],
        at,
        whole,
        ffn_gain.reshape(1, width),
        expert_gate,
        gate_other,
        expert_up,
        up_other,
        expert_down,
        down_other,
        shared_gate,
        shared_up,
        shared_down,
        mib=24,
    )
    parts = swap(parts, "y")
    back, shared_own, shared_send = call(
        pack_lines,
        [
            shaped(experts * 2 * slots, half),
            shaped(seq, cols, dtype=F32),
            shaped(seq, cols),
        ],
        4 * 2 * group * group * half,
        at,
        line_of.reshape(group, 1),
        parts,
        dense_part,
    )

    results = swap(back.reshape(experts, 2 * slots, half), HUB)
    results = results.reshape(experts * 2 * slots, half)
    shared_out = shared_own + partner(shared_send).astype(F32)
    combine = jnp.sum(jnp.where(hits, route_weight[:, :, None], F32(0.0)), axis=1)
    sums = jnp.concatenate(
        as_lines(combine.astype(BF)) + as_lines(dense_hits.astype(BF)), axis=0
    )
    sums = dot(sums, results).reshape(2, 2, seq, half)
    routed = jnp.concatenate([sums[0, 0], sums[0, 1]], axis=1)
    dense_out = jnp.concatenate([sums[1, 0], sums[1, 1]], axis=1)
    mixed = (resid + routed + shared_out + jax.nn.sigmoid(dense_mix) * dense_out).astype(BF)
    return (mixed, new_state)


def solution(mesh):
    torus = Mesh(mesh.devices.reshape(8, 4, 4, 2), ("z", "x", "y", "c"))
    return jax.shard_map(
        step,
        mesh=torus,
        in_specs=(
            P(EP, None),
            P(EP, TP, None, None),
            P(),
            P(EP, TP),
            P(EP, TP),
            P(EP, TP),
            P(EP, TP),
            P(TP),
            P(TP),
            P(TP, None),
            P(),
            P(EP, None),
            P(EP, None),
            P(EP, None, TP),
            P(EP, None, TP),
            P(EP, TP, None),
            P(None, TP),
            P(None, TP),
            P(TP, None),
            P(TP, EP),
            P(TP, EP),
            P(EP, TP),
            P(TP),
        ),
        out_specs=(P(EP, TP), P(EP, TP, None, None)),
        check_vma=False,
    )
```

```python
import jax
import jax.numpy as jnp
from jax import lax
from jax.experimental import pallas as pl
from jax.experimental.pallas import tpu as pltpu
from jax.sharding import Mesh
from jax.sharding import PartitionSpec as P

EP = ("z", "x")
TP = ("y", "c")
HUB = ("z", "x", "c")


EPS = 1e-06
BF = jnp.bfloat16
F32 = jnp.float32


def swap(x, axis):
    return lax.all_to_all(x, axis, split_axis=0, concat_axis=0, tiled=True)


def partner(x):
    return lax.ppermute(x, "c", [(0, 1), (1, 0)])


def shift(x, axis, by):
    size = lax.axis_size(axis)
    return lax.ppermute(x, axis, [(i, (i + by) % size) for i in range(size)])


def pick(x, index):
    return lax.dynamic_index_in_dim(x, index, 0, keepdims=False)


def dot(a, b):
    return jnp.dot(a, b, preferred_element_type=F32)


def silu(x):
    return x * jax.nn.sigmoid(x)


def call(body, outs, flops, *args, mib=12, scratch=()):
    moved = sum(a.size * a.dtype.itemsize for a in args) + sum(
        o.size * o.dtype.itemsize for o in outs
    )
    specs = [
        pl.BlockSpec(memory_space=pltpu.SMEM if a.dtype == jnp.int32 and a.ndim == 1 else pltpu.VMEM)
        for a in args
    ]
    return pl.pallas_call(
        body,
        out_shape=outs,
        in_specs=specs,
        out_specs=[pl.BlockSpec(memory_space=pltpu.VMEM) for _ in outs],
        scratch_shapes=scratch,
        cost_estimate=pl.CostEstimate(flops=flops, bytes_accessed=moved, transcendentals=0),
        compiler_params=pltpu.CompilerParams(vmem_limit_bytes=mib * 2**20),
    )(*args)


def shaped(*dims, dtype=BF):
    return jax.ShapeDtypeStruct(dims, dtype)


def prepare(at, tokens, gain, wq, wf, wi, wo, dg, du, dd, spread_w, dense, t0, t1, t2, t3, held):
    x = at[2]
    for i, block in enumerate((dg, du, dd)):
        dense[i] = block[...]
    for i, block in enumerate((wq, wf, wi, wo)):
        width = block.shape[1]
        value = block[...]
        for z in range(spread_w.shape[0]):
            spread_w[z, :, i * width : (i + 1) * width] = value
    wide = tokens[...].astype(F32)
    wide = wide * lax.rsqrt(jnp.mean(wide * wide, axis=1, keepdims=True) + EPS) * gain[...]
    low = lax.broadcasted_iota(jnp.int32, (wide.shape[0], 128), 1) < 64

    def tile(i):
        return wide[:, i * 128 : (i + 1) * 128]

    for to in range(4):
        for k in range(4):
            a, b = tile(4 * k + to // 2), tile(4 * k + 2 + to // 2)
            if to % 2 == 0:
                value = jnp.where(low, a, pltpu.roll(b, 64, 1))
            else:
                value = jnp.where(low, pltpu.roll(a, 64, 1), b)
            held[to, :, k * 128 : (k + 1) * 128] = value.astype(BF)
    for d, out in enumerate((t0, t1, t2, t3)):
        out[...] = held[lax.rem(x + d, 4)]


def recur(at, p0, p1, p2, p3, bound, gain, state, w_out, decay_out, key_out, value_out, keep, give, read):
    first = at[1] == 0
    seq = p0.shape[0]
    total = (
        p0[...].astype(F32) + p1[...].astype(F32) + p2[...].astype(F32) + p3[...].astype(F32)
    )
    total = total.astype(BF).astype(F32)
    query, forget, values, gate = (total[:, i * 128 : (i + 1) * 128] for i in range(4))
    forget = jax.nn.sigmoid(forget)
    low = bound[...]
    decay = low + (1.0 - low) * forget
    key = (1.0 - low) * (1.0 - forget)
    decay_out[...] = decay
    key_out[...] = key
    value_out[...] = values
    turned = jnp.transpose(query * decay)
    for b in range(seq):
        read[b : b + 1, :] = jnp.sum(turned[:, b : b + 1] * state[b], axis=0, keepdims=True)
    readout = read[...] + jnp.sum(query * key, axis=1, keepdims=True) * values
    readout = readout * lax.rsqrt(jnp.mean(readout * readout, axis=1, keepdims=True) + EPS)
    head = (readout * gain[...] * silu(gate)).astype(BF)
    cols = keep.shape[2]
    for y in range(keep.shape[0]):
        cut = slice(2 * y * cols, (2 * y + 1) * cols)
        cut_next = slice((2 * y + 1) * cols, (2 * y + 2) * cols)
        even = dot(head, w_out[:, cut]).astype(BF)
        odd = dot(head, w_out[:, cut_next]).astype(BF)
        keep[y] = jnp.where(first, even, odd)
        give[y] = jnp.where(first, odd, even)


def dispatch(at, heads, tokens, slots, resid, own, lines):
    cols = resid.shape[1]
    half = cols // 2
    seq = resid.shape[0]
    start = pl.multiple_of((2 * at[0] + at[1]) * cols, cols)
    total = tokens[:, pl.ds(start, cols)].astype(F32)
    for i in range(heads.shape[0]):
        total = total + heads[i].astype(F32)
    resid[...] = total
    rows = total.astype(BF)
    own[...] = rows
    chunk = 192
    place = lax.broadcasted_iota(jnp.int32, (chunk, seq), 0)
    for h in range(2):
        shifted = place - 12 * h
        dense = shifted == slots[4:5, :]
        for z in range(lines.shape[0] // chunk):
            here = shifted + z * chunk
            hit = dense
            for k in range(4):
                hit = hit | (here == slots[k : k + 1, :])
            part = dot(jnp.where(hit, 1.0, 0.0).astype(BF), rows[:, h * half : (h + 1) * half])
            if h == 0:
                lines[z * chunk : (z + 1) * chunk, :] = part.astype(BF)
            else:
                before = lines[z * chunk : (z + 1) * chunk, :].astype(F32)
                lines[z * chunk : (z + 1) * chunk, :] = (before + part).astype(BF)


def finish(lines, within, slots, weight, resid, shared, shared_other, mix, out):
    seq, cols = out.shape
    half = cols // 2
    place = lax.broadcasted_iota(jnp.int32, (seq, lines.shape[0]), 1)
    gate = jax.nn.sigmoid(mix[...])
    base = resid[...] + shared[...] + shared_other[...].astype(F32)
    for h in range(2):
        routed = jnp.zeros(place.shape, F32)
        for k in range(4):
            routed = jnp.where(place == slots[:, k : k + 1] + 12 * h, weight[:, k : k + 1], routed)
        dense = jnp.where(within[...] == slots[:, 4:5] + 12 * h, 1.0, 0.0)
        cut = slice(h * half, (h + 1) * half)
        total = base[:, cut] + dot(routed.astype(BF), lines[...])
        total = total + gate[:, cut] * dot(dense.astype(BF), lines[...])
        out[:, cut] = total.astype(BF)


def unpack_rows(at, line_of, lines, own, other, both, dense):
    first = at[1] == 0
    group = line_of.shape[1]
    count = dense.shape[1]
    cols = dense.shape[2]
    half = cols // 2
    part = group // 8
    groups = lines.shape[0] // group
    move = jnp.where(
        lax.broadcasted_iota(jnp.int32, (group, group), 0) == line_of[...], 1.0, 0.0
    ).astype(BF)
    mine, others = own[...], other[...]
    both_rows = [
        jnp.where(first, mine, others),
        jnp.where(first, others, mine),
    ]
    for g in range(groups):
        rows = dot(move, lines[g * group : (g + 1) * group, :]).astype(BF)
        here = slice(g * part, (g + 1) * part)
        for side in range(2):
            for h in range(2):
                base = (side * 2 + h) * 2 * part
                at_col = side * cols + h * half
                for copy in range(both.shape[0]):
                    both[copy, here, at_col : at_col + half] = rows[base : base + part]
                dense[side, here, h * half : (h + 1) * half] = rows[base + part : base + 2 * part]
    for side in range(2):
        for copy in range(both.shape[0]):
            both[copy, count:, side * cols : (side + 1) * cols] = both_rows[side]


def dense_first_half(at, rows, gain, *refs):
    y, c = at[0], at[1]
    own_w, other_w, outs = refs[:4], refs[4:8], refs[8:]
    ny = len(outs)
    size = rows.shape[1] // ny
    cols = rows.shape[2]

    def turned(side):
        return jnp.concatenate(
            [
                rows[side, pl.ds(pl.multiple_of(lax.rem(y + d, ny) * size, size), size), :]
                for d in range(ny)
            ],
            axis=0,
        ).astype(F32)

    own, other = turned(c), turned(1 - c)
    square = jnp.sum(own * own + other * other, axis=1, keepdims=True)
    high = square.astype(BF).astype(F32)
    low = square - high
    own = (own * gain[pl.ds(2 * y + c, 1), :]).astype(BF)
    other = (other * gain[pl.ds(2 * y + 1 - c, 1), :]).astype(BF)
    for kind in range(2):
        for i in range(4):
            value = (dot(own, own_w[i][kind]) + dot(other, other_w[i][kind])).astype(BF)
            at_col = (kind * 4 + i) * cols
            for d in range(ny):
                outs[d][:, at_col : at_col + cols] = value[d * size : (d + 1) * size]
    lane = lax.broadcasted_iota(jnp.int32, (square.shape[0], 128), 1)
    both = jnp.where(lane < 64, high, low).astype(BF)
    for d in range(ny):
        outs[d][:, 8 * cols : 8 * cols + 128] = both[d * size : (d + 1) * size]


def dense_activation(a, b, c, d, out):
    width = out.shape[1]
    features = 2048

    def summed(cut):
        return (
            a[:, cut].astype(F32) + b[:, cut].astype(F32) + c[:, cut].astype(F32) + d[:, cut].astype(F32)
        )

    square = summed(slice(2 * width, 2 * width + 128))
    total = square[:, 0:1] + square[:, 64:65]
    scale = lax.rsqrt(total / features + EPS)
    gate = summed(slice(0, width)) * scale
    up = summed(slice(width, 2 * width)) * scale
    out[...] = (silu(gate) * up).astype(BF)


def dense_second_half(at, *refs):
    y = at[0]
    hidden, own_w, other_w, out = refs[:4], refs[4:8], refs[8:12], refs[12]
    ny = len(hidden)
    size, cols = hidden[0].shape[0], out.shape[2]
    rows = jnp.concatenate([h[...] for h in hidden], axis=0)
    for side, weights in enumerate((own_w, other_w)):
        total = None
        for i in range(4):
            term = dot(rows[:, i * cols : (i + 1) * cols], weights[i][2])
            total = term if total is None else total + term
        total = total.astype(BF)
        for d in range(ny):
            start = pl.multiple_of(lax.rem(y + ny - d, ny) * size, size)
            out[side, pl.ds(start, size), :] = total[d * size : (d + 1) * size]


def experts_and_shared(
    at, whole, gain, gate, gate_other, up, up_other, down, down_other,
    shared_gate, shared_up, shared_down, parts,
):
    c = at[1]
    ny, lines, block = whole.shape
    count = lines - 48
    square = jnp.zeros((lines, 1), F32)
    rows = []
    for i in range(ny):
        value = whole[i].astype(F32)
        square = square + jnp.sum(value * value, axis=1, keepdims=True)
        rows.append(value)
    scale = lax.rsqrt(square / (ny * block) + EPS)
    rows = [
        (value * scale * gain[:, i * block : (i + 1) * block]).astype(BF)
        for i, value in enumerate(rows)
    ]
    gate_pre = up_pre = gate_shared = up_shared = None

    def more(total, term):
        return term if total is None else total + term

    for i in range(ny):
        cut = slice(i * block, (i + 1) * block)
        gates = jnp.concatenate([gate[c, cut, :], gate_other[cut, :]], axis=1)
        ups = jnp.concatenate([up[c, cut, :], up_other[cut, :]], axis=1)
        shared = jnp.concatenate([shared_gate[cut, :], shared_up[cut, :]], axis=1)
        gate_pre = more(gate_pre, dot(rows[i][:count], gates))
        up_pre = more(up_pre, dot(rows[i][:count], ups))
        gate_shared = more(gate_shared, dot(rows[i][count:], shared))
    half = gate.shape[2]
    hidden = (silu(gate_pre) * up_pre).astype(BF)
    shared_hidden = (silu(gate_shared[:, :half]) * gate_shared[:, half:]).astype(BF)
    for i in range(ny):
        cut = slice(i * block, (i + 1) * block)
        downs = jnp.concatenate([down[c, :, cut], down_other[:, cut]], axis=0)
        parts[i, :count, :] = dot(hidden, downs).astype(BF)
        parts[i, count:, :] = dot(shared_hidden, shared_down[:, cut]).astype(BF)


def pack_lines(at, line_of, parts, dense, lines, shared_own, shared_send):
    first = at[1] == 0
    group = line_of.shape[0]
    part = group // 8
    cols = dense.shape[2]
    half = cols // 2
    count = dense.shape[1]
    groups = lines.shape[0] // group
    move = jnp.where(
        lax.broadcasted_iota(jnp.int32, (group, group), 1) == line_of[...], 1.0, 0.0
    ).astype(BF)
    total = parts[0].astype(F32)
    for i in range(1, parts.shape[0]):
        total = total + parts[i].astype(F32)
    routed = total[:count].astype(BF)
    shared = total[count:]
    shared_own[...] = jnp.where(first, shared[:, :cols], shared[:, cols:])
    shared_send[...] = jnp.where(first, shared[:, cols:], shared[:, :cols]).astype(BF)
    for g in range(groups):
        here = slice(g * part, (g + 1) * part)
        own, other = dense[0, here, :], dense[1, here, :]
        sides = [jnp.where(first, own, other), jnp.where(first, other, own)]
        stack = []
        for side in range(2):
            for h in range(2):
                at_col = side * cols + h * half
                stack.append(routed[here, at_col : at_col + half])
                stack.append(sides[side][:, h * half : (h + 1) * half])
        rows = jnp.concatenate(stack, axis=0)
        lines[g * group : (g + 1) * group, :] = dot(move, rows).astype(BF)


def step(
    tokens,
    state,
    norm_gain,
    w_query,
    w_forget,
    w_input,
    w_outgate,
    lower_bound,
    head_gain,
    w_output,
    ffn_gain,
    route_ids,
    route_weight,
    expert_gate,
    expert_up,
    expert_down,
    shared_gate,
    shared_up,
    shared_down,
    dense_gate,
    dense_up,
    dense_down,
    dense_mix,
):
    nz, nx, ny, nc = (lax.axis_size(a) for a in ("z", "x", "y", "c"))
    x, y, c = (lax.axis_index(a) for a in ("x", "y", "c"))
    seq, width = tokens.shape
    rows_w, chan = w_query.shape
    head_dim = state.shape[2]
    cols = width // (ny * nc)

    at = jnp.stack([y, c, x]).astype(jnp.int32)

    topk = route_ids.shape[1]
    experts = nz * nx * nc
    cap = max(2, 2 * seq * topk // experts)
    slots = 2 * cap
    half = cols // 2
    flat_ids = route_ids.reshape(-1)
    onehot = (flat_ids[:, None] == jnp.arange(experts, dtype=jnp.int32)[None, :]).astype(jnp.int32)
    rank = jnp.sum((jnp.cumsum(onehot, axis=0) - onehot) * onehot, axis=1)
    lines_of = (flat_ids * (2 * slots) + rank).reshape(seq, topk)
    token_ids = jnp.arange(seq, dtype=jnp.int32)
    dense_of = (token_ids // cap) * (2 * slots) + cap + token_ids % cap
    slot_cols = jnp.concatenate(
        [lines_of, dense_of[:, None], jnp.zeros((seq, 8 - topk - 1), jnp.int32)], axis=1
    )
    slot_rows = slot_cols.T
    within = (jnp.arange(experts * 2 * slots, dtype=jnp.int32) % (nx * nc * 2 * slots))[None, :]

    spread_w, dense_block, *columns = call(
        prepare,
        [shaped(nz, rows_w, 4 * chan), shaped(3, *dense_gate.shape)]
        + [shaped(seq, nz * rows_w)] * nx,
        10**6,
        at,
        tokens,
        norm_gain.reshape(1, width),
        w_query,
        w_forget,
        w_input,
        w_outgate,
        dense_gate,
        dense_up,
        dense_down,
        scratch=[pltpu.VMEM((nx, seq, nz * rows_w), BF)],
    )
    weights = swap(spread_w, "z").reshape(nz * rows_w, 4 * chan)
    mine = [columns[0]] + [shift(columns[d], "x", d) for d in range(1, nx)]
    part = dot(jnp.concatenate(mine, axis=0), weights).astype(BF)
    part = part.reshape(nx, seq, 4 * chan)
    pieces = [part[0]] + [shift(part[d], "x", -d) for d in range(1, nx)]

    dense_own = [dense_block] + [shift(dense_block, "x", d) for d in range(1, nx)]
    dense_other = [partner(block) for block in dense_own]
    gate_other, up_other, down_other = (
        partner(pick(stack, 1 - c)) for stack in (expert_gate, expert_up, expert_down)
    )

    decay, keygate, values, keep, give = call(
        recur,
        [shaped(seq, chan, dtype=F32)] * 3 + [shaped(ny, seq, cols)] * 2,
        4 * state.size,
        at,
        *pieces,
        lower_bound.reshape(1, chan),
        head_gain.reshape(1, chan),
        state.reshape(seq, head_dim, head_dim),
        w_output,
        scratch=[pltpu.VMEM((seq, head_dim), F32)],
    )
    shape = (seq, 1, head_dim)
    new_state = (
        decay.reshape(shape)[..., None] * state
        + keygate.reshape(shape)[..., None] * values.reshape(shape)[:, :, None, :]
    )

    pair = (keep.astype(F32) + partner(give).astype(F32)).astype(BF)
    heads = swap(pair, "y")
    resid, own, outgoing = call(
        dispatch,
        [
            shaped(seq, cols, dtype=F32),
            shaped(seq, cols),
            shaped(experts * 2 * slots, half),
        ],
        4 * experts * 2 * slots * seq * half,
        at,
        heads,
        tokens,
        slot_rows,
    )
    arrived = swap(outgoing.reshape(experts, 2 * slots, half), HUB)
    other = partner(own)
    count = nz * nx * cap

    group = 8 * nc * 2 * slots
    lines = jnp.arange(group, dtype=jnp.int32)
    source, rest = lines // (4 * slots), lines % (4 * slots)
    side, h, kind, r = (
        rest // (2 * slots),
        rest // slots % 2,
        rest // cap % 2,
        rest % cap,
    )
    line_of = ((side * 2 + h) * 2 + kind) * (8 * cap) + source * cap + r
    both, dense_rows = call(
        unpack_rows,
        [shaped(ny, count + seq, nc * cols), shaped(nc, count, cols)],
        4 * 2 * group * group * half,
        at,
        line_of.reshape(1, group),
        arrived.reshape(-1, half),
        own,
        other,
    )
    whole = swap(both, "y")

    hidden_width = nx * dense_gate.shape[1]
    quarter = count // ny
    pre = call(
        dense_first_half,
        [shaped(quarter, 2 * hidden_width + 128)] * ny,
        2 * count * nc * cols * 2 * hidden_width,
        at,
        dense_rows,
        ffn_gain.reshape(ny * nc, cols),
        *dense_own,
        *dense_other,
    )
    pre = [pre[0]] + [shift(pre[d], "y", d) for d in range(1, ny)]
    (hidden,) = call(dense_activation, [shaped(quarter, hidden_width)], 10**6, *pre)
    hidden = [hidden] + [shift(hidden, "y", d) for d in range(1, ny)]
    (dense_part,) = call(
        dense_second_half,
        [shaped(nc, count, cols)],
        2 * count * nc * cols * hidden_width,
        at,
        *hidden,
        *dense_own,
        *dense_other,
    )

    (parts,) = call(
        experts_and_shared,
        [shaped(ny, count + seq, nc * cols)],
        2 * 3 * (count * 2 + seq) * width * expert_gate.shape[2],
        at,
        whole,
        ffn_gain.reshape(1, width),
        expert_gate,
        gate_other,
        expert_up,
        up_other,
        expert_down,
        down_other,
        shared_gate,
        shared_up,
        shared_down,
        mib=24,
    )
    parts = swap(parts, "y")
    back, shared_own, shared_send = call(
        pack_lines,
        [
            shaped(experts * 2 * slots, half),
            shaped(seq, cols, dtype=F32),
            shaped(seq, cols),
        ],
        4 * 2 * group * group * half,
        at,
        line_of.reshape(group, 1),
        parts,
        dense_part,
    )

    results = swap(back.reshape(experts, 2 * slots, half), HUB)
    (mixed,) = call(
        finish,
        [shaped(seq, cols)],
        8 * experts * 2 * slots * seq * half,
        results.reshape(experts * 2 * slots, half),
        within,
        slot_cols,
        route_weight,
        resid,
        shared_own,
        partner(shared_send),
        dense_mix.reshape(1, cols),
    )
    return (mixed, new_state)


def solution(mesh):
    torus = Mesh(mesh.devices.reshape(8, 4, 4, 2), ("z", "x", "y", "c"))
    return jax.shard_map(
        step,
        mesh=torus,
        in_specs=(
            P(EP, None),
            P(EP, TP, None, None),
            P(),
            P(EP, TP),
            P(EP, TP),
            P(EP, TP),
            P(EP, TP),
            P(TP),
            P(TP),
            P(TP, None),
            P(),
            P(EP, None),
            P(EP, None),
            P(EP, None, TP),
            P(EP, None, TP),
            P(EP, TP, None),
            P(None, TP),
            P(None, TP),
            P(TP, None),
            P(TP, EP),
            P(TP, EP),
            P(EP, TP),
            P(TP),
        ),
        out_specs=(P(EP, TP), P(EP, TP, None, None)),
        check_vma=False,
    )
```

```python
import jax
import jax.numpy as jnp
from jax import lax
from jax.experimental import pallas as pl
from jax.experimental.pallas import tpu as pltpu
from jax.sharding import Mesh
from jax.sharding import PartitionSpec as P

EP = ("z", "x")
TP = ("y", "c")
HUB = ("z", "x", "c")


EPS = 1e-06
BF = jnp.bfloat16
F32 = jnp.float32


def swap(x, axis):
    return lax.all_to_all(x, axis, split_axis=0, concat_axis=0, tiled=True)


def partner(x):
    return lax.ppermute(x, "c", [(0, 1), (1, 0)])


def shift(x, axis, by):
    size = lax.axis_size(axis)
    return lax.ppermute(x, axis, [(i, (i + by) % size) for i in range(size)])


def pick(x, index):
    return lax.dynamic_index_in_dim(x, index, 0, keepdims=False)


def dot(a, b):
    return jnp.dot(a, b, preferred_element_type=F32)


def silu(x):
    return x * jax.nn.sigmoid(x)


def call(body, outs, flops, *args, mib=0, scratch=()):
    moved = sum(a.size * a.dtype.itemsize for a in args) + sum(
        o.size * o.dtype.itemsize for o in outs
    )
    specs = [
        pl.BlockSpec(memory_space=pltpu.SMEM if a.dtype == jnp.int32 and a.ndim == 1 else pltpu.VMEM)
        for a in args
    ]
    return pl.pallas_call(
        body,
        out_shape=outs,
        in_specs=specs,
        out_specs=[pl.BlockSpec(memory_space=pltpu.VMEM) for _ in outs],
        scratch_shapes=scratch,
        cost_estimate=pl.CostEstimate(flops=flops, bytes_accessed=moved, transcendentals=0),
        compiler_params=pltpu.CompilerParams(vmem_limit_bytes=mib * 2**20) if mib else None,
    )(*args)


def shaped(*dims, dtype=BF):
    return jax.ShapeDtypeStruct(dims, dtype)


def prepare(at, tokens, gain, wq, wf, wi, wo, dg, du, dd, spread_w, dense, t0, t1, t2, t3, held):
    x = at[2]
    for i, block in enumerate((dg, du, dd)):
        dense[i] = block[...]
    for i, block in enumerate((wq, wf, wi, wo)):
        width = block.shape[1]
        value = block[...]
        for z in range(spread_w.shape[0]):
            spread_w[z, :, i * width : (i + 1) * width] = value
    wide = tokens[...].astype(F32)
    wide = wide * lax.rsqrt(jnp.mean(wide * wide, axis=1, keepdims=True) + EPS) * gain[...]
    low = lax.broadcasted_iota(jnp.int32, (wide.shape[0], 128), 1) < 64

    def tile(i):
        return wide[:, i * 128 : (i + 1) * 128]

    for to in range(4):
        for k in range(4):
            a, b = tile(4 * k + to // 2), tile(4 * k + 2 + to // 2)
            if to % 2 == 0:
                value = jnp.where(low, a, pltpu.roll(b, 64, 1))
            else:
                value = jnp.where(low, pltpu.roll(a, 64, 1), b)
            held[to, :, k * 128 : (k + 1) * 128] = value.astype(BF)
    for d, out in enumerate((t0, t1, t2, t3)):
        out[...] = held[lax.rem(x + d, 4)]


def recur(at, p0, p1, p2, p3, bound, gain, state, w_out, decay_out, key_out, value_out, keep, give, read):
    first = at[1] == 0
    seq = p0.shape[0]
    total = (
        p0[...].astype(F32) + p1[...].astype(F32) + p2[...].astype(F32) + p3[...].astype(F32)
    )
    total = total.astype(BF).astype(F32)
    query, forget, values, gate = (total[:, i * 128 : (i + 1) * 128] for i in range(4))
    forget = jax.nn.sigmoid(forget)
    low = bound[...]
    decay = low + (1.0 - low) * forget
    key = (1.0 - low) * (1.0 - forget)
    decay_out[...] = decay
    key_out[...] = key
    value_out[...] = values
    turned = jnp.transpose(query * decay)
    for b in range(seq):
        read[b : b + 1, :] = jnp.sum(turned[:, b : b + 1] * state[b], axis=0, keepdims=True)
    readout = read[...] + jnp.sum(query * key, axis=1, keepdims=True) * values
    readout = readout * lax.rsqrt(jnp.mean(readout * readout, axis=1, keepdims=True) + EPS)
    head = (readout * gain[...] * silu(gate)).astype(BF)
    cols = keep.shape[2]
    for y in range(keep.shape[0]):
        cut = slice(2 * y * cols, (2 * y + 1) * cols)
        cut_next = slice((2 * y + 1) * cols, (2 * y + 2) * cols)
        even = dot(head, w_out[:, cut]).astype(BF)
        odd = dot(head, w_out[:, cut_next]).astype(BF)
        keep[y] = jnp.where(first, even, odd)
        give[y] = jnp.where(first, odd, even)


def dispatch(at, heads, tokens, slots, resid, own, lines):
    cols = resid.shape[1]
    half = cols // 2
    seq = resid.shape[0]
    start = pl.multiple_of((2 * at[0] + at[1]) * cols, cols)
    total = tokens[:, pl.ds(start, cols)].astype(F32)
    for i in range(heads.shape[0]):
        total = total + heads[i].astype(F32)
    resid[...] = total
    rows = total.astype(BF)
    own[...] = rows
    chunk = 192
    place = lax.broadcasted_iota(jnp.int32, (chunk, seq), 0)
    for h in range(2):
        shifted = place - 12 * h
        dense = shifted == slots[4:5, :]
        for z in range(lines.shape[0] // chunk):
            here = shifted + z * chunk
            hit = dense
            for k in range(4):
                hit = hit | (here == slots[k : k + 1, :])
            part = dot(jnp.where(hit, 1.0, 0.0).astype(BF), rows[:, h * half : (h + 1) * half])
            if h == 0:
                lines[z * chunk : (z + 1) * chunk, :] = part.astype(BF)
            else:
                before = lines[z * chunk : (z + 1) * chunk, :].astype(F32)
                lines[z * chunk : (z + 1) * chunk, :] = (before + part).astype(BF)


def finish(lines, within, slots, weight, resid, shared, shared_other, mix, out):
    seq, cols = out.shape
    half = cols // 2
    place = lax.broadcasted_iota(jnp.int32, (seq, lines.shape[0]), 1)
    gate = jax.nn.sigmoid(mix[...])
    base = resid[...] + shared[...] + shared_other[...].astype(F32)
    for h in range(2):
        routed = jnp.zeros(place.shape, F32)
        for k in range(4):
            routed = jnp.where(place == slots[:, k : k + 1] + 12 * h, weight[:, k : k + 1], routed)
        dense = jnp.where(within[...] == slots[:, 4:5] + 12 * h, 1.0, 0.0)
        cut = slice(h * half, (h + 1) * half)
        total = base[:, cut] + dot(routed.astype(BF), lines[...])
        total = total + gate[:, cut] * dot(dense.astype(BF), lines[...])
        out[:, cut] = total.astype(BF)


def unpack_rows(at, line_of, lines, own, other, both, dense):
    first = at[1] == 0
    group = line_of.shape[1]
    count = dense.shape[1]
    cols = dense.shape[2]
    half = cols // 2
    part = group // 8
    groups = lines.shape[0] // group
    move = jnp.where(
        lax.broadcasted_iota(jnp.int32, (group, group), 0) == line_of[...], 1.0, 0.0
    ).astype(BF)
    mine, others = own[...], other[...]
    both_rows = [
        jnp.where(first, mine, others),
        jnp.where(first, others, mine),
    ]
    for g in range(groups):
        rows = dot(move, lines[g * group : (g + 1) * group, :]).astype(BF)
        here = slice(g * part, (g + 1) * part)
        for side in range(2):
            for h in range(2):
                base = (side * 2 + h) * 2 * part
                at_col = side * cols + h * half
                for copy in range(both.shape[0]):
                    both[copy, here, at_col : at_col + half] = rows[base : base + part]
                dense[side, here, h * half : (h + 1) * half] = rows[base + part : base + 2 * part]
    for side in range(2):
        for copy in range(both.shape[0]):
            both[copy, count:, side * cols : (side + 1) * cols] = both_rows[side]


def dense_first_half(at, rows, gain, *refs):
    y, c = at[0], at[1]
    own_w, other_w, outs = refs[:4], refs[4:8], refs[8:]
    ny = len(outs)
    size = rows.shape[1] // ny
    cols = rows.shape[2]

    def turned(side):
        return jnp.concatenate(
            [
                rows[side, pl.ds(pl.multiple_of(lax.rem(y + d, ny) * size, size), size), :]
                for d in range(ny)
            ],
            axis=0,
        ).astype(F32)

    own, other = turned(c), turned(1 - c)
    square = jnp.sum(own * own + other * other, axis=1, keepdims=True)
    high = square.astype(BF).astype(F32)
    low = square - high
    own = (own * gain[pl.ds(2 * y + c, 1), :]).astype(BF)
    other = (other * gain[pl.ds(2 * y + 1 - c, 1), :]).astype(BF)
    for kind in range(2):
        for i in range(4):
            value = (dot(own, own_w[i][kind]) + dot(other, other_w[i][kind])).astype(BF)
            at_col = (kind * 4 + i) * cols
            for d in range(ny):
                outs[d][:, at_col : at_col + cols] = value[d * size : (d + 1) * size]
    lane = lax.broadcasted_iota(jnp.int32, (square.shape[0], 128), 1)
    both = jnp.where(lane < 64, high, low).astype(BF)
    for d in range(ny):
        outs[d][:, 8 * cols : 8 * cols + 128] = both[d * size : (d + 1) * size]


def dense_activation(a, b, c, d, out):
    width = out.shape[1]
    features = 2048

    def summed(cut):
        return (
            a[:, cut].astype(F32) + b[:, cut].astype(F32) + c[:, cut].astype(F32) + d[:, cut].astype(F32)
        )

    square = summed(slice(2 * width, 2 * width + 128))
    total = square[:, 0:1] + square[:, 64:65]
    scale = lax.rsqrt(total / features + EPS)
    gate = summed(slice(0, width)) * scale
    up = summed(slice(width, 2 * width)) * scale
    out[...] = (silu(gate) * up).astype(BF)


def dense_second_half(at, *refs):
    y = at[0]
    hidden, own_w, other_w, out = refs[:4], refs[4:8], refs[8:12], refs[12]
    ny = len(hidden)
    size, cols = hidden[0].shape[0], out.shape[2]
    rows = jnp.concatenate([h[...] for h in hidden], axis=0)
    for side, weights in enumerate((own_w, other_w)):
        total = None
        for i in range(4):
            term = dot(rows[:, i * cols : (i + 1) * cols], weights[i][2])
            total = term if total is None else total + term
        total = total.astype(BF)
        for d in range(ny):
            start = pl.multiple_of(lax.rem(y + ny - d, ny) * size, size)
            out[side, pl.ds(start, size), :] = total[d * size : (d + 1) * size]


def experts_and_shared(
    at, whole, gain, gate, gate_other, up, up_other, down, down_other,
    shared_gate, shared_up, shared_down, parts,
):
    c = at[1]
    ny, lines, block = whole.shape
    count = lines - 48
    square = jnp.zeros((lines, 1), F32)
    rows = []
    for i in range(ny):
        value = whole[i].astype(F32)
        square = square + jnp.sum(value * value, axis=1, keepdims=True)
        rows.append(value)
    scale = lax.rsqrt(square / (ny * block) + EPS)
    rows = [
        (value * scale * gain[:, i * block : (i + 1) * block]).astype(BF)
        for i, value in enumerate(rows)
    ]
    gate_pre = up_pre = gate_shared = up_shared = None

    def more(total, term):
        return term if total is None else total + term

    for i in range(ny):
        cut = slice(i * block, (i + 1) * block)
        gates = jnp.concatenate([gate[c, cut, :], gate_other[cut, :]], axis=1)
        ups = jnp.concatenate([up[c, cut, :], up_other[cut, :]], axis=1)
        shared = jnp.concatenate([shared_gate[cut, :], shared_up[cut, :]], axis=1)
        gate_pre = more(gate_pre, dot(rows[i][:count], gates))
        up_pre = more(up_pre, dot(rows[i][:count], ups))
        gate_shared = more(gate_shared, dot(rows[i][count:], shared))
    half = gate.shape[2]
    hidden = (silu(gate_pre) * up_pre).astype(BF)
    shared_hidden = (silu(gate_shared[:, :half]) * gate_shared[:, half:]).astype(BF)
    for i in range(ny):
        cut = slice(i * block, (i + 1) * block)
        downs = jnp.concatenate([down[c, :, cut], down_other[:, cut]], axis=0)
        parts[i, :count, :] = dot(hidden, downs).astype(BF)
        parts[i, count:, :] = dot(shared_hidden, shared_down[:, cut]).astype(BF)


def pack_lines(at, line_of, parts, dense, lines, shared_own, shared_send):
    first = at[1] == 0
    group = line_of.shape[0]
    part = group // 8
    cols = dense.shape[2]
    half = cols // 2
    count = dense.shape[1]
    groups = lines.shape[0] // group
    move = jnp.where(
        lax.broadcasted_iota(jnp.int32, (group, group), 1) == line_of[...], 1.0, 0.0
    ).astype(BF)
    total = parts[0].astype(F32)
    for i in range(1, parts.shape[0]):
        total = total + parts[i].astype(F32)
    routed = total[:count].astype(BF)
    shared = total[count:]
    shared_own[...] = jnp.where(first, shared[:, :cols], shared[:, cols:])
    shared_send[...] = jnp.where(first, shared[:, cols:], shared[:, :cols]).astype(BF)
    for g in range(groups):
        here = slice(g * part, (g + 1) * part)
        own, other = dense[0, here, :], dense[1, here, :]
        sides = [jnp.where(first, own, other), jnp.where(first, other, own)]
        stack = []
        for side in range(2):
            for h in range(2):
                at_col = side * cols + h * half
                stack.append(routed[here, at_col : at_col + half])
                stack.append(sides[side][:, h * half : (h + 1) * half])
        rows = jnp.concatenate(stack, axis=0)
        lines[g * group : (g + 1) * group, :] = dot(move, rows).astype(BF)


def step(
    tokens,
    state,
    norm_gain,
    w_query,
    w_forget,
    w_input,
    w_outgate,
    lower_bound,
    head_gain,
    w_output,
    ffn_gain,
    route_ids,
    route_weight,
    expert_gate,
    expert_up,
    expert_down,
    shared_gate,
    shared_up,
    shared_down,
    dense_gate,
    dense_up,
    dense_down,
    dense_mix,
):
    nz, nx, ny, nc = (lax.axis_size(a) for a in ("z", "x", "y", "c"))
    x, y, c = (lax.axis_index(a) for a in ("x", "y", "c"))
    seq, width = tokens.shape
    rows_w, chan = w_query.shape
    head_dim = state.shape[2]
    cols = width // (ny * nc)

    at = jnp.stack([y, c, x]).astype(jnp.int32)

    topk = route_ids.shape[1]
    experts = nz * nx * nc
    cap = max(2, 2 * seq * topk // experts)
    slots = 2 * cap
    half = cols // 2
    flat_ids = route_ids.reshape(-1)
    onehot = (flat_ids[:, None] == jnp.arange(experts, dtype=jnp.int32)[None, :]).astype(jnp.int32)
    rank = jnp.sum((jnp.cumsum(onehot, axis=0) - onehot) * onehot, axis=1)
    lines_of = (flat_ids * (2 * slots) + rank).reshape(seq, topk)
    token_ids = jnp.arange(seq, dtype=jnp.int32)
    dense_of = (token_ids // cap) * (2 * slots) + cap + token_ids % cap
    slot_cols = jnp.concatenate(
        [lines_of, dense_of[:, None], jnp.zeros((seq, 8 - topk - 1), jnp.int32)], axis=1
    )
    slot_rows = slot_cols.T
    within = (jnp.arange(experts * 2 * slots, dtype=jnp.int32) % (nx * nc * 2 * slots))[None, :]

    spread_w, dense_block, *columns = call(
        prepare,
        [shaped(nz, rows_w, 4 * chan), shaped(3, *dense_gate.shape)]
        + [shaped(seq, nz * rows_w)] * nx,
        10**6,
        at,
        tokens,
        norm_gain.reshape(1, width),
        w_query,
        w_forget,
        w_input,
        w_outgate,
        dense_gate,
        dense_up,
        dense_down,
        scratch=[pltpu.VMEM((nx, seq, nz * rows_w), BF)],
    )
    weights = swap(spread_w, "z").reshape(nz * rows_w, 4 * chan)
    mine = [columns[0]] + [shift(columns[d], "x", d) for d in range(1, nx)]
    part = dot(jnp.concatenate(mine, axis=0), weights).astype(BF)
    part = part.reshape(nx, seq, 4 * chan)
    pieces = [part[0]] + [shift(part[d], "x", -d) for d in range(1, nx)]

    dense_own = [dense_block] + [shift(dense_block, "x", d) for d in range(1, nx)]
    dense_other = [partner(block) for block in dense_own]
    gate_other, up_other, down_other = (
        partner(pick(stack, 1 - c)) for stack in (expert_gate, expert_up, expert_down)
    )

    decay, keygate, values, keep, give = call(
        recur,
        [shaped(seq, chan, dtype=F32)] * 3 + [shaped(ny, seq, cols)] * 2,
        4 * state.size,
        at,
        *pieces,
        lower_bound.reshape(1, chan),
        head_gain.reshape(1, chan),
        state.reshape(seq, head_dim, head_dim),
        w_output,
        scratch=[pltpu.VMEM((seq, head_dim), F32)],
    )
    shape = (seq, 1, head_dim)
    new_state = (
        decay.reshape(shape)[..., None] * state
        + keygate.reshape(shape)[..., None] * values.reshape(shape)[:, :, None, :]
    )

    pair = (keep.astype(F32) + partner(give).astype(F32)).astype(BF)
    heads = swap(pair, "y")
    resid, own, outgoing = call(
        dispatch,
        [
            shaped(seq, cols, dtype=F32),
            shaped(seq, cols),
            shaped(experts * 2 * slots, half),
        ],
        4 * experts * 2 * slots * seq * half,
        at,
        heads,
        tokens,
        slot_rows,
    )
    arrived = swap(outgoing.reshape(experts, 2 * slots, half), HUB)
    other = partner(own)
    count = nz * nx * cap

    group = 8 * nc * 2 * slots
    lines = jnp.arange(group, dtype=jnp.int32)
    source, rest = lines // (4 * slots), lines % (4 * slots)
    side, h, kind, r = (
        rest // (2 * slots),
        rest // slots % 2,
        rest // cap % 2,
        rest % cap,
    )
    line_of = ((side * 2 + h) * 2 + kind) * (8 * cap) + source * cap + r
    both, dense_rows = call(
        unpack_rows,
        [shaped(ny, count + seq, nc * cols), shaped(nc, count, cols)],
        4 * 2 * group * group * half,
        at,
        line_of.reshape(1, group),
        arrived.reshape(-1, half),
        own,
        other,
    )
    whole = swap(both, "y")

    hidden_width = nx * dense_gate.shape[1]
    quarter = count // ny
    pre = call(
        dense_first_half,
        [shaped(quarter, 2 * hidden_width + 128)] * ny,
        2 * count * nc * cols * 2 * hidden_width,
        at,
        dense_rows,
        ffn_gain.reshape(ny * nc, cols),
        *dense_own,
        *dense_other,
    )
    pre = [pre[0]] + [shift(pre[d], "y", d) for d in range(1, ny)]
    (hidden,) = call(dense_activation, [shaped(quarter, hidden_width)], 10**6, *pre)
    hidden = [hidden] + [shift(hidden, "y", d) for d in range(1, ny)]
    (dense_part,) = call(
        dense_second_half,
        [shaped(nc, count, cols)],
        2 * count * nc * cols * hidden_width,
        at,
        *hidden,
        *dense_own,
        *dense_other,
    )

    (parts,) = call(
        experts_and_shared,
        [shaped(ny, count + seq, nc * cols)],
        2 * 3 * (count * 2 + seq) * width * expert_gate.shape[2],
        at,
        whole,
        ffn_gain.reshape(1, width),
        expert_gate,
        gate_other,
        expert_up,
        up_other,
        expert_down,
        down_other,
        shared_gate,
        shared_up,
        shared_down,
        mib=0,
    )
    parts = swap(parts, "y")
    back, shared_own, shared_send = call(
        pack_lines,
        [
            shaped(experts * 2 * slots, half),
            shaped(seq, cols, dtype=F32),
            shaped(seq, cols),
        ],
        4 * 2 * group * group * half,
        at,
        line_of.reshape(group, 1),
        parts,
        dense_part,
    )

    results = swap(back.reshape(experts, 2 * slots, half), HUB)
    (mixed,) = call(
        finish,
        [shaped(seq, cols)],
        8 * experts * 2 * slots * seq * half,
        results.reshape(experts * 2 * slots, half),
        within,
        slot_cols,
        route_weight,
        resid,
        shared_own,
        partner(shared_send),
        dense_mix.reshape(1, cols),
    )
    return (mixed, new_state)


def solution(mesh):
    torus = Mesh(mesh.devices.reshape(8, 4, 4, 2), ("z", "x", "y", "c"))
    return jax.shard_map(
        step,
        mesh=torus,
        in_specs=(
            P(EP, None),
            P(EP, TP, None, None),
            P(),
            P(EP, TP),
            P(EP, TP),
            P(EP, TP),
            P(EP, TP),
            P(TP),
            P(TP),
            P(TP, None),
            P(),
            P(EP, None),
            P(EP, None),
            P(EP, None, TP),
            P(EP, None, TP),
            P(EP, TP, None),
            P(None, TP),
            P(None, TP),
            P(TP, None),
            P(TP, EP),
            P(TP, EP),
            P(EP, TP),
            P(TP),
        ),
        out_specs=(P(EP, TP), P(EP, TP, None, None)),
        check_vma=False,
    )
```

```python
import jax
import jax.numpy as jnp
from jax import lax
from jax.experimental import pallas as pl
from jax.experimental.pallas import tpu as pltpu
from jax.sharding import Mesh
from jax.sharding import PartitionSpec as P

EP = ("z", "x")
TP = ("y", "c")
HUB = ("z", "x", "c")


EPS = 1e-06
BF = jnp.bfloat16
F32 = jnp.float32


def swap(x, axis):
    return lax.all_to_all(x, axis, split_axis=0, concat_axis=0, tiled=True)


def partner(x):
    return lax.ppermute(x, "c", [(0, 1), (1, 0)])


def shift(x, axis, by):
    size = lax.axis_size(axis)
    return lax.ppermute(x, axis, [(i, (i + by) % size) for i in range(size)])


def pick(x, index):
    return lax.dynamic_index_in_dim(x, index, 0, keepdims=False)


def dot(a, b):
    return jnp.dot(a, b, preferred_element_type=F32)


def silu(x):
    return x * jax.nn.sigmoid(x)


def call(body, outs, flops, kinds, *args, mib=53, scratch=()):
    kinds, out_kinds = kinds.split()
    moved = sum(a.size * a.dtype.itemsize for a in args) + sum(
        o.size * o.dtype.itemsize for o in outs
    )
    space = {"s": pltpu.SMEM, "v": pltpu.VMEM, "h": pltpu.HBM, "l": pltpu.HBM}
    fetched = [i for i, k in enumerate(kinds) if k in "hl"]
    stored = [i for i, k in enumerate(out_kinds) if k == "h"]
    room = [pltpu.VMEM(args[i].shape, args[i].dtype) for i in fetched]
    out_room = [pltpu.VMEM(outs[i].shape, outs[i].dtype) for i in stored]

    def whole(*refs):
        ins, rest = list(refs[: len(args)]), refs[len(args) :]
        results, rest = list(rest[: len(outs)]), rest[len(outs) :]
        in_room, rest = rest[: len(room)], rest[len(room) :]
        result_room, rest = rest[: len(out_room)], rest[len(out_room) :]
        in_sem, out_sem, extra = rest[0], rest[1], rest[2:]
        late = []
        now = []
        for n, i in enumerate(fetched):
            copy = pltpu.make_async_copy(ins[i], in_room[n], in_sem.at[n])
            copy.start()
            (late if kinds[i] == "l" else now).append(copy)
            ins[i] = in_room[n]
        targets = list(results)
        for n, i in enumerate(stored):
            results[i] = result_room[n]
        for copy in now:
            copy.wait()
        if late:
            body([copy.wait for copy in late], *ins, *results, *extra)
        else:
            body(*ins, *results, *extra)
        back = [
            pltpu.make_async_copy(result_room[n], targets[i], out_sem.at[n])
            for n, i in enumerate(stored)
        ]
        for copy in back:
            copy.start()
        for copy in back:
            copy.wait()

    return pl.pallas_call(
        whole,
        out_shape=outs,
        in_specs=[pl.BlockSpec(memory_space=space[k]) for k in kinds],
        out_specs=[pl.BlockSpec(memory_space=space[k]) for k in out_kinds],
        scratch_shapes=[
            *room,
            *out_room,
            pltpu.SemaphoreType.DMA((max(1, len(room)),)),
            pltpu.SemaphoreType.DMA((max(1, len(out_room)),)),
            *scratch,
        ],
        cost_estimate=pl.CostEstimate(flops=flops, bytes_accessed=moved, transcendentals=0),
        compiler_params=pltpu.CompilerParams(vmem_limit_bytes=mib * 2**20),
    )(*args)


def shaped(*dims, dtype=BF):
    return jax.ShapeDtypeStruct(dims, dtype)


def prepare(at, tokens, gain, wq, wf, wi, wo, dg, du, dd, spread_w, dense, t0, t1, t2, t3, held):
    x = at[2]
    for i, block in enumerate((dg, du, dd)):
        dense[i] = block[...]
    for i, block in enumerate((wq, wf, wi, wo)):
        width = block.shape[1]
        value = block[...]
        for z in range(spread_w.shape[0]):
            spread_w[z, :, i * width : (i + 1) * width] = value
    wide = tokens[...].astype(F32)
    wide = wide * lax.rsqrt(jnp.mean(wide * wide, axis=1, keepdims=True) + EPS) * gain[...]
    low = lax.broadcasted_iota(jnp.int32, (wide.shape[0], 128), 1) < 64

    def tile(i):
        return wide[:, i * 128 : (i + 1) * 128]

    for to in range(4):
        for k in range(4):
            a, b = tile(4 * k + to // 2), tile(4 * k + 2 + to // 2)
            if to % 2 == 0:
                value = jnp.where(low, a, pltpu.roll(b, 64, 1))
            else:
                value = jnp.where(low, pltpu.roll(a, 64, 1), b)
            held[to, :, k * 128 : (k + 1) * 128] = value.astype(BF)
    for d, out in enumerate((t0, t1, t2, t3)):
        out[...] = held[lax.rem(x + d, 4)]


def recur(wait, at, p0, p1, p2, p3, bound, gain, state, w_out, decay_out, key_out, value_out, keep, give, read):
    first = at[1] == 0
    seq = p0.shape[0]
    total = (
        p0[...].astype(F32) + p1[...].astype(F32) + p2[...].astype(F32) + p3[...].astype(F32)
    )
    total = total.astype(BF).astype(F32)
    query, forget, values, gate = (total[:, i * 128 : (i + 1) * 128] for i in range(4))
    forget = jax.nn.sigmoid(forget)
    low = bound[...]
    decay = low + (1.0 - low) * forget
    key = (1.0 - low) * (1.0 - forget)
    decay_out[...] = decay
    key_out[...] = key
    value_out[...] = values
    turned = jnp.transpose(query * decay)
    wait[0]()
    for b in range(seq):
        read[b : b + 1, :] = jnp.sum(turned[:, b : b + 1] * state[b], axis=0, keepdims=True)
    readout = read[...] + jnp.sum(query * key, axis=1, keepdims=True) * values
    readout = readout * lax.rsqrt(jnp.mean(readout * readout, axis=1, keepdims=True) + EPS)
    head = (readout * gain[...] * silu(gate)).astype(BF)
    wait[1]()
    cols = keep.shape[2]
    for y in range(keep.shape[0]):
        cut = slice(2 * y * cols, (2 * y + 1) * cols)
        cut_next = slice((2 * y + 1) * cols, (2 * y + 2) * cols)
        even = dot(head, w_out[:, cut]).astype(BF)
        odd = dot(head, w_out[:, cut_next]).astype(BF)
        keep[y] = jnp.where(first, even, odd)
        give[y] = jnp.where(first, odd, even)


def dispatch(at, heads, tokens, slots, resid, own, lines):
    cols = resid.shape[1]
    half = cols // 2
    seq = resid.shape[0]
    start = pl.multiple_of((2 * at[0] + at[1]) * cols, cols)
    total = tokens[:, pl.ds(start, cols)].astype(F32)
    for i in range(heads.shape[0]):
        total = total + heads[i].astype(F32)
    resid[...] = total
    rows = total.astype(BF)
    own[...] = rows
    chunk = 192
    place = lax.broadcasted_iota(jnp.int32, (chunk, seq), 0)
    for h in range(2):
        shifted = place - 12 * h
        dense = shifted == slots[4:5, :]
        for z in range(lines.shape[0] // chunk):
            here = shifted + z * chunk
            hit = dense
            for k in range(4):
                hit = hit | (here == slots[k : k + 1, :])
            part = dot(jnp.where(hit, 1.0, 0.0).astype(BF), rows[:, h * half : (h + 1) * half])
            if h == 0:
                lines[z * chunk : (z + 1) * chunk, :] = part.astype(BF)
            else:
                before = lines[z * chunk : (z + 1) * chunk, :].astype(F32)
                lines[z * chunk : (z + 1) * chunk, :] = (before + part).astype(BF)


def finish(lines, within, slots, weight, resid, shared, shared_other, mix, out):
    seq, cols = out.shape
    half = cols // 2
    place = lax.broadcasted_iota(jnp.int32, (seq, lines.shape[0]), 1)
    gate = jax.nn.sigmoid(mix[...])
    base = resid[...] + shared[...] + shared_other[...].astype(F32)
    for h in range(2):
        routed = jnp.zeros(place.shape, F32)
        for k in range(4):
            routed = jnp.where(place == slots[:, k : k + 1] + 12 * h, weight[:, k : k + 1], routed)
        dense = jnp.where(within[...] == slots[:, 4:5] + 12 * h, 1.0, 0.0)
        cut = slice(h * half, (h + 1) * half)
        total = base[:, cut] + dot(routed.astype(BF), lines[...])
        total = total + gate[:, cut] * dot(dense.astype(BF), lines[...])
        out[:, cut] = total.astype(BF)


def unpack_rows(at, line_of, lines, own, other, both, dense):
    first = at[1] == 0
    group = line_of.shape[1]
    count = dense.shape[1]
    cols = dense.shape[2]
    half = cols // 2
    part = group // 8
    groups = lines.shape[0] // group
    move = jnp.where(
        lax.broadcasted_iota(jnp.int32, (group, group), 0) == line_of[...], 1.0, 0.0
    ).astype(BF)
    mine, others = own[...], other[...]
    both_rows = [
        jnp.where(first, mine, others),
        jnp.where(first, others, mine),
    ]
    for g in range(groups):
        rows = dot(move, lines[g * group : (g + 1) * group, :]).astype(BF)
        here = slice(g * part, (g + 1) * part)
        for side in range(2):
            for h in range(2):
                base = (side * 2 + h) * 2 * part
                at_col = side * cols + h * half
                for copy in range(both.shape[0]):
                    both[copy, here, at_col : at_col + half] = rows[base : base + part]
                dense[side, here, h * half : (h + 1) * half] = rows[base + part : base + 2 * part]
    for side in range(2):
        for copy in range(both.shape[0]):
            both[copy, count:, side * cols : (side + 1) * cols] = both_rows[side]


def dense_first_half(at, rows, gain, *refs):
    y, c = at[0], at[1]
    own_w, other_w, outs = refs[:4], refs[4:8], refs[8:]
    ny = len(outs)
    size = rows.shape[1] // ny
    cols = rows.shape[2]

    def turned(side):
        return jnp.concatenate(
            [
                rows[side, pl.ds(pl.multiple_of(lax.rem(y + d, ny) * size, size), size), :]
                for d in range(ny)
            ],
            axis=0,
        ).astype(F32)

    own, other = turned(c), turned(1 - c)
    square = jnp.sum(own * own + other * other, axis=1, keepdims=True)
    high = square.astype(BF).astype(F32)
    low = square - high
    own = (own * gain[pl.ds(2 * y + c, 1), :]).astype(BF)
    other = (other * gain[pl.ds(2 * y + 1 - c, 1), :]).astype(BF)
    for kind in range(2):
        for i in range(4):
            value = (dot(own, own_w[i][kind]) + dot(other, other_w[i][kind])).astype(BF)
            at_col = (kind * 4 + i) * cols
            for d in range(ny):
                outs[d][:, at_col : at_col + cols] = value[d * size : (d + 1) * size]
    lane = lax.broadcasted_iota(jnp.int32, (square.shape[0], 128), 1)
    both = jnp.where(lane < 64, high, low).astype(BF)
    for d in range(ny):
        outs[d][:, 8 * cols : 8 * cols + 128] = both[d * size : (d + 1) * size]


def dense_activation(a, b, c, d, out):
    width = out.shape[1]
    features = 2048

    def summed(cut):
        return (
            a[:, cut].astype(F32) + b[:, cut].astype(F32) + c[:, cut].astype(F32) + d[:, cut].astype(F32)
        )

    square = summed(slice(2 * width, 2 * width + 128))
    total = square[:, 0:1] + square[:, 64:65]
    scale = lax.rsqrt(total / features + EPS)
    gate = summed(slice(0, width)) * scale
    up = summed(slice(width, 2 * width)) * scale
    out[...] = (silu(gate) * up).astype(BF)


def dense_second_half(at, *refs):
    y = at[0]
    hidden, own_w, other_w, out = refs[:4], refs[4:8], refs[8:12], refs[12]
    ny = len(hidden)
    size, cols = hidden[0].shape[0], out.shape[2]
    rows = jnp.concatenate([h[...] for h in hidden], axis=0)
    for side, weights in enumerate((own_w, other_w)):
        total = None
        for i in range(4):
            term = dot(rows[:, i * cols : (i + 1) * cols], weights[i][2])
            total = term if total is None else total + term
        total = total.astype(BF)
        for d in range(ny):
            start = pl.multiple_of(lax.rem(y + ny - d, ny) * size, size)
            out[side, pl.ds(start, size), :] = total[d * size : (d + 1) * size]


def experts_and_shared(
    wait, at, whole, gain, gate, gate_other, up, up_other, down, down_other,
    shared_gate, shared_up, shared_down, parts,
):
    c = at[1]
    ny, lines, block = whole.shape
    count = lines - 48
    square = jnp.zeros((lines, 1), F32)
    rows = []
    for i in range(ny):
        value = whole[i].astype(F32)
        square = square + jnp.sum(value * value, axis=1, keepdims=True)
        rows.append(value)
    scale = lax.rsqrt(square / (ny * block) + EPS)
    rows = [
        (value * scale * gain[:, i * block : (i + 1) * block]).astype(BF)
        for i, value in enumerate(rows)
    ]
    gate_pre = up_pre = gate_shared = None
    for i in (0, 1, 2, 3, 6, 7):
        wait[i]()

    def more(total, term):
        return term if total is None else total + term

    for i in range(ny):
        cut = slice(i * block, (i + 1) * block)
        gates = jnp.concatenate([gate[c, cut, :], gate_other[cut, :]], axis=1)
        ups = jnp.concatenate([up[c, cut, :], up_other[cut, :]], axis=1)
        shared = jnp.concatenate([shared_gate[cut, :], shared_up[cut, :]], axis=1)
        gate_pre = more(gate_pre, dot(rows[i][:count], gates))
        up_pre = more(up_pre, dot(rows[i][:count], ups))
        gate_shared = more(gate_shared, dot(rows[i][count:], shared))
    for i in (4, 5, 8):
        wait[i]()
    half = gate.shape[2]
    hidden = (silu(gate_pre) * up_pre).astype(BF)
    shared_hidden = (silu(gate_shared[:, :half]) * gate_shared[:, half:]).astype(BF)
    for i in range(ny):
        cut = slice(i * block, (i + 1) * block)
        downs = jnp.concatenate([down[c, :, cut], down_other[:, cut]], axis=0)
        parts[i, :count, :] = dot(hidden, downs).astype(BF)
        parts[i, count:, :] = dot(shared_hidden, shared_down[:, cut]).astype(BF)


def pack_lines(at, line_of, parts, dense, lines, shared_own, shared_send):
    first = at[1] == 0
    group = line_of.shape[0]
    part = group // 8
    cols = dense.shape[2]
    half = cols // 2
    count = dense.shape[1]
    groups = lines.shape[0] // group
    move = jnp.where(
        lax.broadcasted_iota(jnp.int32, (group, group), 1) == line_of[...], 1.0, 0.0
    ).astype(BF)
    total = parts[0].astype(F32)
    for i in range(1, parts.shape[0]):
        total = total + parts[i].astype(F32)
    routed = total[:count].astype(BF)
    shared = total[count:]
    shared_own[...] = jnp.where(first, shared[:, :cols], shared[:, cols:])
    shared_send[...] = jnp.where(first, shared[:, cols:], shared[:, :cols]).astype(BF)
    for g in range(groups):
        here = slice(g * part, (g + 1) * part)
        own, other = dense[0, here, :], dense[1, here, :]
        sides = [jnp.where(first, own, other), jnp.where(first, other, own)]
        stack = []
        for side in range(2):
            for h in range(2):
                at_col = side * cols + h * half
                stack.append(routed[here, at_col : at_col + half])
                stack.append(sides[side][:, h * half : (h + 1) * half])
        rows = jnp.concatenate(stack, axis=0)
        lines[g * group : (g + 1) * group, :] = dot(move, rows).astype(BF)


def step(
    tokens,
    state,
    norm_gain,
    w_query,
    w_forget,
    w_input,
    w_outgate,
    lower_bound,
    head_gain,
    w_output,
    ffn_gain,
    route_ids,
    route_weight,
    expert_gate,
    expert_up,
    expert_down,
    shared_gate,
    shared_up,
    shared_down,
    dense_gate,
    dense_up,
    dense_down,
    dense_mix,
):
    nz, nx, ny, nc = (lax.axis_size(a) for a in ("z", "x", "y", "c"))
    x, y, c = (lax.axis_index(a) for a in ("x", "y", "c"))
    seq, width = tokens.shape
    rows_w, chan = w_query.shape
    head_dim = state.shape[2]
    cols = width // (ny * nc)

    at = jnp.stack([y, c, x]).astype(jnp.int32)

    topk = route_ids.shape[1]
    experts = nz * nx * nc
    cap = max(2, 2 * seq * topk // experts)
    slots = 2 * cap
    half = cols // 2
    flat_ids = route_ids.reshape(-1)
    onehot = (flat_ids[:, None] == jnp.arange(experts, dtype=jnp.int32)[None, :]).astype(jnp.int32)
    rank = jnp.sum((jnp.cumsum(onehot, axis=0) - onehot) * onehot, axis=1)
    lines_of = (flat_ids * (2 * slots) + rank).reshape(seq, topk)
    token_ids = jnp.arange(seq, dtype=jnp.int32)
    dense_of = (token_ids // cap) * (2 * slots) + cap + token_ids % cap
    slot_cols = jnp.concatenate(
        [lines_of, dense_of[:, None], jnp.zeros((seq, 8 - topk - 1), jnp.int32)], axis=1
    )
    slot_rows = slot_cols.T
    within = (jnp.arange(experts * 2 * slots, dtype=jnp.int32) % (nx * nc * 2 * slots))[None, :]

    spread_w, dense_block, *columns = call(
        prepare,
        [shaped(nz, rows_w, 4 * chan), shaped(3, *dense_gate.shape)]
        + [shaped(seq, nz * rows_w)] * nx,
        10**6,
        "shhhhhhhhh hhhhhh",
        at,
        tokens,
        norm_gain.reshape(1, width),
        w_query,
        w_forget,
        w_input,
        w_outgate,
        dense_gate,
        dense_up,
        dense_down,
        mib=58,
        scratch=[pltpu.VMEM((nx, seq, nz * rows_w), BF)],
    )
    weights = swap(spread_w, "z").reshape(nz * rows_w, 4 * chan)
    mine = [columns[0]] + [shift(columns[d], "x", d) for d in range(1, nx)]
    part = dot(jnp.concatenate(mine, axis=0), weights).astype(BF)
    part = part.reshape(nx, seq, 4 * chan)
    pieces = [part[0]] + [shift(part[d], "x", -d) for d in range(1, nx)]

    dense_own = [dense_block] + [shift(dense_block, "x", d) for d in range(1, nx)]
    dense_other = [partner(block) for block in dense_own]
    gate_other, up_other, down_other = (
        partner(pick(stack, 1 - c)) for stack in (expert_gate, expert_up, expert_down)
    )

    decay, keygate, values, keep, give = call(
        recur,
        [shaped(seq, chan, dtype=F32)] * 3 + [shaped(ny, seq, cols)] * 2,
        4 * state.size,
        "shvvvhhll hhhvh",
        at,
        *pieces,
        lower_bound.reshape(1, chan),
        head_gain.reshape(1, chan),
        state.reshape(seq, head_dim, head_dim),
        w_output,
        scratch=[pltpu.VMEM((seq, head_dim), F32)],
    )
    shape = (seq, 1, head_dim)
    new_state = (
        decay.reshape(shape)[..., None] * state
        + keygate.reshape(shape)[..., None] * values.reshape(shape)[:, :, None, :]
    )

    pair = (keep.astype(F32) + partner(give).astype(F32)).astype(BF)
    heads = swap(pair, "y")
    resid, own, outgoing = call(
        dispatch,
        [
            shaped(seq, cols, dtype=F32),
            shaped(seq, cols),
            shaped(experts * 2 * slots, half),
        ],
        4 * experts * 2 * slots * seq * half,
        "svhh hhh",
        at,
        heads,
        tokens,
        slot_rows,
    )
    arrived = swap(outgoing.reshape(experts, 2 * slots, half), HUB)
    other = partner(own)
    count = nz * nx * cap

    group = 8 * nc * 2 * slots
    lines = jnp.arange(group, dtype=jnp.int32)
    source, rest = lines // (4 * slots), lines % (4 * slots)
    side, h, kind, r = (
        rest // (2 * slots),
        rest // slots % 2,
        rest // cap % 2,
        rest % cap,
    )
    line_of = ((side * 2 + h) * 2 + kind) * (8 * cap) + source * cap + r
    both, dense_rows = call(
        unpack_rows,
        [shaped(ny, count + seq, nc * cols), shaped(nc, count, cols)],
        4 * 2 * group * group * half,
        "shvhv hh",
        at,
        line_of.reshape(1, group),
        arrived.reshape(-1, half),
        own,
        other,
    )
    whole = swap(both, "y")

    hidden_width = nx * dense_gate.shape[1]
    quarter = count // ny
    pre = call(
        dense_first_half,
        [shaped(quarter, 2 * hidden_width + 128)] * ny,
        2 * count * nc * cols * 2 * hidden_width,
        "shhhhhhhhhh hhhh",
        at,
        dense_rows,
        ffn_gain.reshape(ny * nc, cols),
        *dense_own,
        *dense_other,
    )
    pre = [pre[0]] + [shift(pre[d], "y", d) for d in range(1, ny)]
    (hidden,) = call(
        dense_activation, [shaped(quarter, hidden_width)], 10**6, "hvvv h", *pre
    )
    hidden = [hidden] + [shift(hidden, "y", d) for d in range(1, ny)]
    (dense_part,) = call(
        dense_second_half,
        [shaped(nc, count, cols)],
        2 * count * nc * cols * hidden_width,
        "shvvvhhhhhhhh h",
        at,
        *hidden,
        *dense_own,
        *dense_other,
    )

    (parts,) = call(
        experts_and_shared,
        [shaped(ny, count + seq, nc * cols)],
        2 * 3 * (count * 2 + seq) * width * expert_gate.shape[2],
        "svhlllllllll h",
        at,
        whole,
        ffn_gain.reshape(1, width),
        expert_gate,
        gate_other,
        expert_up,
        up_other,
        expert_down,
        down_other,
        shared_gate,
        shared_up,
        shared_down,
    )
    parts = swap(parts, "y")
    back, shared_own, shared_send = call(
        pack_lines,
        [
            shaped(experts * 2 * slots, half),
            shaped(seq, cols, dtype=F32),
            shaped(seq, cols),
        ],
        4 * 2 * group * group * half,
        "shvh hhh",
        at,
        line_of.reshape(group, 1),
        parts,
        dense_part,
    )

    results = swap(back.reshape(experts, 2 * slots, half), HUB)
    (mixed,) = call(
        finish,
        [shaped(seq, cols)],
        8 * experts * 2 * slots * seq * half,
        "vhhhhhvh h",
        results.reshape(experts * 2 * slots, half),
        within,
        slot_cols,
        route_weight,
        resid,
        shared_own,
        partner(shared_send),
        dense_mix.reshape(1, cols),
    )
    return (mixed, new_state)


def solution(mesh):
    torus = Mesh(mesh.devices.reshape(8, 4, 4, 2), ("z", "x", "y", "c"))
    return jax.shard_map(
        step,
        mesh=torus,
        in_specs=(
            P(EP, None),
            P(EP, TP, None, None),
            P(),
            P(EP, TP),
            P(EP, TP),
            P(EP, TP),
            P(EP, TP),
            P(TP),
            P(TP),
            P(TP, None),
            P(),
            P(EP, None),
            P(EP, None),
            P(EP, None, TP),
            P(EP, None, TP),
            P(EP, TP, None),
            P(None, TP),
            P(None, TP),
            P(TP, None),
            P(TP, EP),
            P(TP, EP),
            P(EP, TP),
            P(TP),
        ),
        out_specs=(P(EP, TP), P(EP, TP, None, None)),
        check_vma=False,
    )
```

```python
import jax
import jax.numpy as jnp
from jax import lax
from jax.experimental import pallas as pl
from jax.experimental.pallas import tpu as pltpu
from jax.sharding import Mesh
from jax.sharding import PartitionSpec as P

EP = ("z", "x")
TP = ("y", "c")
HUB = ("z", "x", "c")


EPS = 1e-06
BF = jnp.bfloat16
F32 = jnp.float32


def swap(x, axis):
    return lax.all_to_all(x, axis, split_axis=0, concat_axis=0, tiled=True)


def partner(x):
    return lax.ppermute(x, "c", [(0, 1), (1, 0)])


def shift(x, axis, by):
    size = lax.axis_size(axis)
    return lax.ppermute(x, axis, [(i, (i + by) % size) for i in range(size)])


def pick(x, index):
    return lax.dynamic_index_in_dim(x, index, 0, keepdims=False)


def dot(a, b):
    return jnp.dot(a, b, preferred_element_type=F32)


def silu(x):
    return x * jax.nn.sigmoid(x)


def call(body, outs, flops, kinds, *args, mib=53, scratch=()):
    kinds, out_kinds = kinds.split()
    moved = sum(a.size * a.dtype.itemsize for a in args) + sum(
        o.size * o.dtype.itemsize for o in outs
    )
    space = {"s": pltpu.SMEM, "v": pltpu.VMEM}
    fetched = [i for i, k in enumerate(kinds) if k in "hlqe"]
    stored = [i for i, k in enumerate(out_kinds) if k == "h"]
    room = [
        pltpu.VMEM(args[i].shape[1 if kinds[i] == "e" else 0 :], args[i].dtype) for i in fetched
    ]
    pieces = {"h": 1, "l": 1, "q": 4, "e": 4}
    n_sems = sum(pieces[kinds[i]] for i in fetched)
    out_room = [pltpu.VMEM(outs[i].shape, outs[i].dtype) for i in stored]

    def whole(*refs):
        ins, rest = list(refs[: len(args)]), refs[len(args) :]
        results, rest = list(rest[: len(outs)]), rest[len(outs) :]
        in_room, rest = rest[: len(room)], rest[len(room) :]
        result_room, rest = rest[: len(out_room)], rest[len(out_room) :]
        in_sem, out_sem, extra = rest[0], rest[1], rest[2:]
        late, now, order = [], [], []
        sem = 0
        for n, i in enumerate(fetched):
            kind = kinds[i]
            source = ins[i].at[ins[0][1]] if kind == "e" else ins[i]
            parts = pieces[kind]
            size = in_room[n].shape[0] // parts
            copies = []
            for p in range(parts):
                cut = pl.ds(p * size, size)
                copies.append(
                    pltpu.make_async_copy(source.at[cut], in_room[n].at[cut], in_sem.at[sem])
                )
                order.append((p, sem, copies[-1]))
                sem += 1
            if kind == "h":
                now.extend(copies)
            else:
                late.append([copy.wait for copy in copies])
            ins[i] = in_room[n]
        for _, _, copy in sorted(order, key=lambda o: o[:2]):
            copy.start()
        targets = list(results)
        for n, i in enumerate(stored):
            results[i] = result_room[n]
        for copy in now:
            copy.wait()
        if late:
            body(late, *ins, *results, *extra)
        else:
            body(*ins, *results, *extra)
        back = [
            pltpu.make_async_copy(result_room[n], targets[i], out_sem.at[n])
            for n, i in enumerate(stored)
        ]
        for copy in back:
            copy.start()
        for copy in back:
            copy.wait()

    return pl.pallas_call(
        whole,
        out_shape=outs,
        in_specs=[pl.BlockSpec(memory_space=space.get(k, pltpu.HBM)) for k in kinds],
        out_specs=[pl.BlockSpec(memory_space=space.get(k, pltpu.HBM)) for k in out_kinds],
        scratch_shapes=[
            *room,
            *out_room,
            pltpu.SemaphoreType.DMA((max(1, n_sems),)),
            pltpu.SemaphoreType.DMA((max(1, len(out_room)),)),
            *scratch,
        ],
        cost_estimate=pl.CostEstimate(flops=flops, bytes_accessed=moved, transcendentals=0),
        compiler_params=pltpu.CompilerParams(vmem_limit_bytes=mib * 2**20),
    )(*args)


def shaped(*dims, dtype=BF):
    return jax.ShapeDtypeStruct(dims, dtype)


def prepare(at, tokens, gain, wq, wf, wi, wo, dg, du, dd, spread_w, dense, t0, t1, t2, t3, held):
    x = at[2]
    for i, block in enumerate((dg, du, dd)):
        dense[i] = block[...]
    for i, block in enumerate((wq, wf, wi, wo)):
        width = block.shape[1]
        value = block[...]
        for z in range(spread_w.shape[0]):
            spread_w[z, :, i * width : (i + 1) * width] = value
    wide = tokens[...].astype(F32)
    wide = wide * lax.rsqrt(jnp.mean(wide * wide, axis=1, keepdims=True) + EPS) * gain[...]
    low = lax.broadcasted_iota(jnp.int32, (wide.shape[0], 128), 1) < 64

    def tile(i):
        return wide[:, i * 128 : (i + 1) * 128]

    for to in range(4):
        for k in range(4):
            a, b = tile(4 * k + to // 2), tile(4 * k + 2 + to // 2)
            if to % 2 == 0:
                value = jnp.where(low, a, pltpu.roll(b, 64, 1))
            else:
                value = jnp.where(low, pltpu.roll(a, 64, 1), b)
            held[to, :, k * 128 : (k + 1) * 128] = value.astype(BF)
    for d, out in enumerate((t0, t1, t2, t3)):
        out[...] = held[lax.rem(x + d, 4)]


def recur(wait, at, p0, p1, p2, p3, bound, gain, state, w_out, decay_out, key_out, value_out, keep, give, read):
    first = at[1] == 0
    seq = p0.shape[0]
    total = (
        p0[...].astype(F32) + p1[...].astype(F32) + p2[...].astype(F32) + p3[...].astype(F32)
    )
    total = total.astype(BF).astype(F32)
    query, forget, values, gate = (total[:, i * 128 : (i + 1) * 128] for i in range(4))
    forget = jax.nn.sigmoid(forget)
    low = bound[...]
    decay = low + (1.0 - low) * forget
    key = (1.0 - low) * (1.0 - forget)
    decay_out[...] = decay
    key_out[...] = key
    value_out[...] = values
    turned = jnp.transpose(query * decay)
    for b in range(seq):
        if b % (seq // 4) == 0:
            wait[0][b // (seq // 4)]()
        read[b : b + 1, :] = jnp.sum(turned[:, b : b + 1] * state[b], axis=0, keepdims=True)
    readout = read[...] + jnp.sum(query * key, axis=1, keepdims=True) * values
    readout = readout * lax.rsqrt(jnp.mean(readout * readout, axis=1, keepdims=True) + EPS)
    head = (readout * gain[...] * silu(gate)).astype(BF)
    wait[1][0]()
    cols = keep.shape[2]
    for y in range(keep.shape[0]):
        cut = slice(2 * y * cols, (2 * y + 1) * cols)
        cut_next = slice((2 * y + 1) * cols, (2 * y + 2) * cols)
        even = dot(head, w_out[:, cut]).astype(BF)
        odd = dot(head, w_out[:, cut_next]).astype(BF)
        keep[y] = jnp.where(first, even, odd)
        give[y] = jnp.where(first, odd, even)


def dispatch(at, heads, tokens, slots, resid, own, lines):
    cols = resid.shape[1]
    half = cols // 2
    seq = resid.shape[0]
    start = pl.multiple_of((2 * at[0] + at[1]) * cols, cols)
    total = tokens[:, pl.ds(start, cols)].astype(F32)
    for i in range(heads.shape[0]):
        total = total + heads[i].astype(F32)
    resid[...] = total
    rows = total.astype(BF)
    own[...] = rows
    chunk = 192
    place = lax.broadcasted_iota(jnp.int32, (chunk, seq), 0)
    for h in range(2):
        shifted = place - 12 * h
        dense = shifted == slots[4:5, :]
        for z in range(lines.shape[0] // chunk):
            here = shifted + z * chunk
            hit = dense
            for k in range(4):
                hit = hit | (here == slots[k : k + 1, :])
            part = dot(jnp.where(hit, 1.0, 0.0).astype(BF), rows[:, h * half : (h + 1) * half])
            if h == 0:
                lines[z * chunk : (z + 1) * chunk, :] = part.astype(BF)
            else:
                before = lines[z * chunk : (z + 1) * chunk, :].astype(F32)
                lines[z * chunk : (z + 1) * chunk, :] = (before + part).astype(BF)


def finish(lines, within, slots, weight, resid, shared, shared_other, mix, out):
    seq, cols = out.shape
    half = cols // 2
    place = lax.broadcasted_iota(jnp.int32, (seq, lines.shape[0]), 1)
    gate = jax.nn.sigmoid(mix[...])
    base = resid[...] + shared[...] + shared_other[...].astype(F32)
    for h in range(2):
        routed = jnp.zeros(place.shape, F32)
        for k in range(4):
            routed = jnp.where(place == slots[:, k : k + 1] + 12 * h, weight[:, k : k + 1], routed)
        dense = jnp.where(within[...] == slots[:, 4:5] + 12 * h, 1.0, 0.0)
        cut = slice(h * half, (h + 1) * half)
        total = base[:, cut] + dot(routed.astype(BF), lines[...])
        total = total + gate[:, cut] * dot(dense.astype(BF), lines[...])
        out[:, cut] = total.astype(BF)


def unpack_rows(at, line_of, lines, own, other, both, dense):
    first = at[1] == 0
    group = line_of.shape[1]
    count = dense.shape[1]
    cols = dense.shape[2]
    half = cols // 2
    part = group // 8
    groups = lines.shape[0] // group
    move = jnp.where(
        lax.broadcasted_iota(jnp.int32, (group, group), 0) == line_of[...], 1.0, 0.0
    ).astype(BF)
    mine, others = own[...], other[...]
    both_rows = [
        jnp.where(first, mine, others),
        jnp.where(first, others, mine),
    ]
    for g in range(groups):
        rows = dot(move, lines[g * group : (g + 1) * group, :]).astype(BF)
        here = slice(g * part, (g + 1) * part)
        for side in range(2):
            for h in range(2):
                base = (side * 2 + h) * 2 * part
                at_col = side * cols + h * half
                for copy in range(both.shape[0]):
                    both[copy, here, at_col : at_col + half] = rows[base : base + part]
                dense[side, here, h * half : (h + 1) * half] = rows[base + part : base + 2 * part]
    for side in range(2):
        for copy in range(both.shape[0]):
            both[copy, count:, side * cols : (side + 1) * cols] = both_rows[side]


def dense_first_half(wait, at, rows, gain, *refs):
    y, c = at[0], at[1]
    own_w, other_w, outs = refs[:4], refs[4:8], refs[8:]
    ny = len(outs)
    size = rows.shape[1] // ny
    cols = rows.shape[2]

    def turned(side):
        return jnp.concatenate(
            [
                rows[side, pl.ds(pl.multiple_of(lax.rem(y + d, ny) * size, size), size), :]
                for d in range(ny)
            ],
            axis=0,
        ).astype(F32)

    own, other = turned(c), turned(1 - c)
    square = jnp.sum(own * own + other * other, axis=1, keepdims=True)
    high = square.astype(BF).astype(F32)
    low = square - high
    own = (own * gain[pl.ds(2 * y + c, 1), :]).astype(BF)
    other = (other * gain[pl.ds(2 * y + 1 - c, 1), :]).astype(BF)
    for i in range(4):
        wait[i][0]()
        wait[4 + i][0]()
        for kind in range(2):
            value = (dot(own, own_w[i][kind]) + dot(other, other_w[i][kind])).astype(BF)
            at_col = (kind * 4 + i) * cols
            for d in range(ny):
                outs[d][:, at_col : at_col + cols] = value[d * size : (d + 1) * size]
    lane = lax.broadcasted_iota(jnp.int32, (square.shape[0], 128), 1)
    both = jnp.where(lane < 64, high, low).astype(BF)
    for d in range(ny):
        outs[d][:, 8 * cols : 8 * cols + 128] = both[d * size : (d + 1) * size]


def dense_activation(a, b, c, d, out):
    width = out.shape[1]
    features = 2048

    def summed(cut):
        return (
            a[:, cut].astype(F32) + b[:, cut].astype(F32) + c[:, cut].astype(F32) + d[:, cut].astype(F32)
        )

    square = summed(slice(2 * width, 2 * width + 128))
    total = square[:, 0:1] + square[:, 64:65]
    scale = lax.rsqrt(total / features + EPS)
    gate = summed(slice(0, width)) * scale
    up = summed(slice(width, 2 * width)) * scale
    out[...] = (silu(gate) * up).astype(BF)


def dense_second_half(wait, at, *refs):
    y = at[0]
    hidden, own_w, other_w, out = refs[:4], refs[4:8], refs[8:12], refs[12]
    ny = len(hidden)
    size, cols = hidden[0].shape[0], out.shape[2]
    rows = jnp.concatenate([h[...] for h in hidden], axis=0)
    for side, weights in enumerate((own_w, other_w)):
        total = None
        for i in range(4):
            wait[4 * side + i][0]()
            term = dot(rows[:, i * cols : (i + 1) * cols], weights[i][2])
            total = term if total is None else total + term
        total = total.astype(BF)
        for d in range(ny):
            start = pl.multiple_of(lax.rem(y + ny - d, ny) * size, size)
            out[side, pl.ds(start, size), :] = total[d * size : (d + 1) * size]


def experts_and_shared(
    wait, at, whole, gain, gate, gate_other, up, up_other, down, down_other,
    shared_gate, shared_up, shared_down, parts,
):
    ny, lines, block = whole.shape
    count = lines - 48
    half = gate.shape[1]
    square = jnp.zeros((lines, 1), F32)
    gate_pre = up_pre = shared_pre = None

    def more(total, term):
        return term if total is None else total + term

    for i in range(ny):
        cut = slice(i * block, (i + 1) * block)
        for k in (0, 1, 2, 3, 4, 7, 8):
            wait[k][i]()
        value = whole[i].astype(F32)
        square = square + jnp.sum(value * value, axis=1, keepdims=True)
        rows = (value * gain[:, cut]).astype(BF)
        gates = jnp.concatenate([gate[cut, :], gate_other[cut, :]], axis=1)
        ups = jnp.concatenate([up[cut, :], up_other[cut, :]], axis=1)
        shared = jnp.concatenate([shared_gate[cut, :], shared_up[cut, :]], axis=1)
        gate_pre = more(gate_pre, dot(rows[:count], gates))
        up_pre = more(up_pre, dot(rows[:count], ups))
        shared_pre = more(shared_pre, dot(rows[count:], shared))
    scale = lax.rsqrt(square / (ny * block) + EPS)
    hidden = (silu(gate_pre * scale[:count]) * (up_pre * scale[:count])).astype(BF)
    shared_pre = shared_pre * scale[count:]
    shared_hidden = (silu(shared_pre[:, :half]) * shared_pre[:, half:]).astype(BF)
    for k in (5, 6, 9):
        for done in wait[k]:
            done()
    for i in range(ny):
        cut = slice(i * block, (i + 1) * block)
        downs = jnp.concatenate([down[:, cut], down_other[:, cut]], axis=0)
        parts[i, :count, :] = dot(hidden, downs).astype(BF)
        parts[i, count:, :] = dot(shared_hidden, shared_down[:, cut]).astype(BF)


def pack_lines(at, line_of, parts, dense, lines, shared_own, shared_send):
    first = at[1] == 0
    group = line_of.shape[0]
    part = group // 8
    cols = dense.shape[2]
    half = cols // 2
    count = dense.shape[1]
    groups = lines.shape[0] // group
    move = jnp.where(
        lax.broadcasted_iota(jnp.int32, (group, group), 1) == line_of[...], 1.0, 0.0
    ).astype(BF)
    total = parts[0].astype(F32)
    for i in range(1, parts.shape[0]):
        total = total + parts[i].astype(F32)
    routed = total[:count].astype(BF)
    shared = total[count:]
    shared_own[...] = jnp.where(first, shared[:, :cols], shared[:, cols:])
    shared_send[...] = jnp.where(first, shared[:, cols:], shared[:, :cols]).astype(BF)
    for g in range(groups):
        here = slice(g * part, (g + 1) * part)
        own, other = dense[0, here, :], dense[1, here, :]
        sides = [jnp.where(first, own, other), jnp.where(first, other, own)]
        stack = []
        for side in range(2):
            for h in range(2):
                at_col = side * cols + h * half
                stack.append(routed[here, at_col : at_col + half])
                stack.append(sides[side][:, h * half : (h + 1) * half])
        rows = jnp.concatenate(stack, axis=0)
        lines[g * group : (g + 1) * group, :] = dot(move, rows).astype(BF)


def step(
    tokens,
    state,
    norm_gain,
    w_query,
    w_forget,
    w_input,
    w_outgate,
    lower_bound,
    head_gain,
    w_output,
    ffn_gain,
    route_ids,
    route_weight,
    expert_gate,
    expert_up,
    expert_down,
    shared_gate,
    shared_up,
    shared_down,
    dense_gate,
    dense_up,
    dense_down,
    dense_mix,
):
    nz, nx, ny, nc = (lax.axis_size(a) for a in ("z", "x", "y", "c"))
    x, y, c = (lax.axis_index(a) for a in ("x", "y", "c"))
    seq, width = tokens.shape
    rows_w, chan = w_query.shape
    head_dim = state.shape[2]
    cols = width // (ny * nc)

    at = jnp.stack([y, c, x]).astype(jnp.int32)

    topk = route_ids.shape[1]
    experts = nz * nx * nc
    cap = max(2, 2 * seq * topk // experts)
    slots = 2 * cap
    half = cols // 2
    flat_ids = route_ids.reshape(-1)
    onehot = (flat_ids[:, None] == jnp.arange(experts, dtype=jnp.int32)[None, :]).astype(jnp.int32)
    rank = jnp.sum((jnp.cumsum(onehot, axis=0) - onehot) * onehot, axis=1)
    lines_of = (flat_ids * (2 * slots) + rank).reshape(seq, topk)
    token_ids = jnp.arange(seq, dtype=jnp.int32)
    dense_of = (token_ids // cap) * (2 * slots) + cap + token_ids % cap
    slot_cols = jnp.concatenate(
        [lines_of, dense_of[:, None], jnp.zeros((seq, 8 - topk - 1), jnp.int32)], axis=1
    )
    slot_rows = slot_cols.T
    within = (jnp.arange(experts * 2 * slots, dtype=jnp.int32) % (nx * nc * 2 * slots))[None, :]

    spread_w, dense_block, *columns = call(
        prepare,
        [shaped(nz, rows_w, 4 * chan), shaped(3, *dense_gate.shape)]
        + [shaped(seq, nz * rows_w)] * nx,
        10**6,
        "shhhhhhhhh hhhhhh",
        at,
        tokens,
        norm_gain.reshape(1, width),
        w_query,
        w_forget,
        w_input,
        w_outgate,
        dense_gate,
        dense_up,
        dense_down,
        mib=58,
        scratch=[pltpu.VMEM((nx, seq, nz * rows_w), BF)],
    )
    weights = swap(spread_w, "z").reshape(nz * rows_w, 4 * chan)
    mine = [columns[0]] + [shift(columns[d], "x", d) for d in range(1, nx)]
    part = dot(jnp.concatenate(mine, axis=0), weights).astype(BF)
    part = part.reshape(nx, seq, 4 * chan)
    pieces = [part[0]] + [shift(part[d], "x", -d) for d in range(1, nx)]

    dense_own = [dense_block] + [shift(dense_block, "x", d) for d in range(1, nx)]
    dense_other = [partner(block) for block in dense_own]
    gate_other, up_other, down_other = (
        partner(pick(stack, 1 - c)) for stack in (expert_gate, expert_up, expert_down)
    )

    decay, keygate, values, keep, give = call(
        recur,
        [shaped(seq, chan, dtype=F32)] * 3 + [shaped(ny, seq, cols)] * 2,
        4 * state.size,
        "shvvvhhql hhhvh",
        at,
        *pieces,
        lower_bound.reshape(1, chan),
        head_gain.reshape(1, chan),
        state.reshape(seq, head_dim, head_dim),
        w_output,
        scratch=[pltpu.VMEM((seq, head_dim), F32)],
    )
    shape = (seq, 1, head_dim)
    new_state = (
        decay.reshape(shape)[..., None] * state
        + keygate.reshape(shape)[..., None] * values.reshape(shape)[:, :, None, :]
    )

    pair = (keep.astype(F32) + partner(give).astype(F32)).astype(BF)
    heads = swap(pair, "y")
    resid, own, outgoing = call(
        dispatch,
        [
            shaped(seq, cols, dtype=F32),
            shaped(seq, cols),
            shaped(experts * 2 * slots, half),
        ],
        4 * experts * 2 * slots * seq * half,
        "svhh hhh",
        at,
        heads,
        tokens,
        slot_rows,
    )
    arrived = swap(outgoing.reshape(experts, 2 * slots, half), HUB)
    other = partner(own)
    count = nz * nx * cap

    group = 8 * nc * 2 * slots
    lines = jnp.arange(group, dtype=jnp.int32)
    source, rest = lines // (4 * slots), lines % (4 * slots)
    side, h, kind, r = (
        rest // (2 * slots),
        rest // slots % 2,
        rest // cap % 2,
        rest % cap,
    )
    line_of = ((side * 2 + h) * 2 + kind) * (8 * cap) + source * cap + r
    both, dense_rows = call(
        unpack_rows,
        [shaped(ny, count + seq, nc * cols), shaped(nc, count, cols)],
        4 * 2 * group * group * half,
        "shvhv hh",
        at,
        line_of.reshape(1, group),
        arrived.reshape(-1, half),
        own,
        other,
    )
    whole = swap(both, "y")

    hidden_width = nx * dense_gate.shape[1]
    quarter = count // ny
    pre = call(
        dense_first_half,
        [shaped(quarter, 2 * hidden_width + 128)] * ny,
        2 * count * nc * cols * 2 * hidden_width,
        "shhllllllll hhhh",
        at,
        dense_rows,
        ffn_gain.reshape(ny * nc, cols),
        *dense_own,
        *dense_other,
    )
    pre = [pre[0]] + [shift(pre[d], "y", d) for d in range(1, ny)]
    (hidden,) = call(
        dense_activation, [shaped(quarter, hidden_width)], 10**6, "hvvv h", *pre
    )
    hidden = [hidden] + [shift(hidden, "y", d) for d in range(1, ny)]
    (dense_part,) = call(
        dense_second_half,
        [shaped(nc, count, cols)],
        2 * count * nc * cols * hidden_width,
        "shvvvllllllll h",
        at,
        *hidden,
        *dense_own,
        *dense_other,
    )

    (parts,) = call(
        experts_and_shared,
        [shaped(ny, count + seq, nc * cols)],
        2 * 3 * (count * 2 + seq) * width * expert_gate.shape[2],
        "sqheqeqeqqqq h",
        at,
        whole,
        ffn_gain.reshape(1, width),
        expert_gate,
        gate_other,
        expert_up,
        up_other,
        expert_down,
        down_other,
        shared_gate,
        shared_up,
        shared_down,
    )
    parts = swap(parts, "y")
    back, shared_own, shared_send = call(
        pack_lines,
        [
            shaped(experts * 2 * slots, half),
            shaped(seq, cols, dtype=F32),
            shaped(seq, cols),
        ],
        4 * 2 * group * group * half,
        "shvh hhh",
        at,
        line_of.reshape(group, 1),
        parts,
        dense_part,
    )

    results = swap(back.reshape(experts, 2 * slots, half), HUB)
    (mixed,) = call(
        finish,
        [shaped(seq, cols)],
        8 * experts * 2 * slots * seq * half,
        "vhhhhhvh h",
        results.reshape(experts * 2 * slots, half),
        within,
        slot_cols,
        route_weight,
        resid,
        shared_own,
        partner(shared_send),
        dense_mix.reshape(1, cols),
    )
    return (mixed, new_state)


def solution(mesh):
    torus = Mesh(mesh.devices.reshape(8, 4, 4, 2), ("z", "x", "y", "c"))
    return jax.shard_map(
        step,
        mesh=torus,
        in_specs=(
            P(EP, None),
            P(EP, TP, None, None),
            P(),
            P(EP, TP),
            P(EP, TP),
            P(EP, TP),
            P(EP, TP),
            P(TP),
            P(TP),
            P(TP, None),
            P(),
            P(EP, None),
            P(EP, None),
            P(EP, None, TP),
            P(EP, None, TP),
            P(EP, TP, None),
            P(None, TP),
            P(None, TP),
            P(TP, None),
            P(TP, EP),
            P(TP, EP),
            P(EP, TP),
            P(TP),
        ),
        out_specs=(P(EP, TP), P(EP, TP, None, None)),
        check_vma=False,
    )
```

```python
import jax
import jax.numpy as jnp
from jax import lax
from jax.experimental import pallas as pl
from jax.experimental.pallas import tpu as pltpu
from jax.sharding import Mesh
from jax.sharding import PartitionSpec as P

EP = ("z", "x")
TP = ("y", "c")
HUB = ("z", "x", "c")


EPS = 1e-06
BF = jnp.bfloat16
F32 = jnp.float32


def swap(x, axis):
    return lax.all_to_all(x, axis, split_axis=0, concat_axis=0, tiled=True)


def partner(x):
    return lax.ppermute(x, "c", [(0, 1), (1, 0)])


def shift(x, axis, by):
    size = lax.axis_size(axis)
    return lax.ppermute(x, axis, [(i, (i + by) % size) for i in range(size)])


def pick(x, index):
    return lax.dynamic_index_in_dim(x, index, 0, keepdims=False)


def dot(a, b):
    return jnp.dot(a, b, preferred_element_type=F32)


def silu(x):
    return x * jax.nn.sigmoid(x)


def call(body, outs, flops, kinds, *args, mib=52, scratch=()):
    kinds, out_kinds = kinds.split()
    moved = sum(a.size * a.dtype.itemsize for a in args) + sum(
        o.size * o.dtype.itemsize for o in outs
    )
    space = {"s": pltpu.SMEM, "v": pltpu.VMEM}
    fetched = [i for i, k in enumerate(kinds) if k in "hlqegd"]
    stored = [i for i, k in enumerate(out_kinds) if k == "h"]

    def held(i):
        shape = args[i].shape
        return {"e": shape[1:], "d": shape[1:], "g": (2, *shape[1:])}.get(kinds[i], shape)

    room = [pltpu.VMEM(held(i), args[i].dtype) for i in fetched]
    pieces = {"h": 1, "l": 1, "q": 4, "e": 4, "g": 1, "d": 1}
    n_sems = sum(pieces[kinds[i]] for i in fetched)
    out_room = [pltpu.VMEM(outs[i].shape, outs[i].dtype) for i in stored]

    def whole(*refs):
        ins, rest = list(refs[: len(args)]), refs[len(args) :]
        results, rest = list(rest[: len(outs)]), rest[len(outs) :]
        in_room, rest = rest[: len(room)], rest[len(room) :]
        result_room, rest = rest[: len(out_room)], rest[len(out_room) :]
        in_sem, out_sem, extra = rest[0], rest[1], rest[2:]
        late, now, order = [], [], []
        sem = 0
        for n, i in enumerate(fetched):
            kind = kinds[i]
            source = ins[i]
            if kind == "e":
                source = source.at[ins[0][1]]
            elif kind == "d":
                source = source.at[2]
            parts = pieces[kind]
            size = in_room[n].shape[0] // parts
            copies = []
            for p in range(parts):
                cut = pl.ds(p * size, size)
                copies.append(
                    pltpu.make_async_copy(source.at[cut], in_room[n].at[cut], in_sem.at[sem])
                )
                order.append((p, sem, copies[-1]))
                sem += 1
            if kind == "h":
                now.extend(copies)
            else:
                late.append([copy.wait for copy in copies])
            ins[i] = in_room[n]
        for _, _, copy in sorted(order, key=lambda o: o[:2]):
            copy.start()
        targets = list(results)
        for n, i in enumerate(stored):
            results[i] = result_room[n]
        for copy in now:
            copy.wait()
        if late:
            body(late, *ins, *results, *extra)
        else:
            body(*ins, *results, *extra)
        back = [
            pltpu.make_async_copy(result_room[n], targets[i], out_sem.at[n])
            for n, i in enumerate(stored)
        ]
        for copy in back:
            copy.start()
        for copy in back:
            copy.wait()

    return pl.pallas_call(
        whole,
        out_shape=outs,
        in_specs=[pl.BlockSpec(memory_space=space.get(k, pltpu.HBM)) for k in kinds],
        out_specs=[pl.BlockSpec(memory_space=space.get(k, pltpu.HBM)) for k in out_kinds],
        scratch_shapes=[
            *room,
            *out_room,
            pltpu.SemaphoreType.DMA((max(1, n_sems),)),
            pltpu.SemaphoreType.DMA((max(1, len(out_room)),)),
            *scratch,
        ],
        cost_estimate=pl.CostEstimate(flops=flops, bytes_accessed=moved, transcendentals=0),
        compiler_params=pltpu.CompilerParams(vmem_limit_bytes=mib * 2**20),
    )(*args)


def shaped(*dims, dtype=BF):
    return jax.ShapeDtypeStruct(dims, dtype)


def copies(wq, wf, wi, wo, spread_w):
    for i, block in enumerate((wq, wf, wi, wo)):
        width = block.shape[1]
        value = block[...]
        for z in range(spread_w.shape[0]):
            spread_w[z, :, i * width : (i + 1) * width] = value


def prepare(at, tokens, gain, dg, du, dd, dense, t0, t1, t2, t3, held):
    x = at[2]
    for i, block in enumerate((dg, du, dd)):
        dense[i] = block[...]
    wide = tokens[...].astype(F32)
    wide = wide * lax.rsqrt(jnp.mean(wide * wide, axis=1, keepdims=True) + EPS) * gain[...]
    low = lax.broadcasted_iota(jnp.int32, (wide.shape[0], 128), 1) < 64

    def tile(i):
        return wide[:, i * 128 : (i + 1) * 128]

    for to in range(4):
        for k in range(4):
            a, b = tile(4 * k + to // 2), tile(4 * k + 2 + to // 2)
            if to % 2 == 0:
                value = jnp.where(low, a, pltpu.roll(b, 64, 1))
            else:
                value = jnp.where(low, pltpu.roll(a, 64, 1), b)
            held[to, :, k * 128 : (k + 1) * 128] = value.astype(BF)
    for d, out in enumerate((t0, t1, t2, t3)):
        out[...] = held[lax.rem(x + d, 4)]


def recur(wait, at, p0, p1, p2, p3, bound, gain, state, w_out, decay_out, key_out, value_out, keep, give, read):
    first = at[1] == 0
    seq = p0.shape[0]
    total = (
        p0[...].astype(F32) + p1[...].astype(F32) + p2[...].astype(F32) + p3[...].astype(F32)
    )
    total = total.astype(BF).astype(F32)
    query, forget, values, gate = (total[:, i * 128 : (i + 1) * 128] for i in range(4))
    forget = jax.nn.sigmoid(forget)
    low = bound[...]
    decay = low + (1.0 - low) * forget
    key = (1.0 - low) * (1.0 - forget)
    decay_out[...] = decay
    key_out[...] = key
    value_out[...] = values
    turned = jnp.transpose(query * decay)
    for b in range(seq):
        if b % (seq // 4) == 0:
            wait[0][b // (seq // 4)]()
        read[b : b + 1, :] = jnp.sum(turned[:, b : b + 1] * state[b], axis=0, keepdims=True)
    readout = read[...] + jnp.sum(query * key, axis=1, keepdims=True) * values
    readout = readout * lax.rsqrt(jnp.mean(readout * readout, axis=1, keepdims=True) + EPS)
    head = (readout * gain[...] * silu(gate)).astype(BF)
    wait[1][0]()
    cols = keep.shape[2]
    for y in range(keep.shape[0]):
        cut = slice(2 * y * cols, (2 * y + 1) * cols)
        cut_next = slice((2 * y + 1) * cols, (2 * y + 2) * cols)
        even = dot(head, w_out[:, cut]).astype(BF)
        odd = dot(head, w_out[:, cut_next]).astype(BF)
        keep[y] = jnp.where(first, even, odd)
        give[y] = jnp.where(first, odd, even)


def dispatch(at, heads, tokens, slots, resid, own, lines):
    cols = resid.shape[1]
    half = cols // 2
    seq = resid.shape[0]
    start = pl.multiple_of((2 * at[0] + at[1]) * cols, cols)
    total = tokens[:, pl.ds(start, cols)].astype(F32)
    for i in range(heads.shape[0]):
        total = total + heads[i].astype(F32)
    resid[...] = total
    rows = total.astype(BF)
    own[...] = rows
    chunk = 192
    place = lax.broadcasted_iota(jnp.int32, (chunk, seq), 0)
    for h in range(2):
        shifted = place - 12 * h
        dense = shifted == slots[4:5, :]
        for z in range(lines.shape[0] // chunk):
            here = shifted + z * chunk
            hit = dense
            for k in range(4):
                hit = hit | (here == slots[k : k + 1, :])
            part = dot(jnp.where(hit, 1.0, 0.0).astype(BF), rows[:, h * half : (h + 1) * half])
            if h == 0:
                lines[z * chunk : (z + 1) * chunk, :] = part.astype(BF)
            else:
                before = lines[z * chunk : (z + 1) * chunk, :].astype(F32)
                lines[z * chunk : (z + 1) * chunk, :] = (before + part).astype(BF)


def finish(lines, within, slots, weight, resid, shared, shared_other, mix, out):
    seq, cols = out.shape
    half = cols // 2
    place = lax.broadcasted_iota(jnp.int32, (seq, lines.shape[0]), 1)
    gate = jax.nn.sigmoid(mix[...])
    base = resid[...] + shared[...] + shared_other[...].astype(F32)
    for h in range(2):
        routed = jnp.zeros(place.shape, F32)
        for k in range(4):
            routed = jnp.where(place == slots[:, k : k + 1] + 12 * h, weight[:, k : k + 1], routed)
        dense = jnp.where(within[...] == slots[:, 4:5] + 12 * h, 1.0, 0.0)
        cut = slice(h * half, (h + 1) * half)
        total = base[:, cut] + dot(routed.astype(BF), lines[...])
        total = total + gate[:, cut] * dot(dense.astype(BF), lines[...])
        out[:, cut] = total.astype(BF)


def unpack_rows(at, line_of, lines, own, other, both, dense):
    first = at[1] == 0
    group = line_of.shape[1]
    count = dense.shape[1]
    cols = dense.shape[2]
    half = cols // 2
    part = group // 8
    groups = lines.shape[0] // group
    move = jnp.where(
        lax.broadcasted_iota(jnp.int32, (group, group), 0) == line_of[...], 1.0, 0.0
    ).astype(BF)
    mine, others = own[...], other[...]
    both_rows = [
        jnp.where(first, mine, others),
        jnp.where(first, others, mine),
    ]
    for g in range(groups):
        rows = dot(move, lines[g * group : (g + 1) * group, :]).astype(BF)
        here = slice(g * part, (g + 1) * part)
        for side in range(2):
            for h in range(2):
                base = (side * 2 + h) * 2 * part
                at_col = side * cols + h * half
                for copy in range(both.shape[0]):
                    both[copy, here, at_col : at_col + half] = rows[base : base + part]
                dense[side, here, h * half : (h + 1) * half] = rows[base + part : base + 2 * part]
    for side in range(2):
        for copy in range(both.shape[0]):
            both[copy, count:, side * cols : (side + 1) * cols] = both_rows[side]


def dense_first_half(wait, at, rows, gain, *refs):
    y, c = at[0], at[1]
    own_w, other_w, outs = refs[:4], refs[4:8], refs[8:]
    ny = len(outs)
    size = rows.shape[1] // ny
    cols = rows.shape[2]

    def turned(side):
        return jnp.concatenate(
            [
                rows[side, pl.ds(pl.multiple_of(lax.rem(y + d, ny) * size, size), size), :]
                for d in range(ny)
            ],
            axis=0,
        ).astype(F32)

    own, other = turned(c), turned(1 - c)
    square = jnp.sum(own * own + other * other, axis=1, keepdims=True)
    high = square.astype(BF).astype(F32)
    low = square - high
    own = (own * gain[pl.ds(2 * y + c, 1), :]).astype(BF)
    other = (other * gain[pl.ds(2 * y + 1 - c, 1), :]).astype(BF)
    for i in range(4):
        wait[i][0]()
        wait[4 + i][0]()
        for kind in range(2):
            value = (dot(own, own_w[i][kind]) + dot(other, other_w[i][kind])).astype(BF)
            at_col = (kind * 4 + i) * cols
            for d in range(ny):
                outs[d][:, at_col : at_col + cols] = value[d * size : (d + 1) * size]
    lane = lax.broadcasted_iota(jnp.int32, (square.shape[0], 128), 1)
    both = jnp.where(lane < 64, high, low).astype(BF)
    for d in range(ny):
        outs[d][:, 8 * cols : 8 * cols + 128] = both[d * size : (d + 1) * size]


def experts_and_shared(
    wait, at, whole, gain, gate, gate_other, up, up_other, down, down_other,
    shared_gate, shared_up, shared_down, p0, p1, p2, p3, parts,
):
    ny, lines, block = whole.shape
    count = lines - 48
    half = gate.shape[1]
    square = jnp.zeros((lines, 1), F32)
    gate_pre = up_pre = shared_pre = None

    def more(total, term):
        return term if total is None else total + term

    for i in range(ny):
        cut = slice(i * block, (i + 1) * block)
        for k in (0, 1, 2, 3, 4, 7, 8):
            wait[k][i]()
        value = whole[i].astype(F32)
        square = square + jnp.sum(value * value, axis=1, keepdims=True)
        rows = (value * gain[:, cut]).astype(BF)
        gates = jnp.concatenate([gate[cut, :], gate_other[cut, :]], axis=1)
        ups = jnp.concatenate([up[cut, :], up_other[cut, :]], axis=1)
        shared = jnp.concatenate([shared_gate[cut, :], shared_up[cut, :]], axis=1)
        gate_pre = more(gate_pre, dot(rows[:count], gates))
        up_pre = more(up_pre, dot(rows[:count], ups))
        shared_pre = more(shared_pre, dot(rows[count:], shared))
    scale = lax.rsqrt(square / (ny * block) + EPS)
    hidden = (silu(gate_pre * scale[:count]) * (up_pre * scale[:count])).astype(BF)
    shared_pre = shared_pre * scale[count:]
    shared_hidden = (silu(shared_pre[:, :half]) * shared_pre[:, half:]).astype(BF)
    for k in (5, 6, 9):
        for done in wait[k]:
            done()
    for i in range(ny):
        cut = slice(i * block, (i + 1) * block)
        downs = jnp.concatenate([down[:, cut], down_other[:, cut]], axis=0)
        parts[i, :count, :] = dot(hidden, downs).astype(BF)
        parts[i, count:lines, :] = dot(shared_hidden, shared_down[:, cut]).astype(BF)

    width = 2 * block

    def summed(at_col, size):
        part = slice(at_col, at_col + size)
        return sum(p[:, part].astype(F32) for p in (p0, p1, p2, p3))

    tail = summed(2 * width, 128)
    dense_scale = lax.rsqrt((tail[:, 0:1] + tail[:, 64:65]) / (ny * block) + EPS)
    for j in range(2):
        dense_gate = summed(j * block, block) * dense_scale
        dense_up = summed(width + j * block, block) * dense_scale
        dense_hidden = (silu(dense_gate) * dense_up).astype(BF)
        start = lines + j * p0.shape[0]
        for i in range(ny):
            parts[i, start : start + p0.shape[0], :] = dense_hidden


def pack_lines(wait, at, line_of, parts, *refs):
    own_w, other_w, (lines, shared_own, shared_send) = refs[:4], refs[4:8], refs[8:]
    first = at[1] == 0
    group = line_of.shape[0]
    part = group // 8
    groups = lines.shape[0] // group
    count = part * groups
    cols = shared_own.shape[1]
    half = cols // 2
    seq = shared_own.shape[0]
    move = jnp.where(
        lax.broadcasted_iota(jnp.int32, (group, group), 1) == line_of[...], 1.0, 0.0
    ).astype(BF)
    ny = parts.shape[0]
    total = parts[0, : count + seq].astype(F32)
    for i in range(1, ny):
        total = total + parts[i, : count + seq].astype(F32)
    routed = total[:count].astype(BF)
    shared = total[count:]
    shared_own[...] = jnp.where(first, shared[:, :cols], shared[:, cols:])
    shared_send[...] = jnp.where(first, shared[:, cols:], shared[:, :cols]).astype(BF)
    size = count // ny
    hidden = [
        jnp.concatenate([parts[i, start : start + size, :] for i in range(ny)], axis=0)
        for start in (count + seq, count + seq + size)
    ]
    dense = []
    for side, weights in enumerate((own_w, other_w)):
        value = None
        for i in range(4):
            wait[4 * side + i][0]()
            at_col = i % 2 * cols
            term = dot(hidden[i // 2][:, at_col : at_col + cols], weights[i][...])
            value = term if value is None else value + term
        dense.append(value.astype(BF))
    for g in range(groups):
        here = slice(g * part, (g + 1) * part)
        own, other = dense[0][here], dense[1][here]
        sides = [jnp.where(first, own, other), jnp.where(first, other, own)]
        stack = []
        for side in range(2):
            for h in range(2):
                at_col = side * cols + h * half
                stack.append(routed[here, at_col : at_col + half])
                stack.append(sides[side][:, h * half : (h + 1) * half])
        rows = jnp.concatenate(stack, axis=0)
        lines[g * group : (g + 1) * group, :] = dot(move, rows).astype(BF)


def step(
    tokens,
    state,
    norm_gain,
    w_query,
    w_forget,
    w_input,
    w_outgate,
    lower_bound,
    head_gain,
    w_output,
    ffn_gain,
    route_ids,
    route_weight,
    expert_gate,
    expert_up,
    expert_down,
    shared_gate,
    shared_up,
    shared_down,
    dense_gate,
    dense_up,
    dense_down,
    dense_mix,
):
    nz, nx, ny, nc = (lax.axis_size(a) for a in ("z", "x", "y", "c"))
    x, y, c = (lax.axis_index(a) for a in ("x", "y", "c"))
    seq, width = tokens.shape
    rows_w, chan = w_query.shape
    head_dim = state.shape[2]
    cols = width // (ny * nc)

    at = jnp.stack([y, c, x]).astype(jnp.int32)

    topk = route_ids.shape[1]
    experts = nz * nx * nc
    cap = max(2, 2 * seq * topk // experts)
    slots = 2 * cap
    half = cols // 2
    flat_ids = route_ids.reshape(-1)
    onehot = (flat_ids[:, None] == jnp.arange(experts, dtype=jnp.int32)[None, :]).astype(jnp.int32)
    rank = jnp.sum((jnp.cumsum(onehot, axis=0) - onehot) * onehot, axis=1)
    lines_of = (flat_ids * (2 * slots) + rank).reshape(seq, topk)
    token_ids = jnp.arange(seq, dtype=jnp.int32)
    dense_of = (token_ids // cap) * (2 * slots) + cap + token_ids % cap
    slot_cols = jnp.concatenate(
        [lines_of, dense_of[:, None], jnp.zeros((seq, 8 - topk - 1), jnp.int32)], axis=1
    )
    slot_rows = slot_cols.T
    within = (jnp.arange(experts * 2 * slots, dtype=jnp.int32) % (nx * nc * 2 * slots))[None, :]

    (spread_w,) = call(
        copies,
        [shaped(nz, rows_w, 4 * chan)],
        10**6,
        "hhhh h",
        w_query,
        w_forget,
        w_input,
        w_outgate,
        mib=58,
    )
    weights = swap(spread_w, "z").reshape(nz * rows_w, 4 * chan)
    dense_block, *columns = call(
        prepare,
        [shaped(3, *dense_gate.shape)] + [shaped(seq, nz * rows_w)] * nx,
        10**6,
        "shhhhh hhhhh",
        at,
        tokens,
        norm_gain.reshape(1, width),
        dense_gate,
        dense_up,
        dense_down,
        scratch=[pltpu.VMEM((nx, seq, nz * rows_w), BF)],
    )
    mine = [columns[0]] + [shift(columns[d], "x", d) for d in range(1, nx)]
    part = dot(jnp.concatenate(mine, axis=0), weights).astype(BF)
    part = part.reshape(nx, seq, 4 * chan)
    pieces = [part[0]] + [shift(part[d], "x", -d) for d in range(1, nx)]

    dense_own = [dense_block] + [shift(dense_block, "x", d) for d in range(1, nx)]
    dense_other = [partner(block) for block in dense_own]
    gate_other, up_other, down_other = (
        partner(pick(stack, 1 - c)) for stack in (expert_gate, expert_up, expert_down)
    )

    decay, keygate, values, keep, give = call(
        recur,
        [shaped(seq, chan, dtype=F32)] * 3 + [shaped(ny, seq, cols)] * 2,
        4 * state.size,
        "shvvvhhql hhhvh",
        at,
        *pieces,
        lower_bound.reshape(1, chan),
        head_gain.reshape(1, chan),
        state.reshape(seq, head_dim, head_dim),
        w_output,
        scratch=[pltpu.VMEM((seq, head_dim), F32)],
    )
    shape = (seq, 1, head_dim)
    new_state = (
        decay.reshape(shape)[..., None] * state
        + keygate.reshape(shape)[..., None] * values.reshape(shape)[:, :, None, :]
    )

    pair = (keep.astype(F32) + partner(give).astype(F32)).astype(BF)
    heads = swap(pair, "y")
    resid, own, outgoing = call(
        dispatch,
        [
            shaped(seq, cols, dtype=F32),
            shaped(seq, cols),
            shaped(experts * 2 * slots, half),
        ],
        4 * experts * 2 * slots * seq * half,
        "svhh hhh",
        at,
        heads,
        tokens,
        slot_rows,
    )
    arrived = swap(outgoing.reshape(experts, 2 * slots, half), HUB)
    other = partner(own)
    count = nz * nx * cap

    group = 8 * nc * 2 * slots
    lines = jnp.arange(group, dtype=jnp.int32)
    source, rest = lines // (4 * slots), lines % (4 * slots)
    side, h, kind, r = (
        rest // (2 * slots),
        rest // slots % 2,
        rest // cap % 2,
        rest % cap,
    )
    line_of = ((side * 2 + h) * 2 + kind) * (8 * cap) + source * cap + r
    both, dense_rows = call(
        unpack_rows,
        [shaped(ny, count + seq, nc * cols), shaped(nc, count, cols)],
        4 * 2 * group * group * half,
        "shvhv hh",
        at,
        line_of.reshape(1, group),
        arrived.reshape(-1, half),
        own,
        other,
    )
    whole = swap(both, "y")

    hidden_width = nx * dense_gate.shape[1]
    quarter = count // ny
    pre = call(
        dense_first_half,
        [shaped(quarter, 2 * hidden_width + 128)] * ny,
        2 * count * nc * cols * 2 * hidden_width,
        "shhgggggggg hhhh",
        at,
        dense_rows,
        ffn_gain.reshape(ny * nc, cols),
        *dense_own,
        *dense_other,
    )
    pre = [pre[0]] + [shift(pre[d], "y", d) for d in range(1, ny)]
    (parts,) = call(
        experts_and_shared,
        [shaped(ny, count + seq + 2 * quarter, nc * cols)],
        2 * 3 * (count * 2 + seq) * width * expert_gate.shape[2],
        "sqheqeqeqqqqhvvv h",
        at,
        whole,
        ffn_gain.reshape(1, width),
        expert_gate,
        gate_other,
        expert_up,
        up_other,
        expert_down,
        down_other,
        shared_gate,
        shared_up,
        shared_down,
        *pre,
    )
    parts = swap(parts, "y")
    back, shared_own, shared_send = call(
        pack_lines,
        [
            shaped(experts * 2 * slots, half),
            shaped(seq, cols, dtype=F32),
            shaped(seq, cols),
        ],
        4 * 2 * group * group * half,
        "shvdddddddd hhh",
        at,
        line_of.reshape(group, 1),
        parts,
        *dense_own,
        *dense_other,
    )

    results = swap(back.reshape(experts, 2 * slots, half), HUB)
    (mixed,) = call(
        finish,
        [shaped(seq, cols)],
        8 * experts * 2 * slots * seq * half,
        "vhhhhhvh h",
        results.reshape(experts * 2 * slots, half),
        within,
        slot_cols,
        route_weight,
        resid,
        shared_own,
        partner(shared_send),
        dense_mix.reshape(1, cols),
    )
    return (mixed, new_state)


def solution(mesh):
    torus = Mesh(mesh.devices.reshape(8, 4, 4, 2), ("z", "x", "y", "c"))
    return jax.shard_map(
        step,
        mesh=torus,
        in_specs=(
            P(EP, None),
            P(EP, TP, None, None),
            P(),
            P(EP, TP),
            P(EP, TP),
            P(EP, TP),
            P(EP, TP),
            P(TP),
            P(TP),
            P(TP, None),
            P(),
            P(EP, None),
            P(EP, None),
            P(EP, None, TP),
            P(EP, None, TP),
            P(EP, TP, None),
            P(None, TP),
            P(None, TP),
            P(TP, None),
            P(TP, EP),
            P(TP, EP),
            P(EP, TP),
            P(TP),
        ),
        out_specs=(P(EP, TP), P(EP, TP, None, None)),
        check_vma=False,
    )
```

```python
import jax
import jax.numpy as jnp
from jax import lax
from jax.experimental import pallas as pl
from jax.experimental.pallas import tpu as pltpu
from jax.sharding import Mesh
from jax.sharding import PartitionSpec as P

EP = ("z", "x")
TP = ("y", "c")
HUB = ("z", "x", "c")


EPS = 1e-06
BF = jnp.bfloat16
F32 = jnp.float32


def swap(x, axis):
    return lax.all_to_all(x, axis, split_axis=0, concat_axis=0, tiled=True)


def partner(x):
    return lax.ppermute(x, "c", [(0, 1), (1, 0)])


def shift(x, axis, by):
    size = lax.axis_size(axis)
    return lax.ppermute(x, axis, [(i, (i + by) % size) for i in range(size)])


def pick(x, index):
    return lax.dynamic_index_in_dim(x, index, 0, keepdims=False)


def dot(a, b):
    return jnp.dot(a, b, preferred_element_type=F32)


def silu(x):
    return x * jax.nn.sigmoid(x)


def call(body, outs, flops, kinds, *args, mib=52, scratch=()):
    kinds, out_kinds = kinds.split()
    moved = sum(a.size * a.dtype.itemsize for a in args) + sum(
        o.size * o.dtype.itemsize for o in outs
    )
    space = {"s": pltpu.SMEM, "v": pltpu.VMEM}
    fetched = [i for i, k in enumerate(kinds) if k in "hlqegd"]
    stored = [i for i, k in enumerate(out_kinds) if k == "h"]

    def held(i):
        shape = args[i].shape
        return {"e": shape[1:], "d": shape[1:], "g": (2, *shape[1:])}.get(kinds[i], shape)

    room = [pltpu.VMEM(held(i), args[i].dtype) for i in fetched]
    pieces = {"h": 1, "l": 1, "q": 4, "e": 4, "g": 1, "d": 1}
    n_sems = sum(pieces[kinds[i]] for i in fetched)
    out_room = [pltpu.VMEM(outs[i].shape, outs[i].dtype) for i in stored]

    def whole(*refs):
        ins, rest = list(refs[: len(args)]), refs[len(args) :]
        results, rest = list(rest[: len(outs)]), rest[len(outs) :]
        in_room, rest = rest[: len(room)], rest[len(room) :]
        result_room, rest = rest[: len(out_room)], rest[len(out_room) :]
        in_sem, out_sem, extra = rest[0], rest[1], rest[2:]
        late, now, order = [], [], []
        sem = 0
        for n, i in enumerate(fetched):
            kind = kinds[i]
            source = ins[i]
            if kind == "e":
                source = source.at[ins[0][1]]
            elif kind == "d":
                source = source.at[2]
            parts = pieces[kind]
            size = in_room[n].shape[0] // parts
            copies = []
            for p in range(parts):
                cut = pl.ds(p * size, size)
                copies.append(
                    pltpu.make_async_copy(source.at[cut], in_room[n].at[cut], in_sem.at[sem])
                )
                order.append((p, sem, copies[-1]))
                sem += 1
            if kind == "h":
                now.extend(copies)
            else:
                late.append([copy.wait for copy in copies])
            ins[i] = in_room[n]
        for _, _, copy in sorted(order, key=lambda o: o[:2]):
            copy.start()
        targets = list(results)
        for n, i in enumerate(stored):
            results[i] = result_room[n]
        for copy in now:
            copy.wait()
        if late:
            body(late, *ins, *results, *extra)
        else:
            body(*ins, *results, *extra)
        back = [
            pltpu.make_async_copy(result_room[n], targets[i], out_sem.at[n])
            for n, i in enumerate(stored)
        ]
        for copy in back:
            copy.start()
        for copy in back:
            copy.wait()

    return pl.pallas_call(
        whole,
        out_shape=outs,
        in_specs=[pl.BlockSpec(memory_space=space.get(k, pltpu.HBM)) for k in kinds],
        out_specs=[pl.BlockSpec(memory_space=space.get(k, pltpu.HBM)) for k in out_kinds],
        scratch_shapes=[
            *room,
            *out_room,
            pltpu.SemaphoreType.DMA((max(1, n_sems),)),
            pltpu.SemaphoreType.DMA((max(1, len(out_room)),)),
            *scratch,
        ],
        cost_estimate=pl.CostEstimate(flops=flops, bytes_accessed=moved, transcendentals=0),
        compiler_params=pltpu.CompilerParams(vmem_limit_bytes=mib * 2**20),
    )(*args)


def shaped(*dims, dtype=BF):
    return jax.ShapeDtypeStruct(dims, dtype)


def copies(wq, wf, wi, wo, spread_w):
    for i, block in enumerate((wq, wf, wi, wo)):
        width = block.shape[1]
        value = block[...]
        for z in range(spread_w.shape[0]):
            spread_w[z, :, i * width : (i + 1) * width] = value


def prepare(at, tokens, gain, dg, du, dd, dense, t0, t1, t2, t3, held):
    x = at[2]
    for i, block in enumerate((dg, du, dd)):
        dense[i] = block[...]
    wide = tokens[...].astype(F32)
    wide = wide * lax.rsqrt(jnp.mean(wide * wide, axis=1, keepdims=True) + EPS) * gain[...]
    low = lax.broadcasted_iota(jnp.int32, (wide.shape[0], 128), 1) < 64

    def tile(i):
        return wide[:, i * 128 : (i + 1) * 128]

    for to in range(4):
        for k in range(4):
            a, b = tile(4 * k + to // 2), tile(4 * k + 2 + to // 2)
            if to % 2 == 0:
                value = jnp.where(low, a, pltpu.roll(b, 64, 1))
            else:
                value = jnp.where(low, pltpu.roll(a, 64, 1), b)
            held[to, :, k * 128 : (k + 1) * 128] = value.astype(BF)
    for d, out in enumerate((t0, t1, t2, t3)):
        out[...] = held[lax.rem(x + d, 4)]


def recur(wait, at, p0, p1, p2, p3, bound, gain, state, w_out, decay_out, key_out, value_out, keep, give, read):
    first = at[1] == 0
    seq = p0.shape[0]
    total = (
        p0[...].astype(F32) + p1[...].astype(F32) + p2[...].astype(F32) + p3[...].astype(F32)
    )
    total = total.astype(BF).astype(F32)
    query, forget, values, gate = (total[:, i * 128 : (i + 1) * 128] for i in range(4))
    forget = jax.nn.sigmoid(forget)
    low = bound[...]
    decay = low + (1.0 - low) * forget
    key = (1.0 - low) * (1.0 - forget)
    decay_out[...] = decay
    key_out[...] = key
    value_out[...] = values
    turned = jnp.transpose(query * decay)
    for b in range(seq):
        if b % (seq // 4) == 0:
            wait[0][b // (seq // 4)]()
        read[b : b + 1, :] = jnp.sum(turned[:, b : b + 1] * state[b], axis=0, keepdims=True)
    readout = read[...] + jnp.sum(query * key, axis=1, keepdims=True) * values
    readout = readout * lax.rsqrt(jnp.mean(readout * readout, axis=1, keepdims=True) + EPS)
    head = (readout * gain[...] * silu(gate)).astype(BF)
    wait[1][0]()
    cols = keep.shape[2]
    for y in range(keep.shape[0]):
        cut = slice(2 * y * cols, (2 * y + 1) * cols)
        cut_next = slice((2 * y + 1) * cols, (2 * y + 2) * cols)
        even = dot(head, w_out[:, cut]).astype(BF)
        odd = dot(head, w_out[:, cut_next]).astype(BF)
        keep[y] = jnp.where(first, even, odd)
        give[y] = jnp.where(first, odd, even)


def dispatch(at, heads, tokens, slots, resid, own, lines):
    cols = resid.shape[1]
    half = cols // 2
    seq = resid.shape[0]
    start = pl.multiple_of((2 * at[0] + at[1]) * cols, cols)
    total = tokens[:, pl.ds(start, cols)].astype(F32)
    for i in range(heads.shape[0]):
        total = total + heads[i].astype(F32)
    resid[...] = total
    rows = total.astype(BF)
    own[...] = rows
    chunk = 192
    place = lax.broadcasted_iota(jnp.int32, (chunk, seq), 0)
    for h in range(2):
        shifted = place - 12 * h
        dense = shifted == slots[4:5, :]
        for z in range(lines.shape[0] // chunk):
            here = shifted + z * chunk
            hit = dense
            for k in range(4):
                hit = hit | (here == slots[k : k + 1, :])
            part = dot(jnp.where(hit, 1.0, 0.0).astype(BF), rows[:, h * half : (h + 1) * half])
            if h == 0:
                lines[z * chunk : (z + 1) * chunk, :] = part.astype(BF)
            else:
                before = lines[z * chunk : (z + 1) * chunk, :].astype(F32)
                lines[z * chunk : (z + 1) * chunk, :] = (before + part).astype(BF)


def finish(lines, within, slots, weight, resid, shared, shared_other, mix, out):
    seq, cols = out.shape
    half = cols // 2
    place = lax.broadcasted_iota(jnp.int32, (seq, lines.shape[0]), 1)
    gate = jax.nn.sigmoid(mix[...])
    base = resid[...] + shared[...] + shared_other[...].astype(F32)
    for h in range(2):
        routed = jnp.zeros(place.shape, F32)
        for k in range(4):
            routed = jnp.where(place == slots[:, k : k + 1] + 12 * h, weight[:, k : k + 1], routed)
        dense = jnp.where(within[...] == slots[:, 4:5] + 12 * h, 1.0, 0.0)
        cut = slice(h * half, (h + 1) * half)
        total = base[:, cut] + dot(routed.astype(BF), lines[...])
        total = total + gate[:, cut] * dot(dense.astype(BF), lines[...])
        out[:, cut] = total.astype(BF)


def unpack_rows(at, line_of, lines, own, other, both, dense):
    first = at[1] == 0
    group = line_of.shape[1]
    count = dense.shape[1]
    cols = dense.shape[2]
    half = cols // 2
    part = group // 8
    groups = lines.shape[0] // group
    move = jnp.where(
        lax.broadcasted_iota(jnp.int32, (group, group), 0) == line_of[...], 1.0, 0.0
    ).astype(BF)
    mine, others = own[...], other[...]
    both_rows = [
        jnp.where(first, mine, others),
        jnp.where(first, others, mine),
    ]
    for g in range(groups):
        rows = dot(move, lines[g * group : (g + 1) * group, :]).astype(BF)
        here = slice(g * part, (g + 1) * part)
        for side in range(2):
            for h in range(2):
                base = (side * 2 + h) * 2 * part
                at_col = side * cols + h * half
                for copy in range(both.shape[0]):
                    both[copy, here, at_col : at_col + half] = rows[base : base + part]
                dense[side, here, h * half : (h + 1) * half] = rows[base + part : base + 2 * part]
    for side in range(2):
        for copy in range(both.shape[0]):
            both[copy, count:, side * cols : (side + 1) * cols] = both_rows[side]


def dense_first_half(wait, at, rows, gain, *refs):
    y, c = at[0], at[1]
    own_w, other_w, outs = refs[:4], refs[4:8], refs[8:]
    ny = len(outs)
    size = rows.shape[1] // ny
    cols = rows.shape[2]

    def turned(side):
        return jnp.concatenate(
            [
                rows[side, pl.ds(pl.multiple_of(lax.rem(y + d, ny) * size, size), size), :]
                for d in range(ny)
            ],
            axis=0,
        ).astype(F32)

    own, other = turned(c), turned(1 - c)
    square = jnp.sum(own * own + other * other, axis=1, keepdims=True)
    high = square.astype(BF).astype(F32)
    low = square - high
    own = (own * gain[pl.ds(2 * y + c, 1), :]).astype(BF)
    other = (other * gain[pl.ds(2 * y + 1 - c, 1), :]).astype(BF)
    for i in range(4):
        wait[i][0]()
        wait[4 + i][0]()
        for kind in range(2):
            value = (dot(own, own_w[i][kind]) + dot(other, other_w[i][kind])).astype(BF)
            at_col = (kind * 4 + i) * cols
            for d in range(ny):
                outs[d][:, at_col : at_col + cols] = value[d * size : (d + 1) * size]
    lane = lax.broadcasted_iota(jnp.int32, (square.shape[0], 128), 1)
    both = jnp.where(lane < 64, high, low).astype(BF)
    for d in range(ny):
        outs[d][:, 8 * cols : 8 * cols + 128] = both[d * size : (d + 1) * size]


def dense_activation(a, b, c, d, out):
    width = out.shape[1]
    features = 2048

    def summed(cut):
        return (
            a[:, cut].astype(F32) + b[:, cut].astype(F32) + c[:, cut].astype(F32) + d[:, cut].astype(F32)
        )

    square = summed(slice(2 * width, 2 * width + 128))
    total = square[:, 0:1] + square[:, 64:65]
    scale = lax.rsqrt(total / features + EPS)
    gate = summed(slice(0, width)) * scale
    up = summed(slice(width, 2 * width)) * scale
    out[...] = (silu(gate) * up).astype(BF)


def dense_second_half(wait, at, *refs):
    y = at[0]
    hidden, own_w, other_w, out = refs[:4], refs[4:8], refs[8:12], refs[12]
    ny = len(hidden)
    size, cols = hidden[0].shape[0], out.shape[2]
    rows = jnp.concatenate([h[...] for h in hidden], axis=0)
    for side, weights in enumerate((own_w, other_w)):
        total = None
        for i in range(4):
            wait[4 * side + i][0]()
            term = dot(rows[:, i * cols : (i + 1) * cols], weights[i][...])
            total = term if total is None else total + term
        total = total.astype(BF)
        for d in range(ny):
            start = pl.multiple_of(lax.rem(y + ny - d, ny) * size, size)
            out[side, pl.ds(start, size), :] = total[d * size : (d + 1) * size]


def experts_and_shared(
    wait, at, whole, gain, gate, gate_other, up, up_other, down, down_other,
    shared_gate, shared_up, shared_down, parts,
):
    ny, lines, block = whole.shape
    count = lines - 48
    half = gate.shape[1]
    square = jnp.zeros((lines, 1), F32)
    gate_pre = up_pre = shared_pre = None

    def more(total, term):
        return term if total is None else total + term

    for i in range(ny):
        cut = slice(i * block, (i + 1) * block)
        for k in (0, 1, 2, 3, 4, 7, 8):
            wait[k][i]()
        value = whole[i].astype(F32)
        square = square + jnp.sum(value * value, axis=1, keepdims=True)
        rows = (value * gain[:, cut]).astype(BF)
        gates = jnp.concatenate([gate[cut, :], gate_other[cut, :]], axis=1)
        ups = jnp.concatenate([up[cut, :], up_other[cut, :]], axis=1)
        shared = jnp.concatenate([shared_gate[cut, :], shared_up[cut, :]], axis=1)
        gate_pre = more(gate_pre, dot(rows[:count], gates))
        up_pre = more(up_pre, dot(rows[:count], ups))
        shared_pre = more(shared_pre, dot(rows[count:], shared))
    scale = lax.rsqrt(square / (ny * block) + EPS)
    hidden = (silu(gate_pre * scale[:count]) * (up_pre * scale[:count])).astype(BF)
    shared_pre = shared_pre * scale[count:]
    shared_hidden = (silu(shared_pre[:, :half]) * shared_pre[:, half:]).astype(BF)
    for k in (5, 6, 9):
        for done in wait[k]:
            done()
    for i in range(ny):
        cut = slice(i * block, (i + 1) * block)
        downs = jnp.concatenate([down[:, cut], down_other[:, cut]], axis=0)
        parts[i, :count, :] = dot(hidden, downs).astype(BF)
        parts[i, count:, :] = dot(shared_hidden, shared_down[:, cut]).astype(BF)


def pack_lines(at, line_of, parts, dense, lines, shared_own, shared_send):
    first = at[1] == 0
    group = line_of.shape[0]
    part = group // 8
    cols = dense.shape[2]
    half = cols // 2
    count = dense.shape[1]
    groups = lines.shape[0] // group
    move = jnp.where(
        lax.broadcasted_iota(jnp.int32, (group, group), 1) == line_of[...], 1.0, 0.0
    ).astype(BF)
    total = parts[0].astype(F32)
    for i in range(1, parts.shape[0]):
        total = total + parts[i].astype(F32)
    routed = total[:count].astype(BF)
    shared = total[count:]
    shared_own[...] = jnp.where(first, shared[:, :cols], shared[:, cols:])
    shared_send[...] = jnp.where(first, shared[:, cols:], shared[:, :cols]).astype(BF)
    for g in range(groups):
        here = slice(g * part, (g + 1) * part)
        own, other = dense[0, here, :], dense[1, here, :]
        sides = [jnp.where(first, own, other), jnp.where(first, other, own)]
        stack = []
        for side in range(2):
            for h in range(2):
                at_col = side * cols + h * half
                stack.append(routed[here, at_col : at_col + half])
                stack.append(sides[side][:, h * half : (h + 1) * half])
        rows = jnp.concatenate(stack, axis=0)
        lines[g * group : (g + 1) * group, :] = dot(move, rows).astype(BF)


def step(
    tokens,
    state,
    norm_gain,
    w_query,
    w_forget,
    w_input,
    w_outgate,
    lower_bound,
    head_gain,
    w_output,
    ffn_gain,
    route_ids,
    route_weight,
    expert_gate,
    expert_up,
    expert_down,
    shared_gate,
    shared_up,
    shared_down,
    dense_gate,
    dense_up,
    dense_down,
    dense_mix,
):
    nz, nx, ny, nc = (lax.axis_size(a) for a in ("z", "x", "y", "c"))
    x, y, c = (lax.axis_index(a) for a in ("x", "y", "c"))
    seq, width = tokens.shape
    rows_w, chan = w_query.shape
    head_dim = state.shape[2]
    cols = width // (ny * nc)

    at = jnp.stack([y, c, x]).astype(jnp.int32)

    topk = route_ids.shape[1]
    experts = nz * nx * nc
    cap = max(2, 2 * seq * topk // experts)
    slots = 2 * cap
    half = cols // 2
    flat_ids = route_ids.reshape(-1)
    onehot = (flat_ids[:, None] == jnp.arange(experts, dtype=jnp.int32)[None, :]).astype(jnp.int32)
    rank = jnp.sum((jnp.cumsum(onehot, axis=0) - onehot) * onehot, axis=1)
    lines_of = (flat_ids * (2 * slots) + rank).reshape(seq, topk)
    token_ids = jnp.arange(seq, dtype=jnp.int32)
    dense_of = (token_ids // cap) * (2 * slots) + cap + token_ids % cap
    slot_cols = jnp.concatenate(
        [lines_of, dense_of[:, None], jnp.zeros((seq, 8 - topk - 1), jnp.int32)], axis=1
    )
    slot_rows = slot_cols.T
    within = (jnp.arange(experts * 2 * slots, dtype=jnp.int32) % (nx * nc * 2 * slots))[None, :]

    (spread_w,) = call(
        copies,
        [shaped(nz, rows_w, 4 * chan)],
        10**6,
        "hhhh h",
        w_query,
        w_forget,
        w_input,
        w_outgate,
        mib=58,
    )
    weights = swap(spread_w, "z").reshape(nz * rows_w, 4 * chan)
    dense_block, *columns = call(
        prepare,
        [shaped(3, *dense_gate.shape)] + [shaped(seq, nz * rows_w)] * nx,
        10**6,
        "shhhhh hhhhh",
        at,
        tokens,
        norm_gain.reshape(1, width),
        dense_gate,
        dense_up,
        dense_down,
        mib=59,
        scratch=[pltpu.VMEM((nx, seq, nz * rows_w), BF)],
    )
    mine = [columns[0]] + [shift(columns[d], "x", d) for d in range(1, nx)]
    part = dot(jnp.concatenate(mine, axis=0), weights).astype(BF)
    part = part.reshape(nx, seq, 4 * chan)
    pieces = [part[0]] + [shift(part[d], "x", -d) for d in range(1, nx)]

    dense_own = [dense_block] + [shift(dense_block, "x", d) for d in range(1, nx)]
    dense_other = [partner(block) for block in dense_own]
    gate_other, up_other, down_other = (
        partner(pick(stack, 1 - c)) for stack in (expert_gate, expert_up, expert_down)
    )

    decay, keygate, values, keep, give = call(
        recur,
        [shaped(seq, chan, dtype=F32)] * 3 + [shaped(ny, seq, cols)] * 2,
        4 * state.size,
        "shvvvhhql hhhvh",
        at,
        *pieces,
        lower_bound.reshape(1, chan),
        head_gain.reshape(1, chan),
        state.reshape(seq, head_dim, head_dim),
        w_output,
        scratch=[pltpu.VMEM((seq, head_dim), F32)],
    )
    shape = (seq, 1, head_dim)
    new_state = (
        decay.reshape(shape)[..., None] * state
        + keygate.reshape(shape)[..., None] * values.reshape(shape)[:, :, None, :]
    )

    pair = (keep.astype(F32) + partner(give).astype(F32)).astype(BF)
    heads = swap(pair, "y")
    resid, own, outgoing = call(
        dispatch,
        [
            shaped(seq, cols, dtype=F32),
            shaped(seq, cols),
            shaped(experts * 2 * slots, half),
        ],
        4 * experts * 2 * slots * seq * half,
        "svhh hhh",
        at,
        heads,
        tokens,
        slot_rows,
    )
    arrived = swap(outgoing.reshape(experts, 2 * slots, half), HUB)
    other = partner(own)
    count = nz * nx * cap

    group = 8 * nc * 2 * slots
    lines = jnp.arange(group, dtype=jnp.int32)
    source, rest = lines // (4 * slots), lines % (4 * slots)
    side, h, kind, r = (
        rest // (2 * slots),
        rest // slots % 2,
        rest // cap % 2,
        rest % cap,
    )
    line_of = ((side * 2 + h) * 2 + kind) * (8 * cap) + source * cap + r
    both, dense_rows = call(
        unpack_rows,
        [shaped(ny, count + seq, nc * cols), shaped(nc, count, cols)],
        4 * 2 * group * group * half,
        "shvhv hh",
        at,
        line_of.reshape(1, group),
        arrived.reshape(-1, half),
        own,
        other,
    )
    whole = swap(both, "y")

    hidden_width = nx * dense_gate.shape[1]
    quarter = count // ny
    pre = call(
        dense_first_half,
        [shaped(quarter, 2 * hidden_width + 128)] * ny,
        2 * count * nc * cols * 2 * hidden_width,
        "shhgggggggg hhhh",
        at,
        dense_rows,
        ffn_gain.reshape(ny * nc, cols),
        *dense_own,
        *dense_other,
    )
    pre = [pre[0]] + [shift(pre[d], "y", d) for d in range(1, ny)]
    (hidden,) = call(
        dense_activation, [shaped(quarter, hidden_width)], 10**6, "hvvv h", *pre
    )
    hidden = [hidden] + [shift(hidden, "y", d) for d in range(1, ny)]
    (dense_part,) = call(
        dense_second_half,
        [shaped(nc, count, cols)],
        2 * count * nc * cols * hidden_width,
        "shvvvdddddddd h",
        at,
        *hidden,
        *dense_own,
        *dense_other,
    )

    (parts,) = call(
        experts_and_shared,
        [shaped(ny, count + seq, nc * cols)],
        2 * 3 * (count * 2 + seq) * width * expert_gate.shape[2],
        "sqheqeqeqqqq h",
        at,
        whole,
        ffn_gain.reshape(1, width),
        expert_gate,
        gate_other,
        expert_up,
        up_other,
        expert_down,
        down_other,
        shared_gate,
        shared_up,
        shared_down,
    )
    parts = swap(parts, "y")
    back, shared_own, shared_send = call(
        pack_lines,
        [
            shaped(experts * 2 * slots, half),
            shaped(seq, cols, dtype=F32),
            shaped(seq, cols),
        ],
        4 * 2 * group * group * half,
        "shvh hhh",
        at,
        line_of.reshape(group, 1),
        parts,
        dense_part,
    )

    results = swap(back.reshape(experts, 2 * slots, half), HUB)
    (mixed,) = call(
        finish,
        [shaped(seq, cols)],
        8 * experts * 2 * slots * seq * half,
        "vhhhhhvh h",
        results.reshape(experts * 2 * slots, half),
        within,
        slot_cols,
        route_weight,
        resid,
        shared_own,
        partner(shared_send),
        dense_mix.reshape(1, cols),
    )
    return (mixed, new_state)


def solution(mesh):
    torus = Mesh(mesh.devices.reshape(8, 4, 4, 2), ("z", "x", "y", "c"))
    return jax.shard_map(
        step,
        mesh=torus,
        in_specs=(
            P(EP, None),
            P(EP, TP, None, None),
            P(),
            P(EP, TP),
            P(EP, TP),
            P(EP, TP),
            P(EP, TP),
            P(TP),
            P(TP),
            P(TP, None),
            P(),
            P(EP, None),
            P(EP, None),
            P(EP, None, TP),
            P(EP, None, TP),
            P(EP, TP, None),
            P(None, TP),
            P(None, TP),
            P(TP, None),
            P(TP, EP),
            P(TP, EP),
            P(EP, TP),
            P(TP),
        ),
        out_specs=(P(EP, TP), P(EP, TP, None, None)),
        check_vma=False,
    )
```

```python
import jax
import jax.numpy as jnp
from jax import lax
from jax.experimental import pallas as pl
from jax.experimental.pallas import tpu as pltpu
from jax.sharding import Mesh
from jax.sharding import PartitionSpec as P

EP = ("z", "x")
TP = ("y", "c")
HUB = ("z", "x", "c")


EPS = 1e-06
BF = jnp.bfloat16
F32 = jnp.float32


def swap(x, axis):
    return lax.all_to_all(x, axis, split_axis=0, concat_axis=0, tiled=True)


def partner(x):
    return lax.ppermute(x, "c", [(0, 1), (1, 0)])


def shift(x, axis, by):
    size = lax.axis_size(axis)
    return lax.ppermute(x, axis, [(i, (i + by) % size) for i in range(size)])


def pick(x, index):
    return lax.dynamic_index_in_dim(x, index, 0, keepdims=False)


def dot(a, b):
    return jnp.dot(a, b, preferred_element_type=F32)


def silu(x):
    return x * jax.nn.sigmoid(x)


def call(body, outs, flops, kinds, *args, mib=53, scratch=()):
    kinds, out_kinds = kinds.split()
    placed = kinds[0] == "s"
    kinds = kinds[1:] if placed else kinds
    moved = sum(a.size * a.dtype.itemsize for a in args) + sum(
        o.size * o.dtype.itemsize for o in outs
    )
    space = {"v": pltpu.VMEM}
    fetched = [i for i, k in enumerate(kinds) if k in "hlqegd"]
    stored = [i for i, k in enumerate(out_kinds) if k == "h"]

    def held(i):
        shape = args[i].shape
        return {"e": shape[1:], "d": shape[1:], "g": (2, *shape[1:])}.get(kinds[i], shape)

    room = [pltpu.VMEM(held(i), args[i].dtype) for i in fetched]
    pieces = {"h": 1, "l": 1, "q": 4, "e": 4, "g": 1, "d": 1}
    n_sems = sum(pieces[kinds[i]] for i in fetched)
    out_room = [pltpu.VMEM(outs[i].shape, outs[i].dtype) for i in stored]

    def whole(*refs):
        ins, rest = list(refs[: len(args)]), refs[len(args) :]
        results, rest = list(rest[: len(outs)]), rest[len(outs) :]
        in_room, rest = rest[: len(room)], rest[len(room) :]
        result_room, rest = rest[: len(out_room)], rest[len(out_room) :]
        in_sem, out_sem, extra = rest[0], rest[1], rest[2:]
        at = tuple(lax.axis_index(a) for a in ("y", "c", "x"))
        late, now, order = [], [], []
        sem = 0
        for n, i in enumerate(fetched):
            kind = kinds[i]
            source = ins[i]
            if kind == "e":
                source = source.at[at[1]]
            elif kind == "d":
                source = source.at[2]
            parts = pieces[kind]
            size = in_room[n].shape[0] // parts
            copies = []
            for p in range(parts):
                cut = pl.ds(p * size, size)
                copies.append(
                    pltpu.make_async_copy(source.at[cut], in_room[n].at[cut], in_sem.at[sem])
                )
                order.append((p, sem, copies[-1]))
                sem += 1
            if kind == "h":
                now.extend(copies)
            else:
                late.append([copy.wait for copy in copies])
            ins[i] = in_room[n]
        for _, _, copy in sorted(order, key=lambda o: o[:2]):
            copy.start()
        targets = list(results)
        for n, i in enumerate(stored):
            results[i] = result_room[n]
        for copy in now:
            copy.wait()
        before = ([late] if late else []) + ([at] if placed else [])
        body(*before, *ins, *results, *extra)
        back = [
            pltpu.make_async_copy(result_room[n], targets[i], out_sem.at[n])
            for n, i in enumerate(stored)
        ]
        for copy in back:
            copy.start()
        for copy in back:
            copy.wait()

    return pl.pallas_call(
        whole,
        out_shape=outs,
        in_specs=[pl.BlockSpec(memory_space=space.get(k, pltpu.HBM)) for k in kinds],
        out_specs=[pl.BlockSpec(memory_space=space.get(k, pltpu.HBM)) for k in out_kinds],
        scratch_shapes=[
            *room,
            *out_room,
            pltpu.SemaphoreType.DMA((max(1, n_sems),)),
            pltpu.SemaphoreType.DMA((max(1, len(out_room)),)),
            *scratch,
        ],
        cost_estimate=pl.CostEstimate(flops=flops, bytes_accessed=moved, transcendentals=0),
        compiler_params=pltpu.CompilerParams(vmem_limit_bytes=mib * 2**20),
    )(*args)


def shaped(*dims, dtype=BF):
    return jax.ShapeDtypeStruct(dims, dtype)


def copies(wq, wf, wi, wo, spread_w):
    for i, block in enumerate((wq, wf, wi, wo)):
        width = block.shape[1]
        value = block[...]
        for z in range(spread_w.shape[0]):
            spread_w[z, :, i * width : (i + 1) * width] = value


def prepare(at, tokens, gain, dg, du, dd, dense, t0, t1, t2, t3, held):
    x = at[2]
    for i, block in enumerate((dg, du, dd)):
        dense[i] = block[...]
    wide = tokens[...].astype(F32)
    wide = wide * lax.rsqrt(jnp.mean(wide * wide, axis=1, keepdims=True) + EPS) * gain[...]
    low = lax.broadcasted_iota(jnp.int32, (wide.shape[0], 128), 1) < 64

    def tile(i):
        return wide[:, i * 128 : (i + 1) * 128]

    for to in range(4):
        for k in range(4):
            a, b = tile(4 * k + to // 2), tile(4 * k + 2 + to // 2)
            if to % 2 == 0:
                value = jnp.where(low, a, pltpu.roll(b, 64, 1))
            else:
                value = jnp.where(low, pltpu.roll(a, 64, 1), b)
            held[to, :, k * 128 : (k + 1) * 128] = value.astype(BF)
    for d, out in enumerate((t0, t1, t2, t3)):
        out[...] = held[lax.rem(x + d, 4)]


def recur(wait, at, p0, p1, p2, p3, bound, gain, state, w_out, decay_out, key_out, value_out, keep, give, read):
    first = at[1] == 0
    seq = p0.shape[0]
    total = (
        p0[...].astype(F32) + p1[...].astype(F32) + p2[...].astype(F32) + p3[...].astype(F32)
    )
    total = total.astype(BF).astype(F32)
    query, forget, values, gate = (total[:, i * 128 : (i + 1) * 128] for i in range(4))
    forget = jax.nn.sigmoid(forget)
    low = bound[...]
    decay = low + (1.0 - low) * forget
    key = (1.0 - low) * (1.0 - forget)
    decay_out[...] = decay
    key_out[...] = key
    value_out[...] = values
    turned = jnp.transpose(query * decay)
    for b in range(seq):
        if b % (seq // 4) == 0:
            wait[0][b // (seq // 4)]()
        read[b : b + 1, :] = jnp.sum(turned[:, b : b + 1] * state[b], axis=0, keepdims=True)
    readout = read[...] + jnp.sum(query * key, axis=1, keepdims=True) * values
    readout = readout * lax.rsqrt(jnp.mean(readout * readout, axis=1, keepdims=True) + EPS)
    head = (readout * gain[...] * silu(gate)).astype(BF)
    wait[1][0]()
    cols = keep.shape[2]
    for y in range(keep.shape[0]):
        cut = slice(2 * y * cols, (2 * y + 1) * cols)
        cut_next = slice((2 * y + 1) * cols, (2 * y + 2) * cols)
        even = dot(head, w_out[:, cut]).astype(BF)
        odd = dot(head, w_out[:, cut_next]).astype(BF)
        keep[y] = jnp.where(first, even, odd)
        give[y] = jnp.where(first, odd, even)


def dispatch(at, heads, tokens, slots, resid, own, lines):
    cols = resid.shape[1]
    half = cols // 2
    seq = resid.shape[0]
    start = pl.multiple_of((2 * at[0] + at[1]) * cols, cols)
    total = tokens[:, pl.ds(start, cols)].astype(F32)
    for i in range(heads.shape[0]):
        total = total + heads[i].astype(F32)
    resid[...] = total
    rows = total.astype(BF)
    own[...] = rows
    chunk = 192
    place = lax.broadcasted_iota(jnp.int32, (chunk, seq), 0)
    for h in range(2):
        shifted = place - 12 * h
        dense = shifted == slots[4:5, :]
        for z in range(lines.shape[0] // chunk):
            here = shifted + z * chunk
            hit = dense
            for k in range(4):
                hit = hit | (here == slots[k : k + 1, :])
            part = dot(jnp.where(hit, 1.0, 0.0).astype(BF), rows[:, h * half : (h + 1) * half])
            if h == 0:
                lines[z * chunk : (z + 1) * chunk, :] = part.astype(BF)
            else:
                before = lines[z * chunk : (z + 1) * chunk, :].astype(F32)
                lines[z * chunk : (z + 1) * chunk, :] = (before + part).astype(BF)


def finish(lines, within, slots, weight, resid, shared, mix, out):
    seq, cols = out.shape
    half = cols // 2
    place = lax.broadcasted_iota(jnp.int32, (seq, lines.shape[0]), 1)
    gate = jax.nn.sigmoid(mix[...])
    base = resid[...] + shared[...]
    for h in range(2):
        routed = jnp.zeros(place.shape, F32)
        for k in range(4):
            routed = jnp.where(place == slots[:, k : k + 1] + 12 * h, weight[:, k : k + 1], routed)
        dense = jnp.where(within[...] == slots[:, 4:5] + 12 * h, 1.0, 0.0)
        cut = slice(h * half, (h + 1) * half)
        total = base[:, cut] + dot(routed.astype(BF), lines[...])
        total = total + gate[:, cut] * dot(dense.astype(BF), lines[...])
        out[:, cut] = total.astype(BF)


def unpack_rows(line_of, lines, routed, dense):
    group = line_of.shape[1]
    cols = dense.shape[2]
    half = cols // 2
    part = group // 8
    groups = lines.shape[0] // group
    move = jnp.where(
        lax.broadcasted_iota(jnp.int32, (group, group), 0) == line_of[...], 1.0, 0.0
    ).astype(BF)
    for g in range(groups):
        rows = dot(move, lines[g * group : (g + 1) * group, :]).astype(BF)
        here = slice(g * part, (g + 1) * part)
        for side in range(2):
            for h in range(2):
                base = (side * 2 + h) * 2 * part
                at_col = side * cols + h * half
                for copy in range(routed.shape[0]):
                    routed[copy, here, at_col : at_col + half] = rows[base : base + part]
                dense[side, here, h * half : (h + 1) * half] = rows[base + part : base + 2 * part]


def shared_expert(wait, at, s0, s1, s2, s3, gain, gate, up, down, keep, give):
    y, c = at[0], at[1]
    first = c == 0
    cols = keep.shape[2]
    half = gate.shape[1]
    square = total = None
    for k in (0, 1):
        wait[k][0]()
    for d, piece in enumerate((s0, s1, s2, s3)):
        for side, core in enumerate((c, 1 - c)):
            block = 2 * lax.rem(y + 4 - d, 4) + core
            cut = pl.ds(pl.multiple_of(block * cols, cols), cols)
            value = piece[:, side * cols : (side + 1) * cols].astype(F32)
            more = jnp.sum(value * value, axis=1, keepdims=True)
            square = more if square is None else square + more
            rows = (value * gain[pl.ds(block, 1), :]).astype(BF)
            term = dot(rows, jnp.concatenate([gate[cut, :], up[cut, :]], axis=1))
            total = term if total is None else total + term
    total = total * lax.rsqrt(square / (8 * cols) + EPS)
    hidden = (silu(total[:, :half]) * total[:, half:]).astype(BF)
    wait[2][0]()
    for i in range(keep.shape[0]):
        even = dot(hidden, down[:, 2 * i * cols : (2 * i + 1) * cols]).astype(BF)
        odd = dot(hidden, down[:, (2 * i + 1) * cols : (2 * i + 2) * cols]).astype(BF)
        keep[i] = jnp.where(first, even, odd)
        give[i] = jnp.where(first, odd, even)


def dense_first_half(wait, at, rows, gain, *refs):
    y, c = at[0], at[1]
    own_w, other_w, outs = refs[:4], refs[4:8], refs[8:]
    ny = len(outs)
    size = rows.shape[1] // ny
    cols = rows.shape[2]

    def turned(side):
        return jnp.concatenate(
            [
                rows[side, pl.ds(pl.multiple_of(lax.rem(y + d, ny) * size, size), size), :]
                for d in range(ny)
            ],
            axis=0,
        ).astype(F32)

    own, other = turned(c), turned(1 - c)
    square = jnp.sum(own * own + other * other, axis=1, keepdims=True)
    high = square.astype(BF).astype(F32)
    low = square - high
    own = (own * gain[pl.ds(2 * y + c, 1), :]).astype(BF)
    other = (other * gain[pl.ds(2 * y + 1 - c, 1), :]).astype(BF)
    for i in range(4):
        wait[i][0]()
        wait[4 + i][0]()
        for kind in range(2):
            value = (dot(own, own_w[i][kind]) + dot(other, other_w[i][kind])).astype(BF)
            at_col = (kind * 4 + i) * cols
            for d in range(ny):
                outs[d][:, at_col : at_col + cols] = value[d * size : (d + 1) * size]
    lane = lax.broadcasted_iota(jnp.int32, (square.shape[0], 128), 1)
    both = jnp.where(lane < 64, high, low).astype(BF)
    for d in range(ny):
        outs[d][:, 8 * cols : 8 * cols + 128] = both[d * size : (d + 1) * size]


def dense_activation(a, b, c, d, out):
    width = out.shape[1]
    features = 2048

    def summed(cut):
        return (
            a[:, cut].astype(F32) + b[:, cut].astype(F32) + c[:, cut].astype(F32) + d[:, cut].astype(F32)
        )

    square = summed(slice(2 * width, 2 * width + 128))
    total = square[:, 0:1] + square[:, 64:65]
    scale = lax.rsqrt(total / features + EPS)
    gate = summed(slice(0, width)) * scale
    up = summed(slice(width, 2 * width)) * scale
    out[...] = (silu(gate) * up).astype(BF)


def dense_second_half(wait, at, *refs):
    y = at[0]
    hidden, own_w, other_w, out = refs[:4], refs[4:8], refs[8:12], refs[12]
    ny = len(hidden)
    size, cols = hidden[0].shape[0], out.shape[2]
    rows = jnp.concatenate([h[...] for h in hidden], axis=0)
    for side, weights in enumerate((own_w, other_w)):
        total = None
        for i in range(4):
            wait[4 * side + i][0]()
            term = dot(rows[:, i * cols : (i + 1) * cols], weights[i][...])
            total = term if total is None else total + term
        total = total.astype(BF)
        for d in range(ny):
            start = pl.multiple_of(lax.rem(y + ny - d, ny) * size, size)
            out[side, pl.ds(start, size), :] = total[d * size : (d + 1) * size]


def experts(
    wait, at, whole, gain, gate, gate_other, up, up_other, down, down_other,
    shared, shared_other, parts,
):
    ny, count, block = whole.shape
    square = jnp.zeros((count, 1), F32)
    gate_pre = up_pre = None

    def more(total, term):
        return term if total is None else total + term

    for i in range(ny):
        cut = slice(i * block, (i + 1) * block)
        for k in (0, 1, 2, 3, 4):
            wait[k][i]()
        value = whole[i].astype(F32)
        square = square + jnp.sum(value * value, axis=1, keepdims=True)
        rows = (value * gain[:, cut]).astype(BF)
        gates = jnp.concatenate([gate[cut, :], gate_other[cut, :]], axis=1)
        ups = jnp.concatenate([up[cut, :], up_other[cut, :]], axis=1)
        gate_pre = more(gate_pre, dot(rows, gates))
        up_pre = more(up_pre, dot(rows, ups))
    scale = lax.rsqrt(square / (ny * block) + EPS)
    hidden = (silu(gate_pre * scale) * (up_pre * scale)).astype(BF)
    for k in (5, 6):
        for done in wait[k]:
            done()
    tall, cols = shared.shape[1] // 2, shared.shape[2]
    for i in range(ny):
        cut = slice(i * block, (i + 1) * block)
        downs = jnp.concatenate([down[:, cut], down_other[:, cut]], axis=0)
        parts[i, :count, :] = dot(hidden, downs).astype(BF)
        both = (shared[i].astype(F32) + shared_other[i].astype(F32)).astype(BF)
        parts[i, count:, :cols] = both[:tall]
        parts[i, count:, cols:] = both[tall:]


def pack_lines(at, line_of, parts, dense, lines, shared_out):
    first = at[1] == 0
    group = line_of.shape[0]
    part = group // 8
    cols = dense.shape[2]
    half = cols // 2
    count = dense.shape[1]
    groups = lines.shape[0] // group
    move = jnp.where(
        lax.broadcasted_iota(jnp.int32, (group, group), 1) == line_of[...], 1.0, 0.0
    ).astype(BF)
    total = parts[0].astype(F32)
    for i in range(1, parts.shape[0]):
        total = total + parts[i].astype(F32)
    routed = total[:count].astype(BF)
    tall = shared_out.shape[0] // 2
    shared_out[:tall, :] = total[count:, :cols]
    shared_out[tall:, :] = total[count:, cols:]
    for g in range(groups):
        here = slice(g * part, (g + 1) * part)
        own, other = dense[0, here, :], dense[1, here, :]
        sides = [jnp.where(first, own, other), jnp.where(first, other, own)]
        stack = []
        for side in range(2):
            for h in range(2):
                at_col = side * cols + h * half
                stack.append(routed[here, at_col : at_col + half])
                stack.append(sides[side][:, h * half : (h + 1) * half])
        rows = jnp.concatenate(stack, axis=0)
        lines[g * group : (g + 1) * group, :] = dot(move, rows).astype(BF)


def step(
    tokens,
    state,
    norm_gain,
    w_query,
    w_forget,
    w_input,
    w_outgate,
    lower_bound,
    head_gain,
    w_output,
    ffn_gain,
    route_ids,
    route_weight,
    expert_gate,
    expert_up,
    expert_down,
    shared_gate,
    shared_up,
    shared_down,
    dense_gate,
    dense_up,
    dense_down,
    dense_mix,
):
    nz, nx, ny, nc = (lax.axis_size(a) for a in ("z", "x", "y", "c"))
    _, _, c = (lax.axis_index(a) for a in ("x", "y", "c"))
    seq, width = tokens.shape
    rows_w, chan = w_query.shape
    head_dim = state.shape[2]
    cols = width // (ny * nc)

    topk = route_ids.shape[1]
    n_experts = nz * nx * nc
    cap = max(2, 2 * seq * topk // n_experts)
    slots = 2 * cap
    half = cols // 2
    flat_ids = route_ids.reshape(-1)
    onehot = (flat_ids[:, None] == jnp.arange(n_experts, dtype=jnp.int32)[None, :]).astype(jnp.int32)
    rank = jnp.sum((jnp.cumsum(onehot, axis=0) - onehot) * onehot, axis=1)
    lines_of = (flat_ids * (2 * slots) + rank).reshape(seq, topk)
    token_ids = jnp.arange(seq, dtype=jnp.int32)
    dense_of = (token_ids // cap) * (2 * slots) + cap + token_ids % cap
    slot_cols = jnp.concatenate(
        [lines_of, dense_of[:, None], jnp.zeros((seq, 8 - topk - 1), jnp.int32)], axis=1
    )
    slot_rows = slot_cols.T
    within = (jnp.arange(n_experts * 2 * slots, dtype=jnp.int32) % (nx * nc * 2 * slots))[None, :]

    (spread_w,) = call(
        copies,
        [shaped(nz, rows_w, 4 * chan)],
        10**6,
        "hhhh h",
        w_query,
        w_forget,
        w_input,
        w_outgate,
        mib=58,
    )
    weights = swap(spread_w, "z").reshape(nz * rows_w, 4 * chan)
    dense_block, *columns = call(
        prepare,
        [shaped(3, *dense_gate.shape)] + [shaped(seq, nz * rows_w)] * nx,
        10**6,
        "shhhhh hhhhh",
        tokens,
        norm_gain.reshape(1, width),
        dense_gate,
        dense_up,
        dense_down,
        mib=59,
        scratch=[pltpu.VMEM((nx, seq, nz * rows_w), BF)],
    )
    mine = [columns[0]] + [shift(columns[d], "x", d) for d in range(1, nx)]
    part = dot(jnp.concatenate(mine, axis=0), weights).astype(BF)
    part = part.reshape(nx, seq, 4 * chan)
    pieces = [part[0]] + [shift(part[d], "x", -d) for d in range(1, nx)]

    dense_own = [dense_block] + [shift(dense_block, "x", d) for d in range(1, nx)]
    dense_other = [partner(block) for block in dense_own]
    gate_other, up_other, down_other = (
        partner(pick(stack, 1 - c)) for stack in (expert_gate, expert_up, expert_down)
    )

    decay, keygate, values, keep, give = call(
        recur,
        [shaped(seq, chan, dtype=F32)] * 3 + [shaped(ny, seq, cols)] * 2,
        4 * state.size,
        "shvvvhhql hhhvh",
        *pieces,
        lower_bound.reshape(1, chan),
        head_gain.reshape(1, chan),
        state.reshape(seq, head_dim, head_dim),
        w_output,
        scratch=[pltpu.VMEM((seq, head_dim), F32)],
    )
    shape = (seq, 1, head_dim)
    new_state = (
        decay.reshape(shape)[..., None] * state
        + keygate.reshape(shape)[..., None] * values.reshape(shape)[:, :, None, :]
    )

    pair = (keep.astype(F32) + partner(give).astype(F32)).astype(BF)
    heads = swap(pair, "y")
    resid, own, outgoing = call(
        dispatch,
        [
            shaped(seq, cols, dtype=F32),
            shaped(seq, cols),
            shaped(n_experts * 2 * slots, half),
        ],
        4 * n_experts * 2 * slots * seq * half,
        "svhh hhh",
        heads,
        tokens,
        slot_rows,
    )
    arrived = swap(outgoing.reshape(n_experts, 2 * slots, half), HUB)
    other = partner(own)
    count = nz * nx * cap

    group = 8 * nc * 2 * slots
    lines = jnp.arange(group, dtype=jnp.int32)
    source, rest = lines // (4 * slots), lines % (4 * slots)
    side, h, kind, r = (
        rest // (2 * slots),
        rest // slots % 2,
        rest // cap % 2,
        rest % cap,
    )
    line_of = ((side * 2 + h) * 2 + kind) * (8 * cap) + source * cap + r
    lines_own = jnp.concatenate([own, other], axis=1)
    pieces = [lines_own] + [shift(lines_own, "y", d) for d in range(1, ny)]
    shared_keep, shared_give = call(
        shared_expert,
        [shaped(ny, seq, cols)] * 2,
        2 * 3 * seq * width * shared_gate.shape[1],
        "shvvvhlll hh",
        *pieces,
        ffn_gain.reshape(ny * nc, cols),
        shared_gate,
        shared_up,
        shared_down,
    )
    shared_other = partner(shared_give)

    both, dense_rows = call(
        unpack_rows,
        [shaped(ny, count, nc * cols), shaped(nc, count, cols)],
        4 * 2 * group * group * half,
        "hv hh",
        line_of.reshape(1, group),
        arrived.reshape(-1, half),
    )
    whole = swap(both, "y")

    hidden_width = nx * dense_gate.shape[1]
    quarter = count // ny
    pre = call(
        dense_first_half,
        [shaped(quarter, 2 * hidden_width + 128)] * ny,
        2 * count * nc * cols * 2 * hidden_width,
        "shhgggggggg hhhh",
        dense_rows,
        ffn_gain.reshape(ny * nc, cols),
        *dense_own,
        *dense_other,
    )
    pre = [pre[0]] + [shift(pre[d], "y", d) for d in range(1, ny)]
    (hidden,) = call(
        dense_activation, [shaped(quarter, hidden_width)], 10**6, "hvvv h", *pre
    )
    hidden = [hidden] + [shift(hidden, "y", d) for d in range(1, ny)]
    (dense_part,) = call(
        dense_second_half,
        [shaped(nc, count, cols)],
        2 * count * nc * cols * hidden_width,
        "shvvvdddddddd h",
        *hidden,
        *dense_own,
        *dense_other,
    )

    (parts,) = call(
        experts,
        [shaped(ny, count + seq // 2, nc * cols)],
        2 * 3 * count * 2 * width * expert_gate.shape[2],
        "sqheqeqeqhv h",
        whole,
        ffn_gain.reshape(1, width),
        expert_gate,
        gate_other,
        expert_up,
        up_other,
        expert_down,
        down_other,
        shared_keep,
        shared_other,
    )
    parts = swap(parts, "y")
    back, shared_out = call(
        pack_lines,
        [shaped(n_experts * 2 * slots, half), shaped(seq, cols, dtype=F32)],
        4 * 2 * group * group * half,
        "shvh hh",
        line_of.reshape(group, 1),
        parts,
        dense_part,
    )

    results = swap(back.reshape(n_experts, 2 * slots, half), HUB)
    (mixed,) = call(
        finish,
        [shaped(seq, cols)],
        8 * n_experts * 2 * slots * seq * half,
        "vhhhhhh h",
        results.reshape(n_experts * 2 * slots, half),
        within,
        slot_cols,
        route_weight,
        resid,
        shared_out,
        dense_mix.reshape(1, cols),
    )
    return (mixed, new_state)


def solution(mesh):
    torus = Mesh(mesh.devices.reshape(8, 4, 4, 2), ("z", "x", "y", "c"))
    return jax.shard_map(
        step,
        mesh=torus,
        in_specs=(
            P(EP, None),
            P(EP, TP, None, None),
            P(),
            P(EP, TP),
            P(EP, TP),
            P(EP, TP),
            P(EP, TP),
            P(TP),
            P(TP),
            P(TP, None),
            P(),
            P(EP, None),
            P(EP, None),
            P(EP, None, TP),
            P(EP, None, TP),
            P(EP, TP, None),
            P(None, TP),
            P(None, TP),
            P(TP, None),
            P(TP, EP),
            P(TP, EP),
            P(EP, TP),
            P(TP),
        ),
        out_specs=(P(EP, TP), P(EP, TP, None, None)),
        check_vma=False,
    )
```
